256 devices in a mesh: kv: 32 (over z, x), tp: 8 (over y, core).
Axes of the slice: x: 4, y: 4, z: 8, core: 2. Of those that a mesh axis runs over, the one named last changes fastest.
Arguments:
- tokens: bfloat16 [512, 2048], P(None, 'kv'), may hold values from -16 to 16
- norm_gain: bfloat16 [2048], P('kv'), may hold values from 0.099609375 to 1.8984375
- w_query: bfloat16 [2048, 1024], P('kv', 'tp'), may hold values from -0.125 to 0.125
- w_key: bfloat16 [2048, 1024], P('kv', 'tp'), may hold values from -0.125 to 0.125
- w_value: bfloat16 [2048, 2048], P('kv', 'tp'), may hold values from -0.125 to 0.125
- w_gate: bfloat16 [2048, 2048], P('kv', 'tp'), may hold values from -0.125 to 0.125
- w_decay: bfloat16 [2048, 1024], P('kv', 'tp'), may hold values from -0.5 to 0.5
- log_decay: float32 [512, 1024], P('kv', 'tp'), may hold values from -1.5 to 0
- state: float32 [512, 8, 128, 256], P('kv', 'tp'), may hold values from -6 to 6
- out_gain: float32 [256], replicated, may hold values from 0.1 to 1.9
- w_out: bfloat16 [2048, 2048], P('tp', 'kv'), may hold values from -0.125 to 0.125
- mixer_gain: bfloat16 [2048], P('kv'), may hold values from 0.099609375 to 1.8984375
- w_ffgate: bfloat16 [2048, 6144], P('kv', 'tp'), may hold values from -0.125 to 0.125
- w_ffup: bfloat16 [2048, 6144], P('kv', 'tp'), may hold values from -0.125 to 0.125
- w_down: bfloat16 [6144, 2048], P('tp', 'kv'), may hold values from -0.078125 to 0.078125
Outputs:
- result: bfloat16 [512, 2048], P(None, 'kv')
- new_state: float32 [512, 8, 128, 256], P('kv', 'tp')
The draws below stay inside these ranges and needn't reach their ends.
All inputs are finite; a program needn't handle non-finite values.
Results may differ from the reference program's by a relative error of at most 0.028.
Values may be sent and summed in bfloat16 or wider, within the bound.
A program may use at most 64 MiB of HBM per device.

```python
import math
import jax
import jax.numpy as jnp
from jax import lax

D = 2048
HEADS = 8
DK = 128
DV = 256
FF = 6144
BATCH = 512
KW = 1024
VW = 2048
N_TP = 8


def draw_tokens(key, part):
    base = jnp.clip(jax.random.normal(jax.random.fold_in(key, 11), (BATCH, D), jnp.float32), -4.0, 4.0)
    rough = jax.random.uniform(jax.random.fold_in(key, 12), (1, D), jnp.float32, 0.5, 1.5)
    ramp = jnp.exp(jnp.linspace(0.0, math.log(6.0), D))[None, :]
    values = base * ramp * rough / 2.5
    return jnp.clip(values, -16.0, 16.0).astype(jnp.bfloat16)


def steps_of(key, shape, cuts, smallest, largest):
    def one(dim, shards_of):
        draws = jax.random.uniform(jax.random.fold_in(jax.random.fold_in(key, 6), dim), (shards_of,), jnp.float32, smallest / len(cuts), largest / len(cuts))
        return jnp.repeat(jnp.exp(draws), shape[dim] // shards_of).reshape((-1,) + (1,) * (len(shape) - dim - 1))

    loudness = one(*cuts[0])
    for cut in cuts[1:]:
        loudness = loudness * one(*cut)
    return loudness


def noise(own_key, dims, deviation, limit, shards=(), dtype=jnp.bfloat16):
    array = deviation * jax.random.normal(own_key, dims, jnp.float32)
    if shards:
        array = array * steps_of(own_key, dims, shards, -0.22, 0.18)
    return jnp.clip(array, -limit, limit).astype(dtype)


def setup_inputs(seed: int = 0) -> dict:
    arg_keys = jax.random.split(jax.random.key(seed), 16)
    tokens = draw_tokens(jax.random.fold_in(arg_keys[15], 71), 0)
    norm_gain = jnp.clip(1.0 + 0.18 * jax.random.normal(arg_keys[1], (D,), jnp.float32), 0.099609375, 1.8984375).astype(jnp.bfloat16)
    w_query = noise(arg_keys[2], (D, KW), D ** -0.5, 0.125, ((0, 32), (1, 8)))
    w_key = noise(arg_keys[3], (D, KW), D ** -0.5, 0.125, ((0, 32), (1, 8)))
    w_value = noise(arg_keys[4], (D, VW), D ** -0.5, 0.125, ((0, 32), (1, 8)))
    w_gate = noise(arg_keys[5], (D, VW), D ** -0.5, 0.125, ((0, 32), (1, 8)))
    w_decay = noise(arg_keys[6], (D, KW), (D // 16) ** -0.5, 0.5, ((0, 32), (1, 8)))
    log_decay = jnp.clip(-1.5 + 1.5 * jax.random.uniform(arg_keys[7], (BATCH, KW), jnp.float32) ** steps_of(arg_keys[7], (BATCH, KW), ((0, 32), (1, 8)), -0.2, 0.2), -1.5, 0.0)
    state = noise(arg_keys[8], (BATCH, HEADS, DK, DV), 1.0, 6.0, ((0, 32), (1, 8)), jnp.float32)
    out_gain = jnp.clip(1.0 + 0.18 * jax.random.normal(arg_keys[9], (DV,), jnp.float32), 0.1, 1.9)
    w_out = noise(arg_keys[10], (VW, D), VW ** -0.5, 0.125, ((0, 8), (1, 32)))
    mixer_gain = jnp.clip(1.0 + 0.18 * jax.random.normal(arg_keys[11], (D,), jnp.float32), 0.099609375, 1.8984375).astype(jnp.bfloat16)
    w_ffgate = noise(arg_keys[12], (D, FF), D ** -0.5, 0.125, ((0, 32), (1, 8)))
    w_ffup = noise(arg_keys[13], (D, FF), D ** -0.5, 0.125, ((0, 32), (1, 8)))
    w_down = noise(arg_keys[14], (FF, D), FF ** -0.5, 0.078125, ((0, 8), (1, 32)))
    return dict(tokens=tokens, norm_gain=norm_gain, w_query=w_query, w_key=w_key, w_value=w_value, w_gate=w_gate, w_decay=w_decay, log_decay=log_decay, state=state, out_gain=out_gain, w_out=w_out, mixer_gain=mixer_gain, w_ffgate=w_ffgate, w_ffup=w_ffup, w_down=w_down)


eps = 1e-06
gate_norm = 16.0

def group_sum(left, right, groups):
    width = left.shape[1] // groups
    total = jnp.zeros((left.shape[0], right.shape[1]), jnp.float32)
    for group in range(groups):
        part = jnp.dot(left[:, group * width:(group + 1) * width], right[group * width:(group + 1) * width], preferred_element_type=jnp.float32)
        part = lax.optimization_barrier(part.astype(jnp.bfloat16))
        total = total + part.astype(jnp.float32)
    return total

def reference(tokens, norm_gain, w_query, w_key, w_value, w_gate, w_decay, log_decay, state, out_gain, w_out, mixer_gain, w_ffgate, w_ffup, w_down):
    wide = tokens.astype(jnp.float32)
    scaled = (wide * norm_gain.astype(jnp.float32)).astype(jnp.bfloat16)
    inv = lax.rsqrt(lax.optimization_barrier(jnp.mean(wide * wide, axis=1, keepdims=True)) + eps)
    query = jnp.dot(scaled, w_query, preferred_element_type=jnp.float32) * inv
    key = jnp.dot(scaled, w_key, preferred_element_type=jnp.float32) * inv
    value = jnp.dot(scaled, w_value, preferred_element_type=jnp.float32) * inv
    gate = jnp.dot(scaled, w_gate, preferred_element_type=jnp.float32) * inv
    decay_pre = jnp.dot(scaled, w_decay, preferred_element_type=jnp.float32) * inv
    log_a = jax.nn.log_sigmoid(decay_pre) / gate_norm + log_decay
    query = query.reshape(BATCH, HEADS, DK) * DK ** (-0.5)
    key = key.reshape(BATCH, HEADS, DK)
    value = value.reshape(BATCH, HEADS, DV)
    new_state = state * jnp.exp(log_a).reshape(BATCH, HEADS, DK)[..., None] + key[..., None] * value[:, :, None, :]
    attended = jnp.einsum('bhk,bhkv->bhv', query, new_state, precision=lax.Precision.HIGHEST)
    normed = attended * lax.rsqrt(lax.optimization_barrier(jnp.mean(attended * attended, axis=2, keepdims=True)) + eps) * out_gain
    mixed = (normed.reshape(BATCH, VW) * jax.nn.silu(gate)).astype(jnp.bfloat16)
    attn_sum = group_sum(mixed, w_out, N_TP)
    middle = (wide + attn_sum).astype(jnp.bfloat16)
    wide2 = middle.astype(jnp.float32)
    scaled2 = (wide2 * mixer_gain.astype(jnp.float32)).astype(jnp.bfloat16)
    inv2 = lax.rsqrt(lax.optimization_barrier(jnp.mean(wide2 * wide2, axis=1, keepdims=True)) + eps)
    gate2 = jnp.dot(scaled2, w_ffgate, preferred_element_type=jnp.float32) * inv2
    upper = jnp.dot(scaled2, w_ffup, preferred_element_type=jnp.float32) * inv2
    hidden = (jax.nn.silu(gate2) * upper).astype(jnp.bfloat16)
    down_sum = group_sum(hidden, w_down, N_TP)
    result = (wide2 + down_sum).astype(jnp.bfloat16)
    return (result, new_state)
```

```python
import functools

import jax
import jax.numpy as jnp
from jax import lax
from jax.experimental import pallas as pl
from jax.experimental.pallas import tpu as pltpu
from jax.sharding import PartitionSpec as P

MESH = pl.DeviceIdType.MESH
F32 = jnp.float32
BF16 = jnp.bfloat16

D = 2048
DK = 128
DV = 256
EPS = 1e-06
GATE_NORM = 16.0

NX, NY, NZ = 4, 4, 8
NT = 2 * NY
COPIES = 96


def sigmoid(value):
    return 1.0 / (1.0 + jnp.exp(-value))


def halves(low, high):
    return jnp.concatenate([low, high], axis=1)


def as_pair(total):
    high = jnp.broadcast_to(total, (total.shape[0], 128)).astype(BF16).astype(F32)
    low = jnp.broadcast_to(total, (total.shape[0], 128)) - high
    lane = lax.broadcasted_iota(jnp.int32, high.shape, 1)
    return jnp.where(lane < 64, high, low).astype(BF16)


def of_pair(pair):
    return pair[:, 0:1] + pair[:, 64:65]


def packed_products(left, right, lane):
    width = left.shape[1] // 2
    stacked = jnp.concatenate([left[:, :width], left[:, width:]], axis=0)
    total = jnp.dot(stacked, right, preferred_element_type=F32)
    blocks = []
    for j in range(8):
        first = total[0:64, 128 * j : 128 * j + 128]
        second = total[64:128, 128 * j : 128 * j + 128]
        top = first[0:32] + pltpu.roll(second[0:32], 64, 1)
        bottom = pltpu.roll(first[32:64], 64, 1) + second[32:64]
        blocks.append(jnp.where(lane < 64, top, bottom))
    return blocks


def kernel(
    tokens,
    norm_gain,
    w_query,
    w_key,
    w_value,
    w_gate,
    w_decay,
    log_decay,
    state_hbm,
    out_gain,
    w_out,
    mixer_gain,
    w_ffgate,
    w_ffup,
    w_down,
    result,
    state_out,
    state,
    new_state,
    att,
    w_own,
    x_all,
    w_all,
    w_diag,
    part1,
    got1,
    sum1,
    proj,
    mix,
    w_mix,
    part2,
    got2,
    attn_own,
    attn_all,
    tok_own,
    tok_all,
    middle,
    ff_own,
    ff_all,
    part3,
    got3,
    hid,
    part4,
    got4,
    res_own,
    res_all,
    send_sems,
    recv_sems,
    local_sems,
):
    kv = lax.axis_index("kv")
    t = lax.axis_index("tp")
    z, x = lax.div(kv, NX), lax.rem(kv, NX)
    y, core = lax.div(t, 2), lax.rem(t, 2)

    def at_x(d):
        return lax.rem(x + d, NX)

    def at_z(d):
        return lax.rem(z + d, NZ)

    def at_t(d):
        return lax.rem(t + d, NT)

    sent = []
    counter = [0]

    def new_sem(count=1):
        first = counter[0]
        counter[0] += count
        return first

    def send(src, dst, peer, sem=None, recv=None):
        sem = new_sem() if sem is None else sem
        copy = pltpu.make_async_remote_copy(
            src_ref=src,
            dst_ref=dst,
            send_sem=send_sems.at[sem],
            recv_sem=recv_sems.at[sem if recv is None else recv],
            device_id=peer,
            device_id_type=MESH,
        )
        return copy

    def go(copies):
        for copy in copies:
            copy.start()
        sent.extend(copies)
        return copies

    def arrive(copies):
        for copy in copies:
            copy.wait_recv()

    barrier = pltpu.get_barrier_semaphore()

    def greet(peer):
        pl.semaphore_signal(barrier, inc=1, device_id=peer, device_id_type=MESH)

    for d in range(1, NX):
        greet((z * NX + at_x(d), t))
    for d in range(1, NT):
        greet((kv, at_t(d)))
    for d in range(1, NZ):
        greet((at_z(d) * NX + x, t))
        greet((at_z(d) * NX + x, z))

    @pl.when(t != z)
    def _():
        greet((kv, z))

    state_in = pltpu.make_async_copy(state_hbm, state, local_sems.at[0])
    state_in.start()

    square = (64, 64)
    row = lax.broadcasted_iota(jnp.int32, square, 0)
    column = lax.broadcasted_iota(jnp.int32, square, 1)
    gain = jnp.sum(
        jnp.where(row == column, jnp.broadcast_to(norm_gain[...].astype(F32), square), 0.0),
        axis=1,
        keepdims=True,
    )

    def gained(weight):
        return (weight[...].astype(F32) * gain).astype(BF16)

    w_own[0, :, 0:128] = gained(w_query)
    w_own[0, :, 128:256] = gained(w_key)
    w_own[1] = gained(w_value)
    w_own[2] = gained(w_gate)
    w_own[3, :, 0:128] = gained(w_decay)
    w_own[3, :, 128:256] = jnp.zeros((64, 128), BF16)
    x_all[x] = halves(tokens[0:256, :], tokens[256:512, :])
    w_all[x] = w_own[x]

    greetings = (NX - 1) + (NT - 1) + 2 * (NZ - 1)
    pl.semaphore_wait(barrier, greetings + jnp.where(t != z, 1, 0))

    ring_x = [(d, (z * NX + at_x(d), t)) for d in range(1, NX)]
    ring_z = [(d, (at_z(d) * NX + x, t)) for d in range(1, NZ)]
    ring_t = [(d, (kv, at_t(d))) for d in range(1, NT)]
    gather1 = go([send(w_own.at[at_x(d)], w_all.at[x], peer) for d, peer in ring_x])
    gather1 += go([send(x_all.at[x], x_all.at[x], peer) for d, peer in ring_x])

    gains = mixer_gain[...].astype(F32)
    units = halves(
        jnp.transpose(w_ffgate[...].astype(F32), (1, 0)) * gains,
        jnp.transpose(w_ffup[...].astype(F32), (1, 0)) * gains,
    ).astype(BF16)
    for j in range(NZ):
        low, high = slice(96 * j, 96 * j + 48), slice(96 * j + 48, 96 * j + 96)
        ff_own[j, 0] = units[low]
        ff_own[j, 1] = units[high]
        ff_own[j, 2] = halves(w_down[low, :], w_down[high, :])
    lanes_z = pl.ds(pl.multiple_of(z * 128, 128), 128)
    ff_all[:, t, :, lanes_z] = ff_own[z]
    ff_blocks = go(
        [send(ff_own.at[at_z(d)], ff_all.at[:, t, :, lanes_z], peer) for d, peer in ring_z]
    )
    w_mix[:, lanes_z] = halves(w_out[0:128, :], w_out[128:256, :])
    tok_own[...] = halves(tokens[pl.ds(64 * t, 32), :], tokens[pl.ds(64 * t + 32, 32), :])
    tok_all[z] = tok_own[...]
    w_diag[...] = jnp.zeros(w_diag.shape, BF16)

    arrive(gather1)
    lane256 = lax.broadcasted_iota(jnp.int32, (256, 128), 1)
    total = jnp.zeros((256, 512), F32)
    top = jnp.zeros((256, 128), F32)
    bottom = jnp.zeros((256, 128), F32)
    for j in range(NX):
        w_diag[j, 0:64, 0:256] = w_all[j]
        w_diag[j, 64:128, 256:512] = w_all[j]
    for j in range(NX):
        block = x_all[j]
        total += jnp.dot(block, w_diag[j], preferred_element_type=F32)
        wide = block.astype(F32)
        wide = wide * wide
        top += jnp.where(lane256 < 64, wide, 0.0)
        bottom += jnp.where(lane256 < 64, 0.0, wide)
    has_sums = x == NX - 1
    for j in range(NZ):
        rows = slice(64 * (j % 4), 64 * (j % 4) + 64)
        first = 256 * (j // 4)
        part1[j, :, 0:128] = total[rows, first : first + 128].astype(BF16)
        squares = as_pair(jnp.sum((top if j < 4 else bottom)[rows], axis=1, keepdims=True))
        values = total[rows, first + 128 : first + 256]
        part1[j, :, 128:256] = jnp.where(has_sums, squares.astype(F32), values).astype(BF16)
    got1[z] = part1[z]
    scatter1 = go([send(part1.at[at_z(d)], got1.at[z], peer) for d, peer in ring_z])
    mix_blocks = go(
        [send(w_mix.at[:, lanes_z], w_mix.at[:, lanes_z], peer) for d, peer in ring_z]
    )
    tok_blocks = go([send(tok_own, tok_all.at[z], peer) for d, peer in ring_z])

    arrive(ff_blocks)
    partner = (kv, t + 1 - 2 * core)
    ff_y = go(
        [
            send(ff_all.at[:, t], ff_all.at[:, t], (kv, lax.rem(y + d, NY) * 2 + core))
            for d in range(1, NY)
        ]
    )
    ff_core = go([send(ff_all.at[:, t], ff_all.at[:, t], partner)])

    arrive(scatter1)
    total = got1[0].astype(F32)
    for j in range(1, NZ):
        total += got1[j].astype(F32)
    squares = as_pair(of_pair(total[:, 128:256]))
    for j in range(NX):
        rows = slice(16 * j, 16 * j + 16)
        sum1[j, :, 0:128] = total[rows, 0:128].astype(BF16)
        sum1[j, :, 128:256] = jnp.where(
            has_sums, squares[rows].astype(F32), total[rows, 128:256]
        ).astype(BF16)
    proj[x] = sum1[x]
    exchange1 = go([send(sum1.at[at_x(d)], proj.at[x], peer) for d, peer in ring_x])
    state_in.wait()
    arrive(exchange1)

    inv = lax.rsqrt(of_pair(proj[3, :, 128:256].astype(F32)) / D + EPS)
    query = proj[0, :, 0:128].astype(F32) * (inv * DK ** (-0.5))
    keys = proj[0, :, 128:256].astype(F32) * inv
    values = proj[1].astype(F32) * inv
    gate = proj[2].astype(F32) * inv
    decay_pre = proj[3, :, 0:128].astype(F32) * inv
    log_sigmoid = jnp.minimum(decay_pre, 0.0) - jnp.log1p(jnp.exp(-jnp.abs(decay_pre)))
    decay = jnp.exp(log_sigmoid / GATE_NORM + log_decay[...])
    columns = jnp.transpose(
        jnp.concatenate([query, keys, decay, jnp.zeros((80, 128), F32)], axis=0), (1, 0)
    )
    for b in range(16):
        q_col = columns[:, b : b + 1]
        k_col = columns[:, 16 + b : 17 + b]
        a_col = columns[:, 32 + b : 33 + b]
        new = state[b] * a_col + k_col * values[b : b + 1, :]
        new_state[b] = new
        att[b : b + 1, :] = jnp.sum(new * q_col, axis=0, keepdims=True)
    attended = att[...]
    normed = (
        attended
        * lax.rsqrt(jnp.mean(attended * attended, axis=1, keepdims=True) + EPS)
        * out_gain[...]
    )
    mix[x] = (normed * (gate * sigmoid(gate))).astype(BF16)
    gather2 = go([send(mix.at[x], mix.at[x], peer) for d, peer in ring_x])
    state_back = pltpu.make_async_copy(new_state, state_out, local_sems.at[1])
    state_back.start()

    lane32 = lax.broadcasted_iota(jnp.int32, (32, 128), 1)
    arrive(mix_blocks)
    arrive(gather2)
    mixed = mix[...].reshape(64, DV)
    for j, block in enumerate(packed_products(mixed, w_mix[...], lane32)):
        part2[j] = block.astype(BF16)
    got2[t] = part2[t]
    scatter2 = go([send(part2.at[at_t(d)], got2.at[t], peer) for d, peer in ring_t])
    arrive(scatter2)
    total = got2[0].astype(F32)
    for j in range(1, NT):
        total += got2[j].astype(F32)
    attn_own[...] = total.astype(BF16)

    first_send, first_recv = new_sem(NT), 0
    first_recv = first_send
    spread = [
        send(
            attn_own,
            attn_all.at[t],
            (at_z(d) * NX + x, z),
            sem=first_send + d,
            recv=first_recv + t,
        )
        for d in range(NZ)
    ]
    diagonal = t == z

    @pl.when(diagonal)
    def _():
        attn_all[t] = attn_own[...]

    @pl.when(jnp.logical_not(diagonal))
    def _():
        spread[0].start()

    go(spread[1:])

    arrive(ff_y)
    for d in range(1, NY):
        other = lax.rem(y + d, NY) * 2 + core
        ff_core += go([send(ff_all.at[:, other], ff_all.at[:, other], partner)])

    arrive(tok_blocks)
    for j in range(NT):
        copy = pltpu.make_async_remote_copy(
            src_ref=attn_own,
            dst_ref=attn_all.at[j],
            send_sem=send_sems.at[first_send],
            recv_sem=recv_sems.at[first_recv + j],
            device_id=(kv, t),
            device_id_type=MESH,
        )

        @pl.when(jnp.logical_or(t != z, j != t))
        def _(copy=copy):
            copy.wait_recv()

    top = jnp.zeros((32, 128), F32)
    bottom = jnp.zeros((32, 128), F32)
    pieces = []
    for j in range(NZ):
        block = (tok_all[j].astype(F32) + attn_all[j].astype(F32)).astype(BF16)
        middle[j] = block
        wide = block.astype(F32)
        low = jnp.where(lane32 < 64, wide, 0.0)
        high = jnp.where(lane32 < 64, 0.0, wide)
        top += low * low
        bottom += high * high
        pieces.append(
            jnp.concatenate(
                [low, pltpu.roll(high, 64, 1), pltpu.roll(low, 64, 1), high], axis=0
            ).astype(BF16)
        )
    left = jnp.concatenate(pieces, axis=1)
    squares = as_pair(
        jnp.concatenate(
            [jnp.sum(top, axis=1, keepdims=True), jnp.sum(bottom, axis=1, keepdims=True)], axis=0
        )
    )
    arrive(ff_core)
    weights = ff_all[0:2].reshape(NT * 96, 1024)
    terms = lax.dot_general(
        left, weights, (((1,), (1,)), ((), ())), preferred_element_type=F32
    )
    for j in range(NX):
        rows = slice(16 * j, 16 * j + 16)
        part3[j, :, 0:768] = terms[rows].astype(BF16)
        part3[j, :, 768:1536] = terms[64 + 16 * j : 80 + 16 * j].astype(BF16)
        part3[j, :, 1536:1664] = squares[rows]
    got3[x] = part3[x]
    scatter3 = go([send(part3.at[at_x(d)], got3.at[x], peer) for d, peer in ring_x])
    arrive(scatter3)
    total = got3[0].astype(F32)
    for j in range(1, NX):
        total += got3[j].astype(F32)
    inv = lax.rsqrt(of_pair(total[:, 1536:1664]) / D + EPS)
    gate = total[:, 0:768] * inv
    hid[x] = (gate * sigmoid(gate) * (total[:, 768:1536] * inv)).astype(BF16)
    gather3 = go([send(hid.at[x], hid.at[x], peer) for d, peer in ring_x])
    arrive(gather3)

    hidden = hid[...].reshape(64, 768)
    weights = ff_all[2].reshape(NT * 48, 1024)
    for j, block in enumerate(packed_products(hidden, weights, lane32)):
        part4[j] = block.astype(BF16)
    got4[z] = part4[z]
    scatter4 = go([send(part4.at[at_z(d)], got4.at[z], peer) for d, peer in ring_z])
    arrive(scatter4)
    total = got4[0].astype(F32)
    for j in range(1, NZ):
        total += got4[j].astype(F32)
    res_own[...] = (middle[z].astype(F32) + total).astype(BF16)
    res_all[t] = res_own[...]
    gather4 = go([send(res_own, res_all.at[t], peer) for d, peer in ring_t])
    arrive(gather4)
    for j in range(NT):
        block = res_all[j]
        result[64 * j : 64 * j + 32, :] = block[:, 0:64]
        result[64 * j + 32 : 64 * j + 64, :] = block[:, 64:128]

    for copy in sent:
        copy.wait_send()

    @pl.when(jnp.logical_not(diagonal))
    def _():
        spread[0].wait_send()

    state_back.wait()


def body(
    tokens,
    norm_gain,
    w_query,
    w_key,
    w_value,
    w_gate,
    w_decay,
    log_decay,
    state,
    out_gain,
    w_out,
    mixer_gain,
    w_ffgate,
    w_ffup,
    w_down,
):
    vmem = pl.BlockSpec(memory_space=pltpu.VMEM)
    hbm = pl.BlockSpec(memory_space=pl.ANY)
    shape = state.shape
    result, new_state = pl.pallas_call(
        kernel,
        out_shape=(
            jax.ShapeDtypeStruct(tokens.shape, BF16),
            jax.ShapeDtypeStruct((shape[0], DK, DV), F32),
        ),
        in_specs=[vmem] * 8 + [hbm] + [vmem] * 6,
        out_specs=(vmem, hbm),
        scratch_shapes=[
            pltpu.VMEM((16, DK, DV), F32),
            pltpu.VMEM((16, DK, DV), F32),
            pltpu.VMEM((16, DV), F32),
            pltpu.VMEM((NX, 64, 256), BF16),
            pltpu.VMEM((NX, 256, 128), BF16),
            pltpu.VMEM((NX, 64, 256), BF16),
            pltpu.VMEM((NX, 128, 512), BF16),
            pltpu.VMEM((NZ, 64, 256), BF16),
            pltpu.VMEM((NZ, 64, 256), BF16),
            pltpu.VMEM((NX, 16, 256), BF16),
            pltpu.VMEM((NX, 16, 256), BF16),
            pltpu.VMEM((NX, 16, 256), BF16),
            pltpu.VMEM((128, 1024), BF16),
            pltpu.VMEM((NT, 32, 128), BF16),
            pltpu.VMEM((NT, 32, 128), BF16),
            pltpu.VMEM((32, 128), BF16),
            pltpu.VMEM((NT, 32, 128), BF16),
            pltpu.VMEM((32, 128), BF16),
            pltpu.VMEM((NZ, 32, 128), BF16),
            pltpu.VMEM((NZ, 32, 128), BF16),
            pltpu.VMEM((NZ, 3, 48, 128), BF16),
            pltpu.VMEM((3, NT, 48, 1024), BF16),
            pltpu.VMEM((NX, 16, 1664), BF16),
            pltpu.VMEM((NX, 16, 1664), BF16),
            pltpu.VMEM((NX, 16, 768), BF16),
            pltpu.VMEM((NZ, 32, 128), BF16),
            pltpu.VMEM((NZ, 32, 128), BF16),
            pltpu.VMEM((32, 128), BF16),
            pltpu.VMEM((NT, 32, 128), BF16),
            pltpu.SemaphoreType.DMA((COPIES,)),
            pltpu.SemaphoreType.DMA((COPIES,)),
            pltpu.SemaphoreType.DMA((2,)),
        ],
        compiler_params=pltpu.CompilerParams(
            collective_id=0, has_side_effects=True, vmem_limit_bytes=40 * 1024 * 1024
        ),
    )(
        tokens,
        norm_gain.reshape(1, 64),
        w_query,
        w_key,
        w_value,
        w_gate,
        w_decay,
        log_decay,
        state.reshape(shape[0], DK, DV),
        out_gain.reshape(1, DV),
        w_out,
        mixer_gain.reshape(1, 64),
        w_ffgate,
        w_ffup,
        w_down,
    )
    return (result, new_state.reshape(shape))


def solution(mesh):
    return jax.shard_map(
        body,
        mesh=mesh,
        in_specs=(
            P(None, "kv"),
            P("kv"),
            P("kv", "tp"),
            P("kv", "tp"),
            P("kv", "tp"),
            P("kv", "tp"),
            P("kv", "tp"),
            P("kv", "tp"),
            P("kv", "tp", None, None),
            P(),
            P("tp", "kv"),
            P("kv"),
            P("kv", "tp"),
            P("kv", "tp"),
            P("tp", "kv"),
        ),
        out_specs=(P(None, "kv"), P("kv", "tp", None, None)),
        check_vma=False,
    )
```

```python
import functools

import jax
import jax.numpy as jnp
from jax import lax
from jax.experimental import pallas as pl
from jax.experimental.pallas import tpu as pltpu
from jax.sharding import PartitionSpec as P

MESH = pl.DeviceIdType.MESH
F32 = jnp.float32
BF16 = jnp.bfloat16

D = 2048
DK = 128
DV = 256
EPS = 1e-06
GATE_NORM = 16.0

NX, NY, NZ = 4, 4, 8
NT = 2 * NY
COPIES = 96
STATE = 8
FIRST = [0, 1, 2, 3, 4, 5, 6]
LATER = [12, 13, 14, 10, 11, 7, 9, STATE]


def sigmoid(value):
    return 1.0 / (1.0 + jnp.exp(-value))


def halves(low, high):
    return jnp.concatenate([low, high], axis=1)


def as_pair(total):
    high = jnp.broadcast_to(total, (total.shape[0], 128)).astype(BF16).astype(F32)
    low = jnp.broadcast_to(total, (total.shape[0], 128)) - high
    lane = lax.broadcasted_iota(jnp.int32, high.shape, 1)
    return jnp.where(lane < 64, high, low).astype(BF16)


def of_pair(pair):
    return pair[:, 0:1] + pair[:, 64:65]


def packed_products(left, right, lane):
    width = left.shape[1] // 2
    stacked = jnp.concatenate([left[:, :width], left[:, width:]], axis=0)
    total = jnp.dot(stacked, right, preferred_element_type=F32)
    blocks = []
    for j in range(8):
        first = total[0:64, 128 * j : 128 * j + 128]
        second = total[64:128, 128 * j : 128 * j + 128]
        top = first[0:32] + pltpu.roll(second[0:32], 64, 1)
        bottom = pltpu.roll(first[32:64], 64, 1) + second[32:64]
        blocks.append(jnp.where(lane < 64, top, bottom))
    return blocks


def kernel(*refs):
    inputs, (res_out, state_out), refs = refs[:15], refs[15:17], refs[17:]
    held, refs = refs[:15], refs[15:]
    (
        tokens,
        norm_gain,
        w_query,
        w_key,
        w_value,
        w_gate,
        w_decay,
        log_decay,
        state,
        out_gain,
        w_out,
        mixer_gain,
        w_ffgate,
        w_ffup,
        w_down,
    ) = held
    (
        new_state,
        att,
        w_own,
        x_all,
        w_all,
        w_diag,
        part1,
        got1,
        sum1,
        proj,
        mix,
        w_mix,
        part2,
        got2,
        attn_own,
        attn_all,
        tok_own,
        tok_all,
        middle,
        ff_own,
        ff_all,
        part3,
        got3,
        hid,
        part4,
        got4,
        res_own,
        res_all,
        send_sems,
        recv_sems,
        local_sems,
    ) = refs
    kv = lax.axis_index("kv")
    t = lax.axis_index("tp")
    z, x = lax.div(kv, NX), lax.rem(kv, NX)
    y, core = lax.div(t, 2), lax.rem(t, 2)

    def at_x(d):
        return lax.rem(x + d, NX)

    def at_z(d):
        return lax.rem(z + d, NZ)

    def at_t(d):
        return lax.rem(t + d, NT)

    sent = []
    counter = [0]

    def new_sem(count=1):
        first = counter[0]
        counter[0] += count
        return first

    def send(src, dst, peer, sem=None, recv=None):
        sem = new_sem() if sem is None else sem
        copy = pltpu.make_async_remote_copy(
            src_ref=src,
            dst_ref=dst,
            send_sem=send_sems.at[sem],
            recv_sem=recv_sems.at[sem if recv is None else recv],
            device_id=peer,
            device_id_type=MESH,
        )
        return copy

    def go(copies):
        for copy in copies:
            copy.start()
        sent.extend(copies)
        return copies

    def arrive(copies):
        for copy in copies:
            copy.wait_recv()

    barrier = pltpu.get_barrier_semaphore()

    def greet(peer):
        pl.semaphore_signal(barrier, inc=1, device_id=peer, device_id_type=MESH)

    for d in range(1, NX):
        greet((z * NX + at_x(d), t))
    for d in range(1, NT):
        greet((kv, at_t(d)))
    for d in range(1, NZ):
        greet((at_z(d) * NX + x, t))
        greet((at_z(d) * NX + x, z))

    @pl.when(t != z)
    def _():
        greet((kv, z))

    loads = [
        pltpu.make_async_copy(src, dst, local_sems.at[i])
        for i, (src, dst) in enumerate(zip(inputs, held))
    ]
    for i in FIRST + LATER:
        loads[i].start()

    def load(*numbers):
        for i in numbers:
            loads[i].wait()

    with jax.named_scope("wait_first"):
        load(*FIRST)
    square = (64, 64)
    row = lax.broadcasted_iota(jnp.int32, square, 0)
    column = lax.broadcasted_iota(jnp.int32, square, 1)
    gain = jnp.sum(
        jnp.where(row == column, jnp.broadcast_to(norm_gain[...].astype(F32), square), 0.0),
        axis=1,
        keepdims=True,
    )

    def gained(weight):
        return (weight[...].astype(F32) * gain).astype(BF16)

    w_own[0, :, 0:128] = gained(w_query)
    w_own[0, :, 128:256] = gained(w_key)
    w_own[1] = gained(w_value)
    w_own[2] = gained(w_gate)
    w_own[3, :, 0:128] = gained(w_decay)
    w_own[3, :, 128:256] = jnp.zeros((64, 128), BF16)
    own = jnp.concatenate([tokens[:, 0:256], tokens[:, 256:512]], axis=0).astype(F32)
    x_all[x] = jnp.transpose(own, (1, 0)).astype(BF16)
    w_all[x] = w_own[x]

    greetings = (NX - 1) + (NT - 1) + 2 * (NZ - 1)
    with jax.named_scope("wait_barrier"):
        pl.semaphore_wait(barrier, greetings + jnp.where(t != z, 1, 0))

    ring_x = [(d, (z * NX + at_x(d), t)) for d in range(1, NX)]
    ring_z = [(d, (at_z(d) * NX + x, t)) for d in range(1, NZ)]
    ring_t = [(d, (kv, at_t(d))) for d in range(1, NT)]
    gather1 = go([send(w_own.at[at_x(d)], w_all.at[x], peer) for d, peer in ring_x])
    gather1 += go([send(x_all.at[x], x_all.at[x], peer) for d, peer in ring_x])

    with jax.named_scope("wait_later"):
        load(*[i for i in LATER if i != STATE])
    gains = mixer_gain[...].astype(F32)
    units = jnp.transpose(
        jnp.concatenate([w_ffgate[...], w_ffup[...]], axis=0).astype(F32), (1, 0)
    )
    units = (units * jnp.concatenate([gains, gains], axis=1)).astype(BF16)
    down = w_down[...].astype(F32)
    down = jnp.concatenate([down, pltpu.roll(down, 768 - 48, 1)], axis=0)
    down = jnp.transpose(down, (1, 0)).astype(BF16)
    for j in range(NZ):
        low, high = slice(96 * j, 96 * j + 48), slice(96 * j + 48, 96 * j + 96)
        ff_own[j, 0] = units[low]
        ff_own[j, 1] = units[high]
        ff_own[j, 2] = down[low]
    lanes_z = pl.ds(pl.multiple_of(z * 128, 128), 128)
    ff_all[:, t, :, lanes_z] = ff_own[z]
    ff_blocks = go(
        [send(ff_own.at[at_z(d)], ff_all.at[:, t, :, lanes_z], peer) for d, peer in ring_z]
    )
    out_rows = jnp.concatenate([w_out[:, 0:128], w_out[:, 128:256]], axis=0).astype(F32)
    w_mix[:, lanes_z] = jnp.transpose(out_rows, (1, 0)).astype(BF16)
    lane32 = lax.broadcasted_iota(jnp.int32, (32, 128), 1)
    rows = pl.multiple_of(64 * lax.rem(t, 4), 64)
    own = x_all[x, pl.ds(rows, 64), :].astype(F32)
    own = jnp.where(t < 4, own, pltpu.roll(own, 64, 1))
    tok_own[...] = jnp.where(lane32 < 64, own[0:32], pltpu.roll(own[32:64], 64, 1)).astype(BF16)
    tok_all[z] = tok_own[...]
    w_diag[...] = jnp.zeros(w_diag.shape, BF16)

    with jax.named_scope("wait_gather1"):
        arrive(gather1)
    lane256 = lax.broadcasted_iota(jnp.int32, (256, 128), 1)
    total = jnp.zeros((256, 512), F32)
    top = jnp.zeros((256, 128), F32)
    bottom = jnp.zeros((256, 128), F32)
    for j in range(NX):
        w_diag[j, 0:64, 0:256] = w_all[j]
        w_diag[j, 64:128, 256:512] = w_all[j]
    for j in range(NX):
        block = x_all[j]
        total += jnp.dot(block, w_diag[j], preferred_element_type=F32)
        wide = block.astype(F32)
        wide = wide * wide
        top += jnp.where(lane256 < 64, wide, 0.0)
        bottom += jnp.where(lane256 < 64, 0.0, wide)
    has_sums = x == NX - 1
    for j in range(NZ):
        rows = slice(64 * (j % 4), 64 * (j % 4) + 64)
        first = 256 * (j // 4)
        part1[j, :, 0:128] = total[rows, first : first + 128].astype(BF16)
        squares = as_pair(jnp.sum((top if j < 4 else bottom)[rows], axis=1, keepdims=True))
        values = total[rows, first + 128 : first + 256]
        part1[j, :, 128:256] = jnp.where(has_sums, squares.astype(F32), values).astype(BF16)
    got1[z] = part1[z]
    scatter1 = go([send(part1.at[at_z(d)], got1.at[z], peer) for d, peer in ring_z])
    mix_blocks = go(
        [send(w_mix.at[:, lanes_z], w_mix.at[:, lanes_z], peer) for d, peer in ring_z]
    )
    tok_blocks = go([send(tok_own, tok_all.at[z], peer) for d, peer in ring_z])

    with jax.named_scope("wait_ff_blocks"):
        arrive(ff_blocks)
    partner = (kv, t + 1 - 2 * core)
    ff_y = go(
        [
            send(ff_all.at[:, t], ff_all.at[:, t], (kv, lax.rem(y + d, NY) * 2 + core))
            for d in range(1, NY)
        ]
    )
    ff_core = go([send(ff_all.at[:, t], ff_all.at[:, t], partner)])

    with jax.named_scope("wait_scatter1"):
        arrive(scatter1)
    total = got1[0].astype(F32)
    for j in range(1, NZ):
        total += got1[j].astype(F32)
    squares = as_pair(of_pair(total[:, 128:256]))
    for j in range(NX):
        rows = slice(16 * j, 16 * j + 16)
        sum1[j, :, 0:128] = total[rows, 0:128].astype(BF16)
        sum1[j, :, 128:256] = jnp.where(
            has_sums, squares[rows].astype(F32), total[rows, 128:256]
        ).astype(BF16)
    proj[x] = sum1[x]
    exchange1 = go([send(sum1.at[at_x(d)], proj.at[x], peer) for d, peer in ring_x])
    load(STATE)
    with jax.named_scope("wait_exchange1"):
        arrive(exchange1)

    inv = lax.rsqrt(of_pair(proj[3, :, 128:256].astype(F32)) / D + EPS)
    query = proj[0, :, 0:128].astype(F32) * (inv * DK ** (-0.5))
    keys = proj[0, :, 128:256].astype(F32) * inv
    values = proj[1].astype(F32) * inv
    gate = proj[2].astype(F32) * inv
    decay_pre = proj[3, :, 0:128].astype(F32) * inv
    log_sigmoid = jnp.minimum(decay_pre, 0.0) - jnp.log1p(jnp.exp(-jnp.abs(decay_pre)))
    decay = jnp.exp(log_sigmoid / GATE_NORM + log_decay[...])
    columns = jnp.transpose(
        jnp.concatenate([query, keys, decay, jnp.zeros((80, 128), F32)], axis=0), (1, 0)
    )
    for b in range(16):
        q_col = columns[:, b : b + 1]
        k_col = columns[:, 16 + b : 17 + b]
        a_col = columns[:, 32 + b : 33 + b]
        new = state[b] * a_col + k_col * values[b : b + 1, :]
        new_state[b] = new
        att[b : b + 1, :] = jnp.sum(new * q_col, axis=0, keepdims=True)
    attended = att[...]
    normed = (
        attended
        * lax.rsqrt(jnp.mean(attended * attended, axis=1, keepdims=True) + EPS)
        * out_gain[...]
    )
    mix[x] = (normed * (gate * sigmoid(gate))).astype(BF16)
    gather2 = go([send(mix.at[x], mix.at[x], peer) for d, peer in ring_x])
    state_back = pltpu.make_async_copy(new_state, state_out, local_sems.at[15])
    state_back.start()

    with jax.named_scope("wait_mix_blocks"):
        arrive(mix_blocks)
    with jax.named_scope("wait_gather2"):
        arrive(gather2)
    mixed = mix[...].reshape(64, DV)
    for j, block in enumerate(packed_products(mixed, w_mix[...], lane32)):
        part2[j] = block.astype(BF16)
    got2[t] = part2[t]
    scatter2 = go([send(part2.at[at_t(d)], got2.at[t], peer) for d, peer in ring_t])
    with jax.named_scope("wait_scatter2"):
        arrive(scatter2)
    total = got2[0].astype(F32)
    for j in range(1, NT):
        total += got2[j].astype(F32)
    attn_own[...] = total.astype(BF16)

    first_send, first_recv = new_sem(NT), 0
    first_recv = first_send
    spread = [
        send(
            attn_own,
            attn_all.at[t],
            (at_z(d) * NX + x, z),
            sem=first_send + d,
            recv=first_recv + t,
        )
        for d in range(NZ)
    ]
    diagonal = t == z

    @pl.when(diagonal)
    def _():
        attn_all[t] = attn_own[...]

    @pl.when(jnp.logical_not(diagonal))
    def _():
        spread[0].start()

    go(spread[1:])

    with jax.named_scope("wait_ff_y"):
        arrive(ff_y)
    for d in range(1, NY):
        other = lax.rem(y + d, NY) * 2 + core
        ff_core += go([send(ff_all.at[:, other], ff_all.at[:, other], partner)])

    with jax.named_scope("wait_tok_blocks"):
        arrive(tok_blocks)
    def wait_spread(j):
        copy = pltpu.make_async_remote_copy(
            src_ref=attn_own,
            dst_ref=attn_all.at[j],
            send_sem=send_sems.at[first_send],
            recv_sem=recv_sems.at[first_recv + j],
            device_id=(kv, t),
            device_id_type=MESH,
        )

        @pl.when(jnp.logical_or(t != z, j != t))
        def _(copy=copy):
            copy.wait_recv()

    with jax.named_scope("wait_spread"):
        for j in range(NT):
            wait_spread(j)

    top = jnp.zeros((32, 128), F32)
    bottom = jnp.zeros((32, 128), F32)
    pieces = []
    for j in range(NZ):
        block = (tok_all[j].astype(F32) + attn_all[j].astype(F32)).astype(BF16)
        middle[j] = block
        wide = block.astype(F32)
        low = jnp.where(lane32 < 64, wide, 0.0)
        high = jnp.where(lane32 < 64, 0.0, wide)
        top += low * low
        bottom += high * high
        pieces.append(
            jnp.concatenate(
                [low, pltpu.roll(high, 64, 1), pltpu.roll(low, 64, 1), high], axis=0
            ).astype(BF16)
        )
    left = jnp.concatenate(pieces, axis=1)
    squares = as_pair(
        jnp.concatenate(
            [jnp.sum(top, axis=1, keepdims=True), jnp.sum(bottom, axis=1, keepdims=True)], axis=0
        )
    )
    with jax.named_scope("wait_ff_core"):
        arrive(ff_core)
    weights = ff_all[0:2].reshape(NT * 96, 1024)
    terms = lax.dot_general(
        left, weights, (((1,), (1,)), ((), ())), preferred_element_type=F32
    )
    for j in range(NX):
        rows = slice(16 * j, 16 * j + 16)
        part3[j, :, 0:768] = terms[rows].astype(BF16)
        part3[j, :, 768:1536] = terms[64 + 16 * j : 80 + 16 * j].astype(BF16)
        part3[j, :, 1536:1664] = squares[rows]
    got3[x] = part3[x]
    scatter3 = go([send(part3.at[at_x(d)], got3.at[x], peer) for d, peer in ring_x])
    with jax.named_scope("wait_scatter3"):
        arrive(scatter3)
    total = got3[0].astype(F32)
    for j in range(1, NX):
        total += got3[j].astype(F32)
    inv = lax.rsqrt(of_pair(total[:, 1536:1664]) / D + EPS)
    gate = total[:, 0:768] * inv
    hid[x] = (gate * sigmoid(gate) * (total[:, 768:1536] * inv)).astype(BF16)
    gather3 = go([send(hid.at[x], hid.at[x], peer) for d, peer in ring_x])
    with jax.named_scope("wait_gather3"):
        arrive(gather3)

    hidden = hid[...].reshape(64, 768)
    weights = ff_all[2].reshape(NT * 48, 1024)
    for j, block in enumerate(packed_products(hidden, weights, lane32)):
        part4[j] = block.astype(BF16)
    got4[z] = part4[z]
    scatter4 = go([send(part4.at[at_z(d)], got4.at[z], peer) for d, peer in ring_z])
    with jax.named_scope("wait_scatter4"):
        arrive(scatter4)
    total = got4[0].astype(F32)
    for j in range(1, NZ):
        total += got4[j].astype(F32)
    res_own[...] = (middle[z].astype(F32) + total).astype(BF16)
    res_all[t] = res_own[...]
    gather4 = go([send(res_own, res_all.at[t], peer) for d, peer in ring_t])
    with jax.named_scope("wait_gather4"):
        arrive(gather4)
    res_back = pltpu.make_async_copy(res_all, res_out, local_sems.at[16])
    res_back.start()
    for copy in sent:
        copy.wait_send()

    @pl.when(jnp.logical_not(diagonal))
    def _():
        spread[0].wait_send()

    state_back.wait()
    res_back.wait()


def finish(res_all, state_in, result, state_out):
    rows = []
    for j in range(NT):
        block = res_all[j].astype(F32)
        rows += [block, pltpu.roll(block, 64, 1)]
    rows = jnp.concatenate(rows, axis=0)
    result[...] = jnp.transpose(rows, (1, 0))[0:64].astype(BF16)


def body(
    tokens,
    norm_gain,
    w_query,
    w_key,
    w_value,
    w_gate,
    w_decay,
    log_decay,
    state,
    out_gain,
    w_out,
    mixer_gain,
    w_ffgate,
    w_ffup,
    w_down,
):
    vmem = pl.BlockSpec(memory_space=pltpu.VMEM)
    hbm = pl.BlockSpec(memory_space=pltpu.HBM)
    shape = state.shape
    arguments = (
        tokens.T,
        norm_gain.reshape(1, 64),
        w_query,
        w_key,
        w_value,
        w_gate,
        w_decay,
        log_decay,
        state.reshape(shape[0], DK, DV),
        out_gain.reshape(1, DV),
        w_out.T,
        mixer_gain.reshape(1, 64),
        w_ffgate,
        w_ffup,
        w_down.T,
    )
    blocks, new_state = pl.pallas_call(
        kernel,
        out_shape=(
            jax.ShapeDtypeStruct((NT, 32, 128), BF16),
            jax.ShapeDtypeStruct((shape[0], DK, DV), F32),
        ),
        in_specs=[hbm] * 15,
        out_specs=(hbm, hbm),
        scratch_shapes=[pltpu.VMEM(value.shape, value.dtype) for value in arguments]
        + [
            pltpu.VMEM((16, DK, DV), F32),
            pltpu.VMEM((16, DV), F32),
            pltpu.VMEM((NX, 64, 256), BF16),
            pltpu.VMEM((NX, 256, 128), BF16),
            pltpu.VMEM((NX, 64, 256), BF16),
            pltpu.VMEM((NX, 128, 512), BF16),
            pltpu.VMEM((NZ, 64, 256), BF16),
            pltpu.VMEM((NZ, 64, 256), BF16),
            pltpu.VMEM((NX, 16, 256), BF16),
            pltpu.VMEM((NX, 16, 256), BF16),
            pltpu.VMEM((NX, 16, 256), BF16),
            pltpu.VMEM((128, 1024), BF16),
            pltpu.VMEM((NT, 32, 128), BF16),
            pltpu.VMEM((NT, 32, 128), BF16),
            pltpu.VMEM((32, 128), BF16),
            pltpu.VMEM((NT, 32, 128), BF16),
            pltpu.VMEM((32, 128), BF16),
            pltpu.VMEM((NZ, 32, 128), BF16),
            pltpu.VMEM((NZ, 32, 128), BF16),
            pltpu.VMEM((NZ, 3, 48, 128), BF16),
            pltpu.VMEM((3, NT, 48, 1024), BF16),
            pltpu.VMEM((NX, 16, 1664), BF16),
            pltpu.VMEM((NX, 16, 1664), BF16),
            pltpu.VMEM((NX, 16, 768), BF16),
            pltpu.VMEM((NZ, 32, 128), BF16),
            pltpu.VMEM((NZ, 32, 128), BF16),
            pltpu.VMEM((32, 128), BF16),
            pltpu.VMEM((NT, 32, 128), BF16),
            pltpu.SemaphoreType.DMA((COPIES,)),
            pltpu.SemaphoreType.DMA((COPIES,)),
            pltpu.SemaphoreType.DMA((17,)),
        ],
        compiler_params=pltpu.CompilerParams(
            collective_id=0, has_side_effects=True, vmem_limit_bytes=67043328
        ),
    )(*arguments)
    result, new_state = pl.pallas_call(
        finish,
        out_shape=(
            jax.ShapeDtypeStruct((64, 512), BF16),
            jax.ShapeDtypeStruct((shape[0], DK, DV), F32),
        ),
        in_specs=[vmem, hbm],
        out_specs=(vmem, hbm),
        input_output_aliases={1: 1},
    )(blocks, new_state)
    return (result.T, new_state.reshape(shape))


def solution(mesh):
    return jax.shard_map(
        body,
        mesh=mesh,
        in_specs=(
            P(None, "kv"),
            P("kv"),
            P("kv", "tp"),
            P("kv", "tp"),
            P("kv", "tp"),
            P("kv", "tp"),
            P("kv", "tp"),
            P("kv", "tp"),
            P("kv", "tp", None, None),
            P(),
            P("tp", "kv"),
            P("kv"),
            P("kv", "tp"),
            P("kv", "tp"),
            P("tp", "kv"),
        ),
        out_specs=(P(None, "kv"), P("kv", "tp", None, None)),
        check_vma=False,
    )
```

```python
import functools

import jax
import jax.numpy as jnp
from jax import lax
from jax.experimental import pallas as pl
from jax.experimental.pallas import tpu as pltpu
from jax.sharding import PartitionSpec as P

MESH = pl.DeviceIdType.MESH
F32 = jnp.float32
BF16 = jnp.bfloat16

D = 2048
DK = 128
DV = 256
EPS = 1e-06
GATE_NORM = 16.0

NX, NY, NZ = 4, 4, 8
NT = 2 * NY
COPIES = 136
STATE = 8
FAR_X = [2, 1, 3]
FAR_Z = [4, 3, 5, 2, 6, 1, 7]
FAR_T = [4, 5, 2, 3, 6, 7, 1]
PLANE = [(dz, dx) for dz in FAR_Z + [0] for dx in FAR_X + [0] if (dz, dx) != (0, 0)]
FIRST = [0, 1, 2, 3, 4, 5, 6]
LATER = [12, 13, 14, 10, 11, 7, 9, STATE]


def sigmoid(value):
    return 1.0 / (1.0 + jnp.exp(-value))


def halves(low, high):
    return jnp.concatenate([low, high], axis=1)


def as_pair(total):
    high = jnp.broadcast_to(total, (total.shape[0], 128)).astype(BF16).astype(F32)
    low = jnp.broadcast_to(total, (total.shape[0], 128)) - high
    lane = lax.broadcasted_iota(jnp.int32, high.shape, 1)
    return jnp.where(lane < 64, high, low).astype(BF16)


def of_pair(pair):
    return pair[:, 0:1] + pair[:, 64:65]


def packed_products(left, right, lane):
    width = left.shape[1] // 2
    stacked = jnp.concatenate([left[:, :width], left[:, width:]], axis=0)
    total = jnp.dot(stacked, right, preferred_element_type=F32)
    blocks = []
    for j in range(8):
        first = total[0:64, 128 * j : 128 * j + 128]
        second = total[64:128, 128 * j : 128 * j + 128]
        top = first[0:32] + pltpu.roll(second[0:32], 64, 1)
        bottom = pltpu.roll(first[32:64], 64, 1) + second[32:64]
        blocks.append(jnp.where(lane < 64, top, bottom))
    return blocks


def kernel(*refs):
    inputs, (res_out, state_out), refs = refs[:15], refs[15:17], refs[17:]
    held, refs = refs[:15], refs[15:]
    (
        tokens,
        norm_gain,
        w_query,
        w_key,
        w_value,
        w_gate,
        w_decay,
        log_decay,
        state,
        out_gain,
        w_out,
        mixer_gain,
        w_ffgate,
        w_ffup,
        w_down,
    ) = held
    (
        new_state,
        att,
        w_own,
        x_all,
        w_all,
        w_diag,
        part1,
        got1,
        mix,
        w_mix,
        part2,
        got2,
        attn_own,
        attn_all,
        tok_own,
        tok_all,
        middle,
        ff_own,
        ff_all,
        part3,
        got3,
        hid,
        part4,
        got4,
        res_own,
        res_all,
        send_sems,
        recv_sems,
        local_sems,
    ) = refs
    kv = lax.axis_index("kv")
    t = lax.axis_index("tp")
    z, x = lax.div(kv, NX), lax.rem(kv, NX)
    y, core = lax.div(t, 2), lax.rem(t, 2)

    def at_x(d):
        return lax.rem(x + d, NX)

    def at_z(d):
        return lax.rem(z + d, NZ)

    def at_t(d):
        return lax.rem(t + d, NT)

    sent = []
    counter = [0]

    def new_sem(count=1):
        first = counter[0]
        counter[0] += count
        return first

    def send(src, dst, peer, sem=None, recv=None):
        sem = new_sem() if sem is None else sem
        copy = pltpu.make_async_remote_copy(
            src_ref=src,
            dst_ref=dst,
            send_sem=send_sems.at[sem],
            recv_sem=recv_sems.at[sem if recv is None else recv],
            device_id=peer,
            device_id_type=MESH,
        )
        return copy

    def go(copies):
        for copy in copies:
            copy.start()
        sent.extend(copies)
        return copies

    def arrive(copies):
        for copy in copies:
            copy.wait_recv()

    barrier = pltpu.get_barrier_semaphore()

    def greet(peer):
        pl.semaphore_signal(barrier, inc=1, device_id=peer, device_id_type=MESH)

    for dz, dx in PLANE:
        greet((at_z(dz) * NX + at_x(dx), t))
    for d in FAR_T:
        greet((kv, at_t(d)))
    for d in FAR_Z:
        greet((at_z(d) * NX + x, z))

    @pl.when(t != z)
    def _():
        greet((kv, z))

    loads = [
        pltpu.make_async_copy(src, dst, local_sems.at[i])
        for i, (src, dst) in enumerate(zip(inputs, held))
    ]
    for i in FIRST + LATER:
        loads[i].start()

    def load(*numbers):
        for i in numbers:
            loads[i].wait()

    with jax.named_scope("wait_first"):
        load(*FIRST)
    square = (64, 64)
    row = lax.broadcasted_iota(jnp.int32, square, 0)
    column = lax.broadcasted_iota(jnp.int32, square, 1)
    gain = jnp.sum(
        jnp.where(row == column, jnp.broadcast_to(norm_gain[...].astype(F32), square), 0.0),
        axis=1,
        keepdims=True,
    )

    def gained(weight):
        return (weight[...].astype(F32) * gain).astype(BF16)

    w_own[0, :, 0:128] = gained(w_query)
    w_own[0, :, 128:256] = gained(w_key)
    w_own[1] = gained(w_value)
    w_own[2] = gained(w_gate)
    w_own[3, :, 0:128] = gained(w_decay)
    w_own[3, :, 128:256] = jnp.zeros((64, 128), BF16)
    own = jnp.concatenate([tokens[:, 0:256], tokens[:, 256:512]], axis=0).astype(F32)
    x_all[x] = jnp.transpose(own, (1, 0)).astype(BF16)
    w_all[x] = w_own[x]

    greetings = len(PLANE) + len(FAR_T) + len(FAR_Z)
    with jax.named_scope("wait_barrier"):
        pl.semaphore_wait(barrier, greetings + jnp.where(t != z, 1, 0))

    ring_x = [(d, (z * NX + at_x(d), t)) for d in FAR_X]
    ring_z = [(d, (at_z(d) * NX + x, t)) for d in FAR_Z]
    ring_t = [(d, (kv, at_t(d))) for d in FAR_T]
    gather1 = go([send(w_own.at[at_x(d)], w_all.at[x], peer) for d, peer in ring_x])
    gather1 += go([send(x_all.at[x], x_all.at[x], peer) for d, peer in ring_x])

    with jax.named_scope("wait_later"):
        load(*[i for i in LATER if i != STATE])
    gains = mixer_gain[...].astype(F32)
    units = jnp.transpose(
        jnp.concatenate([w_ffgate[...], w_ffup[...]], axis=0).astype(F32), (1, 0)
    )
    units = (units * jnp.concatenate([gains, gains], axis=1)).astype(BF16)
    down = w_down[...].astype(F32)
    down = jnp.concatenate([down, pltpu.roll(down, 768 - 48, 1)], axis=0)
    down = jnp.transpose(down, (1, 0)).astype(BF16)
    for j in range(NZ):
        low, high = slice(96 * j, 96 * j + 48), slice(96 * j + 48, 96 * j + 96)
        ff_own[j, 0] = units[low]
        ff_own[j, 1] = units[high]
        ff_own[j, 2] = down[low]
    lanes_z = pl.ds(pl.multiple_of(z * 128, 128), 128)
    ff_all[:, t, :, lanes_z] = ff_own[z]
    ff_blocks = go(
        [send(ff_own.at[at_z(d)], ff_all.at[:, t, :, lanes_z], peer) for d, peer in ring_z]
    )
    out_rows = jnp.concatenate([w_out[:, 0:128], w_out[:, 128:256]], axis=0).astype(F32)
    w_mix[:, lanes_z] = jnp.transpose(out_rows, (1, 0)).astype(BF16)
    lane32 = lax.broadcasted_iota(jnp.int32, (32, 128), 1)
    rows = pl.multiple_of(64 * lax.rem(t, 4), 64)
    own = x_all[x, pl.ds(rows, 64), :].astype(F32)
    own = jnp.where(t < 4, own, pltpu.roll(own, 64, 1))
    tok_own[...] = jnp.where(lane32 < 64, own[0:32], pltpu.roll(own[32:64], 64, 1)).astype(BF16)
    tok_all[z] = tok_own[...]
    tok_blocks = go([send(tok_own, tok_all.at[z], peer) for d, peer in ring_z])
    w_diag[...] = jnp.zeros(w_diag.shape, BF16)

    with jax.named_scope("wait_gather1"):
        arrive(gather1)
    lane256 = lax.broadcasted_iota(jnp.int32, (256, 128), 1)
    total = jnp.zeros((256, 512), F32)
    top = jnp.zeros((256, 128), F32)
    bottom = jnp.zeros((256, 128), F32)
    for j in range(NX):
        w_diag[j, 0:64, 0:256] = w_all[j]
        w_diag[j, 64:128, 256:512] = w_all[j]
    for j in range(NX):
        block = x_all[j]
        total += jnp.dot(block, w_diag[j], preferred_element_type=F32)
        wide = block.astype(F32)
        wide = wide * wide
        top += jnp.where(lane256 < 64, wide, 0.0)
        bottom += jnp.where(lane256 < 64, 0.0, wide)
    has_sums = x == NX - 1
    for j in range(NZ):
        squares = as_pair(
            jnp.sum((top if j < 4 else bottom)[64 * (j % 4) : 64 * (j % 4) + 64], axis=1, keepdims=True)
        )
        for k in range(NX):
            rows = slice(64 * (j % 4) + 16 * k, 64 * (j % 4) + 16 * k + 16)
            first = 256 * (j // 4)
            part1[j, k, :, 0:128] = total[rows, first : first + 128].astype(BF16)
            part1[j, k, :, 128:256] = jnp.where(
                has_sums,
                squares[16 * k : 16 * k + 16].astype(F32),
                total[rows, first + 128 : first + 256],
            ).astype(BF16)
    got1[x, z] = part1[z, x]
    scatter1 = go(
        [
            send(part1.at[at_z(dz), at_x(dx)], got1.at[x, z], (at_z(dz) * NX + at_x(dx), t))
            for dz, dx in PLANE
        ]
    )
    mix_blocks = go(
        [send(w_mix.at[:, lanes_z], w_mix.at[:, lanes_z], peer) for d, peer in ring_z]
    )

    with jax.named_scope("wait_ff_blocks"):
        arrive(ff_blocks)
    partner = (kv, t + 1 - 2 * core)
    ff_y = go(
        [
            send(ff_all.at[:, t], ff_all.at[:, t], (kv, lax.rem(y + d, NY) * 2 + core))
            for d in range(1, NY)
        ]
    )
    ff_core = go([send(ff_all.at[:, t], ff_all.at[:, t], partner)])

    with jax.named_scope("wait_scatter1"):
        arrive(scatter1)
    proj = []
    for j in range(NX):
        total = got1[j, 0].astype(F32)
        for k in range(1, NZ):
            total += got1[j, k].astype(F32)
        proj.append(total)
    load(STATE)

    inv = lax.rsqrt(of_pair(proj[3][:, 128:256]) / D + EPS)
    query = proj[0][:, 0:128] * (inv * DK ** (-0.5))
    keys = proj[0][:, 128:256] * inv
    values = proj[1] * inv
    gate = proj[2] * inv
    decay_pre = proj[3][:, 0:128] * inv
    log_sigmoid = jnp.minimum(decay_pre, 0.0) - jnp.log1p(jnp.exp(-jnp.abs(decay_pre)))
    decay = jnp.exp(log_sigmoid / GATE_NORM + log_decay[...])
    columns = jnp.transpose(
        jnp.concatenate([query, keys, decay, jnp.zeros((80, 128), F32)], axis=0), (1, 0)
    )
    for b in range(16):
        q_col = columns[:, b : b + 1]
        k_col = columns[:, 16 + b : 17 + b]
        a_col = columns[:, 32 + b : 33 + b]
        new = state[b] * a_col + k_col * values[b : b + 1, :]
        new_state[b] = new
        att[b : b + 1, :] = jnp.sum(new * q_col, axis=0, keepdims=True)
    attended = att[...]
    normed = (
        attended
        * lax.rsqrt(jnp.mean(attended * attended, axis=1, keepdims=True) + EPS)
        * out_gain[...]
    )
    mix[x] = (normed * (gate * sigmoid(gate))).astype(BF16)
    gather2 = go([send(mix.at[x], mix.at[x], peer) for d, peer in ring_x])
    state_back = pltpu.make_async_copy(new_state, state_out, local_sems.at[15])
    state_back.start()

    with jax.named_scope("wait_mix_blocks"):
        arrive(mix_blocks)
    with jax.named_scope("wait_gather2"):
        arrive(gather2)
    mixed = mix[...].reshape(64, DV)
    for j, block in enumerate(packed_products(mixed, w_mix[...], lane32)):
        part2[j] = block.astype(BF16)
    got2[t] = part2[t]
    scatter2 = go([send(part2.at[at_t(d)], got2.at[t], peer) for d, peer in ring_t])
    with jax.named_scope("wait_scatter2"):
        arrive(scatter2)
    total = got2[0].astype(F32)
    for j in range(1, NT):
        total += got2[j].astype(F32)
    attn_own[...] = total.astype(BF16)

    first_send, first_recv = new_sem(NT), 0
    first_recv = first_send
    spread = [
        send(
            attn_own,
            attn_all.at[t],
            (at_z(d) * NX + x, z),
            sem=first_send + d,
            recv=first_recv + t,
        )
        for d in range(NZ)
    ]
    diagonal = t == z

    @pl.when(diagonal)
    def _():
        attn_all[t] = attn_own[...]

    @pl.when(jnp.logical_not(diagonal))
    def _():
        spread[0].start()

    go(spread[1:])

    with jax.named_scope("wait_ff_y"):
        arrive(ff_y)
    for d in range(1, NY):
        other = lax.rem(y + d, NY) * 2 + core
        ff_core += go([send(ff_all.at[:, other], ff_all.at[:, other], partner)])

    with jax.named_scope("wait_tok_blocks"):
        arrive(tok_blocks)
    def wait_spread(j):
        copy = pltpu.make_async_remote_copy(
            src_ref=attn_own,
            dst_ref=attn_all.at[j],
            send_sem=send_sems.at[first_send],
            recv_sem=recv_sems.at[first_recv + j],
            device_id=(kv, t),
            device_id_type=MESH,
        )

        @pl.when(jnp.logical_or(t != z, j != t))
        def _(copy=copy):
            copy.wait_recv()

    with jax.named_scope("wait_spread"):
        for j in range(NT):
            wait_spread(j)

    top = jnp.zeros((32, 128), F32)
    bottom = jnp.zeros((32, 128), F32)
    pieces = []
    for j in range(NZ):
        block = (tok_all[j].astype(F32) + attn_all[j].astype(F32)).astype(BF16)
        middle[j] = block
        wide = block.astype(F32)
        low = jnp.where(lane32 < 64, wide, 0.0)
        high = jnp.where(lane32 < 64, 0.0, wide)
        top += low * low
        bottom += high * high
        pieces.append(
            jnp.concatenate(
                [low, pltpu.roll(high, 64, 1), pltpu.roll(low, 64, 1), high], axis=0
            ).astype(BF16)
        )
    left = jnp.concatenate(pieces, axis=1)
    squares = as_pair(
        jnp.concatenate(
            [jnp.sum(top, axis=1, keepdims=True), jnp.sum(bottom, axis=1, keepdims=True)], axis=0
        )
    )
    with jax.named_scope("wait_ff_core"):
        arrive(ff_core)
    weights = ff_all[0:2].reshape(NT * 96, 1024)
    terms = lax.dot_general(
        left, weights, (((1,), (1,)), ((), ())), preferred_element_type=F32
    )
    for j in range(NX):
        rows = slice(16 * j, 16 * j + 16)
        part3[j, :, 0:768] = terms[rows].astype(BF16)
        part3[j, :, 768:1536] = terms[64 + 16 * j : 80 + 16 * j].astype(BF16)
        part3[j, :, 1536:1664] = squares[rows]
    got3[x] = part3[x]
    scatter3 = go([send(part3.at[at_x(d)], got3.at[x], peer) for d, peer in ring_x])
    with jax.named_scope("wait_scatter3"):
        arrive(scatter3)
    total = got3[0].astype(F32)
    for j in range(1, NX):
        total += got3[j].astype(F32)
    inv = lax.rsqrt(of_pair(total[:, 1536:1664]) / D + EPS)
    gate = total[:, 0:768] * inv
    hid[x] = (gate * sigmoid(gate) * (total[:, 768:1536] * inv)).astype(BF16)
    gather3 = go([send(hid.at[x], hid.at[x], peer) for d, peer in ring_x])
    with jax.named_scope("wait_gather3"):
        arrive(gather3)

    hidden = hid[...].reshape(64, 768)
    weights = ff_all[2].reshape(NT * 48, 1024)
    for j, block in enumerate(packed_products(hidden, weights, lane32)):
        part4[j] = block.astype(BF16)
    got4[z] = part4[z]
    scatter4 = go([send(part4.at[at_z(d)], got4.at[z], peer) for d, peer in ring_z])
    with jax.named_scope("wait_scatter4"):
        arrive(scatter4)
    total = got4[0].astype(F32)
    for j in range(1, NZ):
        total += got4[j].astype(F32)
    res_own[...] = (middle[z].astype(F32) + total).astype(BF16)
    res_all[t] = res_own[...]
    gather4 = go([send(res_own, res_all.at[t], peer) for d, peer in ring_t])
    with jax.named_scope("wait_gather4"):
        arrive(gather4)
    res_back = pltpu.make_async_copy(res_all, res_out, local_sems.at[16])
    res_back.start()
    with jax.named_scope("wait_sends"):
        for copy in sent:
            copy.wait_send()

    @pl.when(jnp.logical_not(diagonal))
    def _():
        spread[0].wait_send()

    with jax.named_scope("wait_state_back"):
        state_back.wait()
    with jax.named_scope("wait_res_back"):
        res_back.wait()


def finish(blocks_in, state_in, result_out, state_out, blocks, state, result, sems):
    first = pltpu.make_async_copy(blocks_in, blocks, sems.at[32])
    first.start()
    count = state.shape[0]
    for i in range(count):
        pltpu.make_async_copy(state_in.at[i], state.at[i], sems.at[i]).start()
    first.wait()
    rows = []
    for j in range(NT):
        block = blocks[j].astype(F32)
        rows += [block, pltpu.roll(block, 64, 1)]
    rows = jnp.concatenate(rows, axis=0)
    result[...] = jnp.transpose(rows, (1, 0))[0:64].astype(BF16)
    last = pltpu.make_async_copy(result, result_out, sems.at[33])
    last.start()
    for i in range(count):
        pltpu.make_async_copy(state_in.at[i], state.at[i], sems.at[i]).wait()
        pltpu.make_async_copy(state.at[i], state_out.at[i], sems.at[16 + i]).start()
    for i in range(count):
        pltpu.make_async_copy(state.at[i], state_out.at[i], sems.at[16 + i]).wait()
    last.wait()


def body(
    tokens,
    norm_gain,
    w_query,
    w_key,
    w_value,
    w_gate,
    w_decay,
    log_decay,
    state,
    out_gain,
    w_out,
    mixer_gain,
    w_ffgate,
    w_ffup,
    w_down,
):
    hbm = pl.BlockSpec(memory_space=pltpu.HBM)
    shape = state.shape
    arguments = (
        tokens.T,
        norm_gain.reshape(1, 64),
        w_query,
        w_key,
        w_value,
        w_gate,
        w_decay,
        log_decay,
        state.reshape(shape[0], DK, DV),
        out_gain.reshape(1, DV),
        w_out.T,
        mixer_gain.reshape(1, 64),
        w_ffgate,
        w_ffup,
        w_down.T,
    )
    blocks, new_state = pl.pallas_call(
        kernel,
        out_shape=(
            jax.ShapeDtypeStruct((NT, 32, 128), BF16),
            jax.ShapeDtypeStruct((shape[0], DK, DV), F32),
        ),
        in_specs=[hbm] * 15,
        out_specs=(hbm, hbm),
        scratch_shapes=[pltpu.VMEM(value.shape, value.dtype) for value in arguments]
        + [
            pltpu.VMEM((16, DK, DV), F32),
            pltpu.VMEM((16, DV), F32),
            pltpu.VMEM((NX, 64, 256), BF16),
            pltpu.VMEM((NX, 256, 128), BF16),
            pltpu.VMEM((NX, 64, 256), BF16),
            pltpu.VMEM((NX, 128, 512), BF16),
            pltpu.VMEM((NZ, NX, 16, 256), BF16),
            pltpu.VMEM((NX, NZ, 16, 256), BF16),
            pltpu.VMEM((NX, 16, 256), BF16),
            pltpu.VMEM((128, 1024), BF16),
            pltpu.VMEM((NT, 32, 128), BF16),
            pltpu.VMEM((NT, 32, 128), BF16),
            pltpu.VMEM((32, 128), BF16),
            pltpu.VMEM((NT, 32, 128), BF16),
            pltpu.VMEM((32, 128), BF16),
            pltpu.VMEM((NZ, 32, 128), BF16),
            pltpu.VMEM((NZ, 32, 128), BF16),
            pltpu.VMEM((NZ, 3, 48, 128), BF16),
            pltpu.VMEM((3, NT, 48, 1024), BF16),
            pltpu.VMEM((NX, 16, 1664), BF16),
            pltpu.VMEM((NX, 16, 1664), BF16),
            pltpu.VMEM((NX, 16, 768), BF16),
            pltpu.VMEM((NZ, 32, 128), BF16),
            pltpu.VMEM((NZ, 32, 128), BF16),
            pltpu.VMEM((32, 128), BF16),
            pltpu.VMEM((NT, 32, 128), BF16),
            pltpu.SemaphoreType.DMA((COPIES,)),
            pltpu.SemaphoreType.DMA((COPIES,)),
            pltpu.SemaphoreType.DMA((17,)),
        ],
        compiler_params=pltpu.CompilerParams(
            collective_id=0, has_side_effects=True, vmem_limit_bytes=67043328
        ),
    )(*arguments)
    result, new_state = pl.pallas_call(
        finish,
        out_shape=(
            jax.ShapeDtypeStruct((64, 512), BF16),
            jax.ShapeDtypeStruct((shape[0], DK, DV), F32),
        ),
        in_specs=[hbm, hbm],
        out_specs=(hbm, hbm),
        scratch_shapes=[
            pltpu.VMEM((NT, 32, 128), BF16),
            pltpu.VMEM((shape[0], DK, DV), F32),
            pltpu.VMEM((64, 512), BF16),
            pltpu.SemaphoreType.DMA((34,)),
        ],
        compiler_params=pltpu.CompilerParams(vmem_limit_bytes=67043328),
    )(blocks, new_state)
    return (result.T, new_state.reshape(shape))


def solution(mesh):
    return jax.shard_map(
        body,
        mesh=mesh,
        in_specs=(
            P(None, "kv"),
            P("kv"),
            P("kv", "tp"),
            P("kv", "tp"),
            P("kv", "tp"),
            P("kv", "tp"),
            P("kv", "tp"),
            P("kv", "tp"),
            P("kv", "tp", None, None),
            P(),
            P("tp", "kv"),
            P("kv"),
            P("kv", "tp"),
            P("kv", "tp"),
            P("tp", "kv"),
        ),
        out_specs=(P(None, "kv"), P("kv", "tp", None, None)),
        check_vma=False,
    )
```

```python
import functools

import jax
import jax.numpy as jnp
from jax import lax
from jax.experimental import pallas as pl
from jax.experimental.pallas import tpu as pltpu
from jax.sharding import PartitionSpec as P

MESH = pl.DeviceIdType.MESH
F32 = jnp.float32
BF16 = jnp.bfloat16

D = 2048
DK = 128
DV = 256
EPS = 1e-06
GATE_NORM = 16.0

NX, NY, NZ = 4, 4, 8
NT = 2 * NY
COPIES = 21
FAR_X = [2, 1, 3]
FAR_Y = [2, 1, 3]
FAR_Z = [4, 3, 5, 2, 6, 1, 7]
FAR_T = [4, 5, 2, 3, 6, 7, 1]
PLANE = [(dz, dx) for dz in FAR_Z + [0] for dx in FAR_X + [0] if (dz, dx) != (0, 0)]
LOADS = [(0, 0), (1, 1), (2, 0), (3, 0), (4, 0), (5, 0), (6, 0)]
LOADS += [(10, 3), (12, 2), (13, 2), (14, 2), (11, 4), (7, 5), (9, 6), (8, 7)]


def sigmoid(value):
    return 1.0 / (1.0 + jnp.exp(-value))


def halves(low, high):
    return jnp.concatenate([low, high], axis=1)


def as_pair(total):
    high = jnp.broadcast_to(total, (total.shape[0], 128)).astype(BF16).astype(F32)
    low = jnp.broadcast_to(total, (total.shape[0], 128)) - high
    lane = lax.broadcasted_iota(jnp.int32, high.shape, 1)
    return jnp.where(lane < 64, high, low).astype(BF16)


def of_pair(pair):
    return pair[:, 0:1] + pair[:, 64:65]


def packed_products(left, right, lane):
    width = left.shape[1] // 2
    stacked = jnp.concatenate([left[:, :width], left[:, width:]], axis=0)
    total = jnp.dot(stacked, right, preferred_element_type=F32)
    blocks = []
    for j in range(8):
        first = total[0:64, 128 * j : 128 * j + 128]
        second = total[64:128, 128 * j : 128 * j + 128]
        top = first[0:32] + pltpu.roll(second[0:32], 64, 1)
        bottom = pltpu.roll(first[32:64], 64, 1) + second[32:64]
        blocks.append(jnp.where(lane < 64, top, bottom))
    return blocks


def kernel(*refs):
    inputs, (res_out, state_out), refs = refs[:15], refs[15:17], refs[17:]
    held, refs = refs[:15], refs[15:]
    (
        tokens,
        norm_gain,
        w_query,
        w_key,
        w_value,
        w_gate,
        w_decay,
        log_decay,
        state,
        out_gain,
        w_out,
        mixer_gain,
        w_ffgate,
        w_ffup,
        w_down,
    ) = held
    (
        new_state,
        att,
        w_own,
        x_all,
        w_all,
        w_diag,
        part1,
        got1,
        mix,
        w_mix,
        part2,
        got2,
        attn_own,
        attn_all,
        tok_own,
        tok_all,
        middle,
        ff_own,
        ff_all,
        part3,
        got3,
        hid,
        part4,
        got4,
        res_own,
        res_all,
        send_sems,
        recv_sems,
        local_sems,
    ) = refs
    kv = lax.axis_index("kv")
    t = lax.axis_index("tp")
    z, x = lax.div(kv, NX), lax.rem(kv, NX)
    y, core = lax.div(t, 2), lax.rem(t, 2)

    def at_x(d):
        return lax.rem(x + d, NX)

    def at_z(d):
        return lax.rem(z + d, NZ)

    def at_t(d):
        return lax.rem(t + d, NT)

    counter = [0]
    unsent = []

    class Exchange:
        def __init__(self, size):
            self.number = counter[0]
            self.size = size
            counter[0] += 1
            unsent.append(self)

        def send(self, src, dst, peer):
            pltpu.make_async_remote_copy(
                src_ref=src,
                dst_ref=dst,
                send_sem=send_sems.at[self.number],
                recv_sem=recv_sems.at[self.number],
                device_id=peer,
                device_id_type=MESH,
            ).start()

        def wait(self, sems, size):
            pltpu.make_async_copy(size, size, sems.at[self.number]).wait()

        def arrive(self):
            self.wait(recv_sems, self.size)

        def leave(self):
            self.wait(send_sems, self.size)

    barrier = pltpu.get_barrier_semaphore()

    def greet(peer):
        pl.semaphore_signal(barrier, inc=1, device_id=peer, device_id_type=MESH)

    for dz, dx in PLANE:
        greet((at_z(dz) * NX + at_x(dx), t))
    for d in FAR_T:
        greet((kv, at_t(d)))
    for d in FAR_Z:
        greet((at_z(d) * NX + x, z))

    @pl.when(t != z)
    def _():
        greet((kv, z))

    for i, sem in LOADS:
        pltpu.make_async_copy(inputs[i], held[i], local_sems.at[sem]).start()

    def loaded(sem, size):
        pltpu.make_async_copy(size, size, local_sems.at[sem]).wait()

    with jax.named_scope("wait_first"):
        loaded(0, part1.at[0:22])
        loaded(1, norm_gain)
    square = (64, 64)
    row = lax.broadcasted_iota(jnp.int32, square, 0)
    column = lax.broadcasted_iota(jnp.int32, square, 1)
    gain = jnp.sum(
        jnp.where(row == column, jnp.broadcast_to(norm_gain[...].astype(F32), square), 0.0),
        axis=1,
        keepdims=True,
    )

    def gained(weight):
        return (weight[...].astype(F32) * gain).astype(BF16)

    w_own[0, :, 0:128] = gained(w_query)
    w_own[0, :, 128:256] = gained(w_key)
    w_own[1] = gained(w_value)
    w_own[2] = gained(w_gate)
    w_own[3, :, 0:128] = gained(w_decay)
    w_own[3, :, 128:256] = jnp.zeros((64, 128), BF16)
    own = jnp.concatenate([tokens[:, 0:256], tokens[:, 256:512]], axis=0).astype(F32)
    x_all[x] = jnp.transpose(own, (1, 0)).astype(BF16)
    w_all[x] = w_own[x]

    greetings = len(PLANE) + len(FAR_T) + len(FAR_Z)
    with jax.named_scope("wait_barrier"):
        pl.semaphore_wait(barrier, greetings + jnp.where(t != z, 1, 0))

    tile_z = w_mix.at[:, 0:128]

    def lanes_of(block):
        return pl.ds(pl.multiple_of(block * 128, 128), 128)

    ring_x = [(d, (z * NX + at_x(d), t)) for d in FAR_X]
    ring_z = [(d, (at_z(d) * NX + x, t)) for d in FAR_Z]
    ring_t = [(d, (kv, at_t(d))) for d in FAR_T]
    gather_w, gather_x = Exchange(w_all.at[0:3]), Exchange(x_all.at[0:3])
    for d, peer in ring_x:
        gather_w.send(w_own.at[at_x(d)], w_all.at[x], peer)
    for d, peer in ring_x:
        gather_x.send(x_all.at[x], x_all.at[x], peer)

    with jax.named_scope("wait_later"):
        loaded(3, w_out)
    out_rows = jnp.concatenate([w_out[:, 0:128], w_out[:, 128:256]], axis=0).astype(F32)
    w_mix[:, lanes_of(z)] = jnp.transpose(out_rows, (1, 0)).astype(BF16)
    mix_steps = []

    def mix_step(step):
        if step > 1:
            for exchange in mix_steps[-1]:
                exchange.arrive()
        exchanges = []
        for way in (1, -1):
            if step <= (4 if way > 0 else 3):
                lanes = lanes_of(at_z(NZ - way * (step - 1)))
                exchange = Exchange(tile_z)
                exchange.send(
                    w_mix.at[:, lanes], w_mix.at[:, lanes], (at_z(NZ + way) * NX + x, t)
                )
                exchanges.append(exchange)
        mix_steps.append(exchanges)

    mix_step(1)

    with jax.named_scope("wait_later"):
        loaded(2, ff_all.at[0, 0:3])
        loaded(4, mixer_gain)
        loaded(5, log_decay)
        loaded(6, out_gain)
    gains = mixer_gain[...].astype(F32)
    units = jnp.transpose(
        jnp.concatenate([w_ffgate[...], w_ffup[...]], axis=0).astype(F32), (1, 0)
    )
    units = (units * jnp.concatenate([gains, gains], axis=1)).astype(BF16)
    down = w_down[...].astype(F32)
    down = jnp.concatenate([down, pltpu.roll(down, 768 - 48, 1)], axis=0)
    down = jnp.transpose(down, (1, 0)).astype(BF16)
    for j in range(NZ):
        low, high = slice(96 * j, 96 * j + 48), slice(96 * j + 48, 96 * j + 96)
        ff_own[j, 0] = units[low]
        ff_own[j, 1] = units[high]
        ff_own[j, 2] = down[low]
    lanes_z = lanes_of(z)
    ff_all[:, t, :, lanes_z] = ff_own[z]
    ff_blocks = Exchange(ff_own.at[0:7])
    for d, peer in ring_z:
        ff_blocks.send(ff_own.at[at_z(d)], ff_all.at[:, t, :, lanes_z], peer)
    lane32 = lax.broadcasted_iota(jnp.int32, (32, 128), 1)
    rows = pl.multiple_of(64 * lax.rem(t, 4), 64)
    own = x_all[x, pl.ds(rows, 64), :].astype(F32)
    own = jnp.where(t < 4, own, pltpu.roll(own, 64, 1))
    tok_own[...] = jnp.where(lane32 < 64, own[0:32], pltpu.roll(own[32:64], 64, 1)).astype(BF16)
    tok_all[z] = tok_own[...]
    w_diag[...] = jnp.zeros(w_diag.shape, BF16)

    with jax.named_scope("wait_gather1"):
        gather_w.arrive()
        gather_x.arrive()
    mix_step(2)
    lane256 = lax.broadcasted_iota(jnp.int32, (256, 128), 1)
    total = jnp.zeros((256, 512), F32)
    top = jnp.zeros((256, 128), F32)
    bottom = jnp.zeros((256, 128), F32)
    for j in range(NX):
        w_diag[j, 0:64, 0:256] = w_all[j]
        w_diag[j, 64:128, 256:512] = w_all[j]
    for j in range(NX):
        block = x_all[j]
        total += jnp.dot(block, w_diag[j], preferred_element_type=F32)
        wide = block.astype(F32)
        wide = wide * wide
        top += jnp.where(lane256 < 64, wide, 0.0)
        bottom += jnp.where(lane256 < 64, 0.0, wide)
    has_sums = x == NX - 1
    for j in range(NZ):
        squares = as_pair(
            jnp.sum((top if j < 4 else bottom)[64 * (j % 4) : 64 * (j % 4) + 64], axis=1, keepdims=True)
        )
        for k in range(NX):
            rows = slice(64 * (j % 4) + 16 * k, 64 * (j % 4) + 16 * k + 16)
            first = 256 * (j // 4)
            part1[NX * j + k, :, 0:128] = total[rows, first : first + 128].astype(BF16)
            part1[NX * j + k, :, 128:256] = jnp.where(
                has_sums,
                squares[16 * k : 16 * k + 16].astype(F32),
                total[rows, first + 128 : first + 256],
            ).astype(BF16)
    got1[x * NZ + z] = part1[kv]
    scatter1 = Exchange(got1.at[0:31])
    for dz, dx in PLANE:
        peer = at_z(dz) * NX + at_x(dx)
        scatter1.send(part1.at[peer], got1.at[x * NZ + z], (peer, t))
    tok_blocks = Exchange(tok_all.at[0:7])
    for d, peer in ring_z:
        tok_blocks.send(tok_own, tok_all.at[z], peer)

    with jax.named_scope("wait_ff_blocks"):
        ff_blocks.arrive()
    partner = (kv, t + 1 - 2 * core)
    ff_y, ff_core = Exchange(ff_all.at[:, 0:3]), Exchange(ff_all.at[:, 0:4])
    for d in FAR_Y:
        ff_y.send(ff_all.at[:, t], ff_all.at[:, t], (kv, lax.rem(y + d, NY) * 2 + core))
    ff_core.send(ff_all.at[:, t], ff_all.at[:, t], partner)
    mix_step(3)

    with jax.named_scope("wait_scatter1"):
        scatter1.arrive()
    mix_step(4)
    proj = []
    for j in range(NX):
        total = got1[NZ * j].astype(F32)
        for k in range(1, NZ):
            total += got1[NZ * j + k].astype(F32)
        proj.append(total)
    loaded(7, state)

    inv = lax.rsqrt(of_pair(proj[3][:, 128:256]) / D + EPS)
    query = proj[0][:, 0:128] * (inv * DK ** (-0.5))
    keys = proj[0][:, 128:256] * inv
    values = proj[1] * inv
    gate = proj[2] * inv
    decay_pre = proj[3][:, 0:128] * inv
    log_sigmoid = jnp.minimum(decay_pre, 0.0) - jnp.log1p(jnp.exp(-jnp.abs(decay_pre)))
    decay = jnp.exp(log_sigmoid / GATE_NORM + log_decay[...])
    columns = jnp.transpose(
        jnp.concatenate([query, keys, decay, jnp.zeros((80, 128), F32)], axis=0), (1, 0)
    )
    for b in range(16):
        q_col = columns[:, b : b + 1]
        k_col = columns[:, 16 + b : 17 + b]
        a_col = columns[:, 32 + b : 33 + b]
        new = state[b] * a_col + k_col * values[b : b + 1, :]
        new_state[b] = new
        att[b : b + 1, :] = jnp.sum(new * q_col, axis=0, keepdims=True)
    attended = att[...]
    normed = (
        attended
        * lax.rsqrt(jnp.mean(attended * attended, axis=1, keepdims=True) + EPS)
        * out_gain[...]
    )
    mix[x] = (normed * (gate * sigmoid(gate))).astype(BF16)
    gather2 = Exchange(mix.at[0:3])
    for d, peer in ring_x:
        gather2.send(mix.at[x], mix.at[x], peer)
    state_back = pltpu.make_async_copy(new_state, state_out, local_sems.at[8])
    state_back.start()

    with jax.named_scope("wait_mix_blocks"):
        for exchange in mix_steps[-1]:
            exchange.arrive()
    with jax.named_scope("wait_gather2"):
        gather2.arrive()
    mixed = mix[...].reshape(64, DV)
    for j, block in enumerate(packed_products(mixed, w_mix[...], lane32)):
        part2[j] = block.astype(BF16)
    got2[t] = part2[t]
    scatter2 = Exchange(got2.at[0:7])
    for d, peer in ring_t:
        scatter2.send(part2.at[at_t(d)], got2.at[t], peer)
    with jax.named_scope("wait_scatter2"):
        scatter2.arrive()
    total = got2[0].astype(F32)
    for j in range(1, NT):
        total += got2[j].astype(F32)
    attn_own[...] = total.astype(BF16)

    spread = Exchange(attn_all)
    diagonal = t == z
    for d in FAR_Z:
        spread.send(attn_own, attn_all.at[t], (at_z(d) * NX + x, z))

    @pl.when(jnp.logical_not(diagonal))
    def _():
        spread.send(attn_own, attn_all.at[t], (kv, z))

    @pl.when(diagonal)
    def _():
        attn_all[t] = attn_own[...]

    def spread_wait(sems):
        @pl.when(diagonal)
        def _():
            spread.wait(sems, attn_all.at[0:7])

        @pl.when(jnp.logical_not(diagonal))
        def _():
            spread.wait(sems, attn_all)

    with jax.named_scope("wait_ff_y"):
        ff_y.arrive()
    for d in range(1, NY):
        other = lax.rem(y + d, NY) * 2 + core
        ff_core.send(ff_all.at[:, other], ff_all.at[:, other], partner)

    with jax.named_scope("wait_tok_blocks"):
        tok_blocks.arrive()
    with jax.named_scope("wait_spread"):
        spread_wait(recv_sems)

    top = jnp.zeros((32, 128), F32)
    bottom = jnp.zeros((32, 128), F32)
    pieces = []
    for j in range(NZ):
        block = (tok_all[j].astype(F32) + attn_all[j].astype(F32)).astype(BF16)
        middle[j] = block
        wide = block.astype(F32)
        low = jnp.where(lane32 < 64, wide, 0.0)
        high = jnp.where(lane32 < 64, 0.0, wide)
        top += low * low
        bottom += high * high
        pieces.append(
            jnp.concatenate(
                [low, pltpu.roll(high, 64, 1), pltpu.roll(low, 64, 1), high], axis=0
            ).astype(BF16)
        )
    left = jnp.concatenate(pieces, axis=1)
    squares = as_pair(
        jnp.concatenate(
            [jnp.sum(top, axis=1, keepdims=True), jnp.sum(bottom, axis=1, keepdims=True)], axis=0
        )
    )
    with jax.named_scope("wait_ff_core"):
        ff_core.arrive()
    weights = ff_all[0:2].reshape(NT * 96, 1024)
    terms = lax.dot_general(
        left, weights, (((1,), (1,)), ((), ())), preferred_element_type=F32
    )
    for j in range(NX):
        rows = slice(16 * j, 16 * j + 16)
        part3[j, :, 0:768] = terms[rows].astype(BF16)
        part3[j, :, 768:1536] = terms[64 + 16 * j : 80 + 16 * j].astype(BF16)
        part3[j, :, 1536:1664] = squares[rows]
    got3[x] = part3[x]
    scatter3 = Exchange(got3.at[0:3])
    for d, peer in ring_x:
        scatter3.send(part3.at[at_x(d)], got3.at[x], peer)
    with jax.named_scope("wait_scatter3"):
        scatter3.arrive()
    total = got3[0].astype(F32)
    for j in range(1, NX):
        total += got3[j].astype(F32)
    inv = lax.rsqrt(of_pair(total[:, 1536:1664]) / D + EPS)
    gate = total[:, 0:768] * inv
    hid[x] = (gate * sigmoid(gate) * (total[:, 768:1536] * inv)).astype(BF16)
    gather3 = Exchange(hid.at[0:3])
    for d, peer in ring_x:
        gather3.send(hid.at[x], hid.at[x], peer)
    with jax.named_scope("wait_gather3"):
        gather3.arrive()

    hidden = hid[...].reshape(64, 768)
    weights = ff_all[2].reshape(NT * 48, 1024)
    for j, block in enumerate(packed_products(hidden, weights, lane32)):
        part4[j] = block.astype(BF16)
    got4[z] = part4[z]
    scatter4 = Exchange(got4.at[0:7])
    for d, peer in ring_z:
        scatter4.send(part4.at[at_z(d)], got4.at[z], peer)
    with jax.named_scope("wait_scatter4"):
        scatter4.arrive()
    total = got4[0].astype(F32)
    for j in range(1, NZ):
        total += got4[j].astype(F32)
    res_own[...] = (middle[z].astype(F32) + total).astype(BF16)
    res_all[t] = res_own[...]
    gather4 = Exchange(res_all.at[0:7])
    for d, peer in ring_t:
        gather4.send(res_own, res_all.at[t], peer)
    with jax.named_scope("wait_gather4"):
        gather4.arrive()
    res_back = pltpu.make_async_copy(res_all, res_out, local_sems.at[9])
    res_back.start()
    with jax.named_scope("wait_sends"):
        for exchange in unsent:
            if exchange is spread:
                spread_wait(send_sems)
            else:
                exchange.leave()
    with jax.named_scope("wait_state_back"):
        state_back.wait()
    with jax.named_scope("wait_res_back"):
        res_back.wait()


def finish(blocks_in, state_in, result_out, state_out, blocks, state, result, sems):
    first = pltpu.make_async_copy(blocks_in, blocks, sems.at[0])
    last = pltpu.make_async_copy(result, result_out, sems.at[1])
    everything = pltpu.make_async_copy(state, state, sems.at[2])
    parts = [pl.ds(2 * i, 2) for i in range(8)]
    first.start()
    for i, part in enumerate(parts):
        pltpu.make_async_copy(state_in.at[part], state.at[part], sems.at[3 + i]).start()
    first.wait()
    rows = []
    for j in range(NT):
        block = blocks[j].astype(F32)
        rows += [block, pltpu.roll(block, 64, 1)]
    rows = jnp.concatenate(rows, axis=0)
    result[...] = jnp.transpose(rows, (1, 0))[0:64].astype(BF16)
    last.start()
    for i, part in enumerate(parts):
        pltpu.make_async_copy(state_in.at[part], state.at[part], sems.at[3 + i]).wait()
        pltpu.make_async_copy(state.at[part], state_out.at[part], sems.at[2]).start()
    everything.wait()
    last.wait()


def body(
    tokens,
    norm_gain,
    w_query,
    w_key,
    w_value,
    w_gate,
    w_decay,
    log_decay,
    state,
    out_gain,
    w_out,
    mixer_gain,
    w_ffgate,
    w_ffup,
    w_down,
):
    hbm = pl.BlockSpec(memory_space=pltpu.HBM)
    shape = state.shape
    arguments = (
        tokens.T,
        norm_gain.reshape(1, 64),
        w_query,
        w_key,
        w_value,
        w_gate,
        w_decay,
        log_decay,
        state.reshape(shape[0], DK, DV),
        out_gain.reshape(1, DV),
        w_out.T,
        mixer_gain.reshape(1, 64),
        w_ffgate,
        w_ffup,
        w_down.T,
    )
    blocks, new_state = pl.pallas_call(
        kernel,
        out_shape=(
            jax.ShapeDtypeStruct((NT, 32, 128), BF16),
            jax.ShapeDtypeStruct((shape[0], DK, DV), F32),
        ),
        in_specs=[hbm] * 15,
        out_specs=(hbm, hbm),
        scratch_shapes=[pltpu.VMEM(value.shape, value.dtype) for value in arguments]
        + [
            pltpu.VMEM((16, DK, DV), F32),
            pltpu.VMEM((16, DV), F32),
            pltpu.VMEM((NX, 64, 256), BF16),
            pltpu.VMEM((NX, 256, 128), BF16),
            pltpu.VMEM((NX, 64, 256), BF16),
            pltpu.VMEM((NX, 128, 512), BF16),
            pltpu.VMEM((NZ * NX, 16, 256), BF16),
            pltpu.VMEM((NX * NZ, 16, 256), BF16),
            pltpu.VMEM((NX, 16, 256), BF16),
            pltpu.VMEM((128, 1024), BF16),
            pltpu.VMEM((NT, 32, 128), BF16),
            pltpu.VMEM((NT, 32, 128), BF16),
            pltpu.VMEM((32, 128), BF16),
            pltpu.VMEM((NT, 32, 128), BF16),
            pltpu.VMEM((32, 128), BF16),
            pltpu.VMEM((NZ, 32, 128), BF16),
            pltpu.VMEM((NZ, 32, 128), BF16),
            pltpu.VMEM((NZ, 3, 48, 128), BF16),
            pltpu.VMEM((3, NT, 48, 1024), BF16),
            pltpu.VMEM((NX, 16, 1664), BF16),
            pltpu.VMEM((NX, 16, 1664), BF16),
            pltpu.VMEM((NX, 16, 768), BF16),
            pltpu.VMEM((NZ, 32, 128), BF16),
            pltpu.VMEM((NZ, 32, 128), BF16),
            pltpu.VMEM((32, 128), BF16),
            pltpu.VMEM((NT, 32, 128), BF16),
            pltpu.SemaphoreType.DMA((COPIES,)),
            pltpu.SemaphoreType.DMA((COPIES,)),
            pltpu.SemaphoreType.DMA((10,)),
        ],
        compiler_params=pltpu.CompilerParams(
            collective_id=0, has_side_effects=True, vmem_limit_bytes=67043328
        ),
    )(*arguments)
    result, new_state = pl.pallas_call(
        finish,
        out_shape=(
            jax.ShapeDtypeStruct((64, 512), BF16),
            jax.ShapeDtypeStruct((shape[0], DK, DV), F32),
        ),
        in_specs=[hbm, hbm],
        out_specs=(hbm, hbm),
        scratch_shapes=[
            pltpu.VMEM((NT, 32, 128), BF16),
            pltpu.VMEM((shape[0], DK, DV), F32),
            pltpu.VMEM((64, 512), BF16),
            pltpu.SemaphoreType.DMA((11,)),
        ],
        compiler_params=pltpu.CompilerParams(vmem_limit_bytes=67043328),
    )(blocks, new_state)
    return (result.T, new_state.reshape(shape))


def solution(mesh):
    return jax.shard_map(
        body,
        mesh=mesh,
        in_specs=(
            P(None, "kv"),
            P("kv"),
            P("kv", "tp"),
            P("kv", "tp"),
            P("kv", "tp"),
            P("kv", "tp"),
            P("kv", "tp"),
            P("kv", "tp"),
            P("kv", "tp", None, None),
            P(),
            P("tp", "kv"),
            P("kv"),
            P("kv", "tp"),
            P("kv", "tp"),
            P("tp", "kv"),
        ),
        out_specs=(P(None, "kv"), P("kv", "tp", None, None)),
        check_vma=False,
    )
```

```python
import functools

import jax
import jax.numpy as jnp
from jax import lax
from jax.experimental import pallas as pl
from jax.experimental.pallas import tpu as pltpu
from jax.sharding import PartitionSpec as P

MESH = pl.DeviceIdType.MESH
F32 = jnp.float32
BF16 = jnp.bfloat16

D = 2048
DK = 128
DV = 256
EPS = 1e-06
GATE_NORM = 16.0

NX, NY, NZ = 4, 4, 8
NT = 2 * NY
COPIES = 24
FAR_X = [2, 1, 3]
FAR_Y = [2, 1, 3]
FAR_Z = [4, 3, 5, 2, 6, 1, 7]
FAR_T = [4, 5, 2, 3, 6, 7, 1]
PLANE = [(dz, dx) for dz in FAR_Z + [0] for dx in FAR_X + [0] if (dz, dx) != (0, 0)]
LOADS = [(0, 0), (1, 1), (2, 0), (3, 0), (4, 0), (5, 0), (6, 0)]
LOADS += [(10, 3), (12, 2), (13, 2), (14, 2), (11, 4), (7, 5), (9, 6), (8, 7)]


def sigmoid(value):
    return 1.0 / (1.0 + jnp.exp(-value))


def halves(low, high):
    return jnp.concatenate([low, high], axis=1)


def as_pair(total):
    high = jnp.broadcast_to(total, (total.shape[0], 128)).astype(BF16).astype(F32)
    low = jnp.broadcast_to(total, (total.shape[0], 128)) - high
    lane = lax.broadcasted_iota(jnp.int32, high.shape, 1)
    return jnp.where(lane < 64, high, low).astype(BF16)


def of_pair(pair):
    return pair[:, 0:1] + pair[:, 64:65]


def packed_products(left, right, lane):
    width = left.shape[1] // 2
    stacked = jnp.concatenate([left[:, :width], left[:, width:]], axis=0)
    total = jnp.dot(stacked, right, preferred_element_type=F32)
    blocks = []
    for j in range(8):
        first = total[0:64, 128 * j : 128 * j + 128]
        second = total[64:128, 128 * j : 128 * j + 128]
        top = first[0:32] + pltpu.roll(second[0:32], 64, 1)
        bottom = pltpu.roll(first[32:64], 64, 1) + second[32:64]
        blocks.append(jnp.where(lane < 64, top, bottom))
    return blocks


def kernel(*refs):
    inputs, (result, new_state), refs = refs[:15], refs[15:17], refs[17:]
    held, refs = refs[:15], refs[15:]
    (
        tokens,
        norm_gain,
        w_query,
        w_key,
        w_value,
        w_gate,
        w_decay,
        log_decay,
        state,
        out_gain,
        w_out,
        mixer_gain,
        w_ffgate,
        w_ffup,
        w_down,
    ) = held
    (
        att,
        w_own,
        x_all,
        w_all,
        w_diag,
        part1,
        got1,
        mix,
        w_mix,
        part2,
        got2,
        attn_own,
        attn_all,
        tok_own,
        tok_all,
        middle,
        up_own,
        up_all,
        down_own,
        down_all,
        part3,
        got3,
        hid,
        part4,
        got4,
        res_own,
        res_all,
        send_sems,
        recv_sems,
        local_sems,
    ) = refs
    kv = lax.axis_index("kv")
    t = lax.axis_index("tp")
    z, x = lax.div(kv, NX), lax.rem(kv, NX)
    y, core = lax.div(t, 2), lax.rem(t, 2)

    def at_x(d):
        return lax.rem(x + d, NX)

    def at_z(d):
        return lax.rem(z + d, NZ)

    def at_t(d):
        return lax.rem(t + d, NT)

    counter = [0]
    unsent = []

    class Exchange:
        def __init__(self, size):
            self.number = counter[0]
            self.size = size
            counter[0] += 1
            unsent.append(self)

        def send(self, src, dst, peer):
            pltpu.make_async_remote_copy(
                src_ref=src,
                dst_ref=dst,
                send_sem=send_sems.at[self.number],
                recv_sem=recv_sems.at[self.number],
                device_id=peer,
                device_id_type=MESH,
            ).start()

        def wait(self, sems, size):
            pltpu.make_async_copy(size, size, sems.at[self.number]).wait()

        def arrive(self):
            self.wait(recv_sems, self.size)

        def leave(self):
            self.wait(send_sems, self.size)

    for i, sem in LOADS:
        pltpu.make_async_copy(inputs[i], held[i], local_sems.at[sem]).start()

    barrier = pltpu.get_barrier_semaphore()

    def greet(peer):
        pl.semaphore_signal(barrier, inc=1, device_id=peer, device_id_type=MESH)

    for dz, dx in PLANE:
        greet((at_z(dz) * NX + at_x(dx), t))
    for d in FAR_T:
        greet((kv, at_t(d)))
    for d in FAR_Z:
        greet((at_z(d) * NX + x, z))

    @pl.when(t != z)
    def _():
        greet((kv, z))

    def loaded(sem, size):
        pltpu.make_async_copy(size, size, local_sems.at[sem]).wait()

    with jax.named_scope("wait_first"):
        loaded(0, part1.at[0:22])
        loaded(1, norm_gain)
    square = (64, 64)
    row = lax.broadcasted_iota(jnp.int32, square, 0)
    column = lax.broadcasted_iota(jnp.int32, square, 1)
    gain = jnp.sum(
        jnp.where(row == column, jnp.broadcast_to(norm_gain[...].astype(F32), square), 0.0),
        axis=1,
        keepdims=True,
    )

    def gained(weight):
        return (weight[...].astype(F32) * gain).astype(BF16)

    w_own[0, :, 0:128] = gained(w_query)
    w_own[0, :, 128:256] = gained(w_key)
    w_own[1] = gained(w_value)
    w_own[2] = gained(w_gate)
    w_own[3, :, 0:128] = gained(w_decay)
    w_own[3, :, 128:256] = jnp.zeros((64, 128), BF16)
    own = jnp.concatenate([tokens[:, 0:256], tokens[:, 256:512]], axis=0).astype(F32)
    x_all[x] = jnp.transpose(own, (1, 0)).astype(BF16)
    w_all[x] = w_own[x]

    greetings = len(PLANE) + len(FAR_T) + len(FAR_Z)
    with jax.named_scope("wait_barrier"):
        pl.semaphore_wait(barrier, greetings + jnp.where(t != z, 1, 0))

    tile_z = w_mix.at[:, 0:128]

    def lanes_of(block):
        return pl.ds(pl.multiple_of(block * 128, 128), 128)

    ring_x = [(d, (z * NX + at_x(d), t)) for d in FAR_X]
    ring_z = [(d, (at_z(d) * NX + x, t)) for d in FAR_Z]
    ring_t = [(d, (kv, at_t(d))) for d in FAR_T]
    gather_w, gather_x = Exchange(w_all.at[0:3]), Exchange(x_all.at[0:3])
    for d, peer in ring_x:
        gather_w.send(w_own.at[at_x(d)], w_all.at[x], peer)
    for d, peer in ring_x:
        gather_x.send(x_all.at[x], x_all.at[x], peer)

    with jax.named_scope("wait_later"):
        loaded(3, w_out)
    out_rows = jnp.concatenate([w_out[:, 0:128], w_out[:, 128:256]], axis=0).astype(F32)
    w_mix[:, lanes_of(z)] = jnp.transpose(out_rows, (1, 0)).astype(BF16)
    mix_steps = []

    def mix_step(step):
        if step > 1:
            for exchange in mix_steps[-1]:
                exchange.arrive()
        exchanges = []
        for way in (1, -1):
            if step <= (4 if way > 0 else 3):
                lanes = lanes_of(at_z(NZ - way * (step - 1)))
                exchange = Exchange(tile_z)
                exchange.send(
                    w_mix.at[:, lanes], w_mix.at[:, lanes], (at_z(NZ + way) * NX + x, t)
                )
                exchanges.append(exchange)
        mix_steps.append(exchanges)

    mix_step(1)

    with jax.named_scope("wait_later"):
        loaded(2, up_all.at[0, 0:3])
        loaded(4, mixer_gain)
        loaded(5, log_decay)
        loaded(6, out_gain)
    gains = mixer_gain[...].astype(F32)
    units = jnp.transpose(
        jnp.concatenate([w_ffgate[...], w_ffup[...]], axis=0).astype(F32), (1, 0)
    )
    units = (units * jnp.concatenate([gains, gains], axis=1)).astype(BF16)
    down = w_down[...].astype(F32)
    down = jnp.concatenate([down, pltpu.roll(down, 768 - 48, 1)], axis=0)
    down = jnp.transpose(down, (1, 0)).astype(BF16)
    for j in range(NZ):
        up_own[j, 0] = units[96 * j : 96 * j + 48]
        up_own[j, 1] = units[96 * j + 48 : 96 * j + 96]
        down_own[j] = down[96 * j : 96 * j + 48]
    lanes_z = lanes_of(z)
    up_all[:, t, :, lanes_z] = up_own[z]
    down_all[t, :, lanes_z] = down_own[z]
    up_blocks = Exchange(up_own.at[0:7])
    for d, peer in ring_z:
        up_blocks.send(up_own.at[at_z(d)], up_all.at[:, t, :, lanes_z], peer)
    lane32 = lax.broadcasted_iota(jnp.int32, (32, 128), 1)
    rows = pl.multiple_of(64 * lax.rem(t, 4), 64)
    own = x_all[x, pl.ds(rows, 64), :].astype(F32)
    own = jnp.where(t < 4, own, pltpu.roll(own, 64, 1))
    tok_own[...] = jnp.where(lane32 < 64, own[0:32], pltpu.roll(own[32:64], 64, 1)).astype(BF16)
    tok_all[z] = tok_own[...]
    w_diag[...] = jnp.zeros(w_diag.shape, BF16)

    with jax.named_scope("wait_gather1"):
        gather_w.arrive()
        gather_x.arrive()
    mix_step(2)
    lane256 = lax.broadcasted_iota(jnp.int32, (256, 128), 1)
    total = jnp.zeros((256, 512), F32)
    top = jnp.zeros((256, 128), F32)
    bottom = jnp.zeros((256, 128), F32)
    for j in range(NX):
        w_diag[j, 0:64, 0:256] = w_all[j]
        w_diag[j, 64:128, 256:512] = w_all[j]
    for j in range(NX):
        block = x_all[j]
        total += jnp.dot(block, w_diag[j], preferred_element_type=F32)
        wide = block.astype(F32)
        wide = wide * wide
        top += jnp.where(lane256 < 64, wide, 0.0)
        bottom += jnp.where(lane256 < 64, 0.0, wide)
    has_sums = x == NX - 1
    for j in range(NZ):
        squares = as_pair(
            jnp.sum((top if j < 4 else bottom)[64 * (j % 4) : 64 * (j % 4) + 64], axis=1, keepdims=True)
        )
        for k in range(NX):
            rows = slice(64 * (j % 4) + 16 * k, 64 * (j % 4) + 16 * k + 16)
            first = 256 * (j // 4)
            part1[NX * j + k, :, 0:128] = total[rows, first : first + 128].astype(BF16)
            part1[NX * j + k, :, 128:256] = jnp.where(
                has_sums,
                squares[16 * k : 16 * k + 16].astype(F32),
                total[rows, first + 128 : first + 256],
            ).astype(BF16)
    got1[x * NZ + z] = part1[kv]
    scatter1 = Exchange(got1.at[0:31])
    for dz, dx in PLANE:
        peer = at_z(dz) * NX + at_x(dx)
        scatter1.send(part1.at[peer], got1.at[x * NZ + z], (peer, t))
    down_blocks = Exchange(down_own.at[0:7])
    for d, peer in ring_z:
        down_blocks.send(down_own.at[at_z(d)], down_all.at[t, :, lanes_z], peer)
    tok_blocks = Exchange(tok_all.at[0:7])
    for d, peer in ring_z:
        tok_blocks.send(tok_own, tok_all.at[z], peer)

    with jax.named_scope("wait_up_blocks"):
        up_blocks.arrive()
    partner = (kv, t + 1 - 2 * core)

    def along_y(d):
        return lax.rem(y + d, NY) * 2 + core

    up_y, up_core = Exchange(up_all.at[:, 0:3]), Exchange(up_all.at[:, 0:4])
    for d in FAR_Y:
        up_y.send(up_all.at[:, t], up_all.at[:, t], (kv, along_y(d)))
    up_core.send(up_all.at[:, t], up_all.at[:, t], partner)
    mix_step(3)

    with jax.named_scope("wait_scatter1"):
        scatter1.arrive()
    mix_step(4)
    proj = []
    for j in range(NX):
        total = got1[NZ * j].astype(F32)
        for k in range(1, NZ):
            total += got1[NZ * j + k].astype(F32)
        proj.append(total)
    loaded(7, state)

    inv = lax.rsqrt(of_pair(proj[3][:, 128:256]) / D + EPS)
    query = proj[0][:, 0:128] * (inv * DK ** (-0.5))
    keys = proj[0][:, 128:256] * inv
    values = proj[1] * inv
    gate = proj[2] * inv
    decay_pre = proj[3][:, 0:128] * inv
    log_sigmoid = jnp.minimum(decay_pre, 0.0) - jnp.log1p(jnp.exp(-jnp.abs(decay_pre)))
    decay = jnp.exp(log_sigmoid / GATE_NORM + log_decay[...])
    columns = jnp.transpose(
        jnp.concatenate([query, keys, decay, jnp.zeros((80, 128), F32)], axis=0), (1, 0)
    )
    for b in range(16):
        q_col = columns[:, b : b + 1]
        k_col = columns[:, 16 + b : 17 + b]
        a_col = columns[:, 32 + b : 33 + b]
        new = state[b] * a_col + k_col * values[b : b + 1, :]
        new_state[b] = new
        att[b : b + 1, :] = jnp.sum(new * q_col, axis=0, keepdims=True)
    attended = att[...]
    normed = (
        attended
        * lax.rsqrt(jnp.mean(attended * attended, axis=1, keepdims=True) + EPS)
        * out_gain[...]
    )
    mix[x] = (normed * (gate * sigmoid(gate))).astype(BF16)
    gather2 = Exchange(mix.at[0:3])
    for d, peer in ring_x:
        gather2.send(mix.at[x], mix.at[x], peer)

    with jax.named_scope("wait_mix_blocks"):
        for exchange in mix_steps[-1]:
            exchange.arrive()
    with jax.named_scope("wait_gather2"):
        gather2.arrive()
    mixed = mix[...].reshape(64, DV)
    for j, block in enumerate(packed_products(mixed, w_mix[...], lane32)):
        part2[j] = block.astype(BF16)
    got2[t] = part2[t]
    scatter2 = Exchange(got2.at[0:7])
    for d, peer in ring_t:
        scatter2.send(part2.at[at_t(d)], got2.at[t], peer)
    with jax.named_scope("wait_scatter2"):
        scatter2.arrive()
    total = got2[0].astype(F32)
    for j in range(1, NT):
        total += got2[j].astype(F32)
    attn_own[...] = total.astype(BF16)

    spread = Exchange(attn_all)
    diagonal = t == z
    for d in FAR_Z:
        spread.send(attn_own, attn_all.at[t], (at_z(d) * NX + x, z))

    @pl.when(jnp.logical_not(diagonal))
    def _():
        spread.send(attn_own, attn_all.at[t], (kv, z))

    @pl.when(diagonal)
    def _():
        attn_all[t] = attn_own[...]

    def spread_wait(sems):
        @pl.when(diagonal)
        def _():
            spread.wait(sems, attn_all.at[0:7])

        @pl.when(jnp.logical_not(diagonal))
        def _():
            spread.wait(sems, attn_all)

    with jax.named_scope("wait_down_blocks"):
        down_blocks.arrive()
    down_y, down_core = Exchange(down_all.at[0:3]), Exchange(down_all.at[0:4])
    for d in FAR_Y:
        down_y.send(down_all.at[t], down_all.at[t], (kv, along_y(d)))
    with jax.named_scope("wait_up_y"):
        up_y.arrive()
    for d in range(1, NY):
        other = along_y(d)
        up_core.send(up_all.at[:, other], up_all.at[:, other], partner)
    down_core.send(down_all.at[t], down_all.at[t], partner)

    with jax.named_scope("wait_tok_blocks"):
        tok_blocks.arrive()
    with jax.named_scope("wait_spread"):
        spread_wait(recv_sems)

    top = jnp.zeros((32, 128), F32)
    bottom = jnp.zeros((32, 128), F32)
    pieces = []
    for j in range(NZ):
        block = (tok_all[j].astype(F32) + attn_all[j].astype(F32)).astype(BF16)
        middle[j] = block
        wide = block.astype(F32)
        low = jnp.where(lane32 < 64, wide, 0.0)
        high = jnp.where(lane32 < 64, 0.0, wide)
        top += low * low
        bottom += high * high
        pieces.append(
            jnp.concatenate(
                [low, pltpu.roll(high, 64, 1), pltpu.roll(low, 64, 1), high], axis=0
            ).astype(BF16)
        )
    left = jnp.concatenate(pieces, axis=1)
    squares = as_pair(
        jnp.concatenate(
            [jnp.sum(top, axis=1, keepdims=True), jnp.sum(bottom, axis=1, keepdims=True)], axis=0
        )
    )
    with jax.named_scope("wait_up_core"):
        up_core.arrive()
    weights = up_all[...].reshape(NT * 96, 1024)
    terms = lax.dot_general(
        left, weights, (((1,), (1,)), ((), ())), preferred_element_type=F32
    )
    for j in range(NX):
        rows = slice(16 * j, 16 * j + 16)
        part3[j, :, 0:768] = terms[rows].astype(BF16)
        part3[j, :, 768:1536] = terms[64 + 16 * j : 80 + 16 * j].astype(BF16)
        part3[j, :, 1536:1664] = squares[rows]
    got3[x] = part3[x]
    scatter3 = Exchange(got3.at[0:3])
    for d, peer in ring_x:
        scatter3.send(part3.at[at_x(d)], got3.at[x], peer)
    with jax.named_scope("wait_down_y"):
        down_y.arrive()
    for d in range(1, NY):
        other = along_y(d)
        down_core.send(down_all.at[other], down_all.at[other], partner)
    with jax.named_scope("wait_scatter3"):
        scatter3.arrive()
    total = got3[0].astype(F32)
    for j in range(1, NX):
        total += got3[j].astype(F32)
    inv = lax.rsqrt(of_pair(total[:, 1536:1664]) / D + EPS)
    gate = total[:, 0:768] * inv
    hid[x] = (gate * sigmoid(gate) * (total[:, 768:1536] * inv)).astype(BF16)
    gather3 = Exchange(hid.at[0:3])
    for d, peer in ring_x:
        gather3.send(hid.at[x], hid.at[x], peer)
    with jax.named_scope("wait_down_core"):
        down_core.arrive()
    with jax.named_scope("wait_gather3"):
        gather3.arrive()

    hidden = hid[...].reshape(64, 768)
    weights = down_all[...].reshape(NT * 48, 1024)
    for j, block in enumerate(packed_products(hidden, weights, lane32)):
        part4[j] = block.astype(BF16)
    got4[z] = part4[z]
    scatter4 = Exchange(got4.at[0:7])
    for d, peer in ring_z:
        scatter4.send(part4.at[at_z(d)], got4.at[z], peer)
    with jax.named_scope("wait_scatter4"):
        scatter4.arrive()
    total = got4[0].astype(F32)
    for j in range(1, NZ):
        total += got4[j].astype(F32)
    res_own[...] = (middle[z].astype(F32) + total).astype(BF16)
    res_all[t] = res_own[...]
    gather4 = Exchange(res_all.at[0:7])
    for d, peer in ring_t:
        gather4.send(res_own, res_all.at[t], peer)
    with jax.named_scope("wait_gather4"):
        gather4.arrive()
    rows = []
    for j in range(NT):
        block = res_all[j].astype(F32)
        rows += [block, pltpu.roll(block, 64, 1)]
    rows = jnp.concatenate(rows, axis=0)
    result[...] = jnp.transpose(rows, (1, 0))[0:64].astype(BF16)
    with jax.named_scope("wait_sends"):
        for exchange in unsent:
            if exchange is spread:
                spread_wait(send_sems)
            else:
                exchange.leave()

def finish(result_in, state_in, result_out, state_out, sems):
    result = pltpu.make_async_copy(result_in, result_out, sems.at[0])
    states = pltpu.make_async_copy(state_in, state_out, sems.at[1])
    parts = [pl.ds(2 * i, 2) for i in range(8)]
    result.start()
    for part in parts:
        pltpu.make_async_copy(state_in.at[part], state_out.at[part], sems.at[1]).start()
    result.wait()
    states.wait()


def body(
    tokens,
    norm_gain,
    w_query,
    w_key,
    w_value,
    w_gate,
    w_decay,
    log_decay,
    state,
    out_gain,
    w_out,
    mixer_gain,
    w_ffgate,
    w_ffup,
    w_down,
):
    vmem = pl.BlockSpec(memory_space=pltpu.VMEM)
    hbm = pl.BlockSpec(memory_space=pltpu.HBM)
    shape = state.shape
    arguments = (
        tokens.T,
        norm_gain.reshape(1, 64),
        w_query,
        w_key,
        w_value,
        w_gate,
        w_decay,
        log_decay,
        state.reshape(shape[0], DK, DV),
        out_gain.reshape(1, DV),
        w_out.T,
        mixer_gain.reshape(1, 64),
        w_ffgate,
        w_ffup,
        w_down.T,
    )
    arguments = [pltpu.with_memory_space_constraint(value, pltpu.HBM) for value in arguments]
    result, new_state = pl.pallas_call(
        kernel,
        out_shape=(
            pltpu.VMEM((64, 512), BF16),
            pltpu.VMEM((shape[0], DK, DV), F32),
        ),
        in_specs=[hbm] * 15,
        out_specs=(vmem, vmem),
        scratch_shapes=[pltpu.VMEM(value.shape, value.dtype) for value in arguments]
        + [
            pltpu.VMEM((16, DV), F32),
            pltpu.VMEM((NX, 64, 256), BF16),
            pltpu.VMEM((NX, 256, 128), BF16),
            pltpu.VMEM((NX, 64, 256), BF16),
            pltpu.VMEM((NX, 128, 512), BF16),
            pltpu.VMEM((NZ * NX, 16, 256), BF16),
            pltpu.VMEM((NX * NZ, 16, 256), BF16),
            pltpu.VMEM((NX, 16, 256), BF16),
            pltpu.VMEM((128, 1024), BF16),
            pltpu.VMEM((NT, 32, 128), BF16),
            pltpu.VMEM((NT, 32, 128), BF16),
            pltpu.VMEM((32, 128), BF16),
            pltpu.VMEM((NT, 32, 128), BF16),
            pltpu.VMEM((32, 128), BF16),
            pltpu.VMEM((NZ, 32, 128), BF16),
            pltpu.VMEM((NZ, 32, 128), BF16),
            pltpu.VMEM((NZ, 2, 48, 128), BF16),
            pltpu.VMEM((2, NT, 48, 1024), BF16),
            pltpu.VMEM((NZ, 48, 128), BF16),
            pltpu.VMEM((NT, 48, 1024), BF16),
            pltpu.VMEM((NX, 16, 1664), BF16),
            pltpu.VMEM((NX, 16, 1664), BF16),
            pltpu.VMEM((NX, 16, 768), BF16),
            pltpu.VMEM((NZ, 32, 128), BF16),
            pltpu.VMEM((NZ, 32, 128), BF16),
            pltpu.VMEM((32, 128), BF16),
            pltpu.VMEM((NT, 32, 128), BF16),
            pltpu.SemaphoreType.DMA((COPIES,)),
            pltpu.SemaphoreType.DMA((COPIES,)),
            pltpu.SemaphoreType.DMA((8,)),
        ],
        compiler_params=pltpu.CompilerParams(
            collective_id=0, has_side_effects=True, vmem_limit_bytes=40 * 1024 * 1024
        ),
    )(*arguments)
    result, new_state = pl.pallas_call(
        finish,
        out_shape=(
            jax.ShapeDtypeStruct((64, 512), BF16),
            jax.ShapeDtypeStruct((shape[0], DK, DV), F32),
        ),
        in_specs=[vmem, vmem],
        out_specs=(hbm, hbm),
        scratch_shapes=[pltpu.SemaphoreType.DMA((2,))],
        compiler_params=pltpu.CompilerParams(vmem_limit_bytes=8 * 1024 * 1024),
    )(result, new_state)
    return (result.T, new_state.reshape(shape))


def solution(mesh):
    return jax.shard_map(
        body,
        mesh=mesh,
        in_specs=(
            P(None, "kv"),
            P("kv"),
            P("kv", "tp"),
            P("kv", "tp"),
            P("kv", "tp"),
            P("kv", "tp"),
            P("kv", "tp"),
            P("kv", "tp"),
            P("kv", "tp", None, None),
            P(),
            P("tp", "kv"),
            P("kv"),
            P("kv", "tp"),
            P("kv", "tp"),
            P("tp", "kv"),
        ),
        out_specs=(P(None, "kv"), P("kv", "tp", None, None)),
        check_vma=False,
    )
```

```python
import functools

import jax
import jax.numpy as jnp
from jax import lax
from jax.experimental import pallas as pl
from jax.experimental.pallas import tpu as pltpu
from jax.sharding import PartitionSpec as P

MESH = pl.DeviceIdType.MESH
F32 = jnp.float32
BF16 = jnp.bfloat16

D = 2048
DK = 128
DV = 256
EPS = 1e-06
GATE_NORM = 16.0

NX, NY, NZ = 4, 4, 8
NT = 2 * NY
COPIES = 27
FAR_X = [2, 1, 3]
FAR_Y = [2, 1, 3]
FAR_Z = [4, 3, 5, 2, 6, 1, 7]
FAR_T = [4, 5, 2, 3, 6, 7, 1]
PLANE = [(dz, dx) for dz in FAR_Z + [0] for dx in FAR_X + [0] if (dz, dx) != (0, 0)]
LOADS = [(0, 0), (1, 1), (2, 0), (3, 0), (4, 0), (5, 0), (6, 0)]
LOADS += [(10, 3), (12, 2), (13, 2), (14, 2), (11, 4), (7, 5), (9, 6), (8, 7)]


def sigmoid(value):
    return 1.0 / (1.0 + jnp.exp(-value))


def halves(low, high):
    return jnp.concatenate([low, high], axis=1)


def as_pair(total):
    high = jnp.broadcast_to(total, (total.shape[0], 128)).astype(BF16).astype(F32)
    low = jnp.broadcast_to(total, (total.shape[0], 128)) - high
    lane = lax.broadcasted_iota(jnp.int32, high.shape, 1)
    return jnp.where(lane < 64, high, low).astype(BF16)


def of_pair(pair):
    return pair[:, 0:1] + pair[:, 64:65]


def packed_products(first, second, lane):
    blocks = []
    for j in range(8):
        low = first[:, 128 * j : 128 * j + 128]
        high = second[:, 128 * j : 128 * j + 128]
        top = low[0:32] + pltpu.roll(high[0:32], 64, 1)
        bottom = pltpu.roll(low[32:64], 64, 1) + high[32:64]
        blocks.append(jnp.where(lane < 64, top, bottom))
    return blocks


def kernel(*refs):
    inputs, (result, new_state), refs = refs[:15], refs[15:17], refs[17:]
    held, refs = refs[:15], refs[15:]
    (
        tokens,
        norm_gain,
        w_query,
        w_key,
        w_value,
        w_gate,
        w_decay,
        log_decay,
        state,
        out_gain,
        w_out,
        mixer_gain,
        w_ffgate,
        w_ffup,
        w_down,
    ) = held
    (
        att,
        w_own,
        x_all,
        w_all,
        w_diag,
        part1,
        got1,
        mix,
        w_mix,
        part2,
        got2,
        attn_own,
        attn_all,
        tok_own,
        tok_all,
        middle,
        up_own,
        up_all,
        down_own,
        down_all,
        part3a,
        got3a,
        part3b,
        got3b,
        hid,
        part4,
        got4,
        res_own,
        res_all,
        send_sems,
        recv_sems,
        local_sems,
    ) = refs
    kv = lax.axis_index("kv")
    t = lax.axis_index("tp")
    z, x = lax.div(kv, NX), lax.rem(kv, NX)
    y, core = lax.div(t, 2), lax.rem(t, 2)

    def at_x(d):
        return lax.rem(x + d, NX)

    def at_z(d):
        return lax.rem(z + d, NZ)

    def at_t(d):
        return lax.rem(t + d, NT)

    counter = [0]
    unsent = []

    class Exchange:
        def __init__(self, size):
            self.number = counter[0]
            self.size = size
            counter[0] += 1
            unsent.append(self)

        def send(self, src, dst, peer):
            pltpu.make_async_remote_copy(
                src_ref=src,
                dst_ref=dst,
                send_sem=send_sems.at[self.number],
                recv_sem=recv_sems.at[self.number],
                device_id=peer,
                device_id_type=MESH,
            ).start()

        def wait(self, sems, size):
            pltpu.make_async_copy(size, size, sems.at[self.number]).wait()

        def arrive(self):
            self.wait(recv_sems, self.size)

        def leave(self):
            self.wait(send_sems, self.size)

    for i, sem in LOADS:
        pltpu.make_async_copy(inputs[i], held[i], local_sems.at[sem]).start()

    barrier = pltpu.get_barrier_semaphore()

    def greet(peer):
        pl.semaphore_signal(barrier, inc=1, device_id=peer, device_id_type=MESH)

    for dz, dx in PLANE:
        greet((at_z(dz) * NX + at_x(dx), t))
    for d in FAR_T:
        greet((kv, at_t(d)))
    for d in FAR_Z:
        greet((at_z(d) * NX + x, z))

    @pl.when(t != z)
    def _():
        greet((kv, z))

    def loaded(sem, size):
        pltpu.make_async_copy(size, size, local_sems.at[sem]).wait()

    with jax.named_scope("wait_first"):
        loaded(0, part1.at[0:22])
        loaded(1, norm_gain)
    square = (64, 64)
    row = lax.broadcasted_iota(jnp.int32, square, 0)
    column = lax.broadcasted_iota(jnp.int32, square, 1)
    gain = jnp.sum(
        jnp.where(row == column, jnp.broadcast_to(norm_gain[...].astype(F32), square), 0.0),
        axis=1,
        keepdims=True,
    )

    def gained(weight):
        return (weight[...].astype(F32) * gain).astype(BF16)

    w_own[0, :, 0:128] = gained(w_query)
    w_own[0, :, 128:256] = gained(w_key)
    w_own[1] = gained(w_value)
    w_own[2] = gained(w_gate)
    w_own[3, :, 0:128] = gained(w_decay)
    w_own[3, :, 128:256] = jnp.zeros((64, 128), BF16)
    own = jnp.concatenate([tokens[:, 0:256], tokens[:, 256:512]], axis=0).astype(F32)
    x_all[x] = jnp.transpose(own, (1, 0)).astype(BF16).reshape(4, 64, 128)
    w_all[x] = w_own[x]

    greetings = len(PLANE) + len(FAR_T) + len(FAR_Z)
    with jax.named_scope("wait_barrier"):
        pl.semaphore_wait(barrier, greetings + jnp.where(t != z, 1, 0))

    tile_z = w_mix.at[:, 0:128]

    def lanes_of(block):
        return pl.ds(pl.multiple_of(block * 128, 128), 128)

    ring_x = [(d, (z * NX + at_x(d), t)) for d in FAR_X]
    ring_z = [(d, (at_z(d) * NX + x, t)) for d in FAR_Z]
    ring_t = [(d, (kv, at_t(d))) for d in FAR_T]
    gather_w = Exchange(w_all.at[0:3])
    gather_x = [Exchange(x_all.at[0:3, 0:2]) for half in range(2)]
    halves_z = [[lax.rem(z + d, 4) for d in steps] for steps in ((1, 2), (0, 3))]
    for d, peer in ring_x:
        gather_w.send(w_own.at[at_x(d)], w_all.at[x], peer)
    for half in range(2):
        for d, peer in ring_x:
            for r in halves_z[half]:
                gather_x[half].send(x_all.at[x, r], x_all.at[x, r], peer)

    with jax.named_scope("wait_later"):
        loaded(3, w_out)
    out_rows = jnp.concatenate([w_out[:, 0:128], w_out[:, 128:256]], axis=0).astype(F32)
    w_mix[:, lanes_of(z)] = jnp.transpose(out_rows, (1, 0)).astype(BF16)
    mix_steps = []

    def mix_step(step):
        if step > 1:
            for exchange in mix_steps[-1]:
                exchange.arrive()
        exchanges = []
        for way in (1, -1):
            if step <= (4 if way > 0 else 3):
                lanes = lanes_of(at_z(NZ - way * (step - 1)))
                exchange = Exchange(tile_z)
                exchange.send(
                    w_mix.at[:, lanes], w_mix.at[:, lanes], (at_z(NZ + way) * NX + x, t)
                )
                exchanges.append(exchange)
        mix_steps.append(exchanges)

    mix_step(1)

    with jax.named_scope("wait_later"):
        loaded(2, up_all.at[0, 0:3])
        loaded(4, mixer_gain)
        loaded(5, log_decay)
        loaded(6, out_gain)
    gains = mixer_gain[...].astype(F32)
    units = jnp.transpose(
        jnp.concatenate([w_ffgate[...], w_ffup[...]], axis=0).astype(F32), (1, 0)
    )
    units = (units * jnp.concatenate([gains, gains], axis=1)).astype(BF16)
    down = w_down[...].astype(F32)
    down = jnp.concatenate([down, pltpu.roll(down, 768 - 48, 1)], axis=0)
    down = jnp.transpose(down, (1, 0)).astype(BF16)
    for j in range(NZ):
        up_own[j, 0] = units[96 * j : 96 * j + 48]
        up_own[j, 1] = units[96 * j + 48 : 96 * j + 96]
        down_own[j] = down[96 * j : 96 * j + 48]
    lanes_z = lanes_of(z)
    up_all[:, t, :, lanes_z] = up_own[z]
    down_all[t, :, lanes_z] = down_own[z]
    up_blocks = Exchange(up_own.at[0:7])
    for d, peer in ring_z:
        up_blocks.send(up_own.at[at_z(d)], up_all.at[:, t, :, lanes_z], peer)
    lane32 = lax.broadcasted_iota(jnp.int32, (32, 128), 1)
    own = x_all[x, lax.rem(t, 4)].astype(F32)
    own = jnp.where(t < 4, own, pltpu.roll(own, 64, 1))
    tok_own[...] = jnp.where(lane32 < 64, own[0:32], pltpu.roll(own[32:64], 64, 1)).astype(BF16)
    tok_all[z] = tok_own[...]
    w_diag[...] = jnp.zeros(w_diag.shape, BF16)

    with jax.named_scope("wait_mix_step"):
        mix_step(2)

    with jax.named_scope("wait_gather1_w"):
        gather_w.arrive()
    for j in range(NX):
        w_diag[j, 0:64, 0:256] = w_all[j]
        w_diag[j, 64:128, 256:512] = w_all[j]
    lane128 = lax.broadcasted_iota(jnp.int32, (128, 128), 1)
    has_sums = x == NX - 1
    scatter1 = Exchange(got1.at[0:31])
    for half, (blocks, steps) in enumerate(zip(halves_z, ([5, 2, 6, 1], [4, 3, 7, 0]))):
        with jax.named_scope(f"wait_gather1_{half}"):
            gather_x[half].arrive()
        total = jnp.zeros((128, 512), F32)
        sums = [jnp.zeros((128, 128), F32)] * 2
        for j in range(NX):
            block = jnp.concatenate([x_all[j, r] for r in blocks], axis=0)
            total += jnp.dot(block, w_diag[j], preferred_element_type=F32)
            wide = block.astype(F32)
            wide = wide * wide
            sums[0] += jnp.where(lane128 < 64, wide, 0.0)
            sums[1] += jnp.where(lane128 < 64, 0.0, wide)
        for i, r in enumerate(blocks):
            for side in range(2):
                squares = as_pair(
                    jnp.sum(sums[side][64 * i : 64 * i + 64], axis=1, keepdims=True)
                )
                first = 256 * side
                for k in range(NX):
                    rows = slice(64 * i + 16 * k, 64 * i + 16 * k + 16)
                    owner = NX * (r + 4 * side) + k
                    part1[owner, :, 0:128] = total[rows, first : first + 128].astype(BF16)
                    part1[owner, :, 128:256] = jnp.where(
                        has_sums,
                        squares[16 * k : 16 * k + 16].astype(F32),
                        total[rows, first + 128 : first + 256],
                    ).astype(BF16)
        for dz in steps:
            for dx in FAR_X + [0]:
                if (dz, dx) != (0, 0):
                    peer = at_z(dz) * NX + at_x(dx)
                    scatter1.send(part1.at[peer], got1.at[x * NZ + z], (peer, t))
    got1[x * NZ + z] = part1[kv]

    with jax.named_scope("wait_up_blocks"):
        up_blocks.arrive()
    partner = (kv, t + 1 - 2 * core)

    def along_y(d):
        return lax.rem(y + d, NY) * 2 + core

    up_y, up_core = Exchange(up_all.at[:, 0:3]), Exchange(up_all.at[:, 0:4])
    for d in FAR_Y:
        up_y.send(up_all.at[:, t], up_all.at[:, t], (kv, along_y(d)))
    up_core.send(up_all.at[:, t], up_all.at[:, t], partner)
    mix_step(3)

    with jax.named_scope("wait_scatter1"):
        scatter1.arrive()
    mix_step(4)
    proj = []
    for j in range(NX):
        total = got1[NZ * j].astype(F32)
        for k in range(1, NZ):
            total += got1[NZ * j + k].astype(F32)
        proj.append(total)
    loaded(7, state)

    inv = lax.rsqrt(of_pair(proj[3][:, 128:256]) / D + EPS)
    query = proj[0][:, 0:128] * (inv * DK ** (-0.5))
    keys = proj[0][:, 128:256] * inv
    values = proj[1] * inv
    gate = proj[2] * inv
    decay_pre = proj[3][:, 0:128] * inv
    log_sigmoid = jnp.minimum(decay_pre, 0.0) - jnp.log1p(jnp.exp(-jnp.abs(decay_pre)))
    decay = jnp.exp(log_sigmoid / GATE_NORM + log_decay[...])
    columns = jnp.transpose(
        jnp.concatenate([query * decay, keys, decay, jnp.zeros((80, 128), F32)], axis=0), (1, 0)
    )
    for b in range(16):
        att[b : b + 1, :] = jnp.sum(state[b] * columns[:, b : b + 1], axis=0, keepdims=True)
    attended = att[...] + jnp.sum(query * keys, axis=1, keepdims=True) * values
    normed = (
        attended
        * lax.rsqrt(jnp.mean(attended * attended, axis=1, keepdims=True) + EPS)
        * out_gain[...]
    )
    mix[x] = (normed * (gate * sigmoid(gate))).astype(BF16)
    gather2 = Exchange(mix.at[0:3])
    for d, peer in ring_x:
        gather2.send(mix.at[x], mix.at[x], peer)
    down_blocks = Exchange(down_own.at[0:7])
    for d, peer in ring_z:
        down_blocks.send(down_own.at[at_z(d)], down_all.at[t, :, lanes_z], peer)
    tok_blocks = Exchange(tok_all.at[0:7])
    for d, peer in ring_z:
        tok_blocks.send(tok_own, tok_all.at[z], peer)
    for b in range(16):
        k_col = columns[:, 16 + b : 17 + b]
        a_col = columns[:, 32 + b : 33 + b]
        new_state[b] = state[b] * a_col + k_col * values[b : b + 1, :]

    with jax.named_scope("wait_mix_blocks"):
        for exchange in mix_steps[-1]:
            exchange.arrive()
    with jax.named_scope("wait_gather2"):
        gather2.arrive()
    mixed = mix[...].reshape(64, DV)
    stacked = jnp.concatenate([mixed[:, 0:128], mixed[:, 128:256]], axis=0)
    total = jnp.dot(stacked, w_mix[...], preferred_element_type=F32)
    for j, block in enumerate(packed_products(total[0:64], total[64:128], lane32)):
        part2[j] = block.astype(BF16)
    got2[t] = part2[t]
    scatter2 = Exchange(got2.at[0:7])
    for d, peer in ring_t:
        scatter2.send(part2.at[at_t(d)], got2.at[t], peer)
    with jax.named_scope("wait_scatter2"):
        scatter2.arrive()
    total = got2[0].astype(F32)
    for j in range(1, NT):
        total += got2[j].astype(F32)
    attn_own[...] = total.astype(BF16)

    spread = Exchange(attn_all)
    diagonal = t == z
    for d in FAR_Z:
        spread.send(attn_own, attn_all.at[t], (at_z(d) * NX + x, z))

    @pl.when(jnp.logical_not(diagonal))
    def _():
        spread.send(attn_own, attn_all.at[t], (kv, z))

    @pl.when(diagonal)
    def _():
        attn_all[t] = attn_own[...]

    def spread_wait(sems):
        @pl.when(diagonal)
        def _():
            spread.wait(sems, attn_all.at[0:7])

        @pl.when(jnp.logical_not(diagonal))
        def _():
            spread.wait(sems, attn_all)

    with jax.named_scope("wait_down_blocks"):
        down_blocks.arrive()
    down_y, down_core = Exchange(down_all.at[0:3]), Exchange(down_all.at[0:4])
    for d in FAR_Y:
        down_y.send(down_all.at[t], down_all.at[t], (kv, along_y(d)))
    with jax.named_scope("wait_up_y"):
        up_y.arrive()
    for d in range(1, NY):
        other = along_y(d)
        up_core.send(up_all.at[:, other], up_all.at[:, other], partner)
    down_core.send(down_all.at[t], down_all.at[t], partner)

    with jax.named_scope("wait_tok_blocks"):
        tok_blocks.arrive()
    with jax.named_scope("wait_spread"):
        spread_wait(recv_sems)

    top = jnp.zeros((32, 128), F32)
    bottom = jnp.zeros((32, 128), F32)
    pieces = []
    for j in range(NZ):
        block = (tok_all[j].astype(F32) + attn_all[j].astype(F32)).astype(BF16)
        middle[j] = block
        wide = block.astype(F32)
        low = jnp.where(lane32 < 64, wide, 0.0)
        high = jnp.where(lane32 < 64, 0.0, wide)
        top += low * low
        bottom += high * high
        pieces.append(
            jnp.concatenate(
                [low, pltpu.roll(high, 64, 1), pltpu.roll(low, 64, 1), high], axis=0
            ).astype(BF16)
        )
    left = jnp.concatenate(pieces, axis=1)
    squares = as_pair(
        jnp.concatenate(
            [jnp.sum(top, axis=1, keepdims=True), jnp.sum(bottom, axis=1, keepdims=True)], axis=0
        )
    )
    with jax.named_scope("wait_up_core"):
        up_core.arrive()
    parts3, gots3 = (part3a, part3b), (got3a, got3b)
    scatter3 = [Exchange(got3.at[0:3]) for got3 in gots3]
    for half, (part3, got3) in enumerate(zip(parts3, gots3)):
        terms = lax.dot_general(
            left,
            up_all[half].reshape(384, 1024),
            (((1,), (1,)), ((), ())),
            preferred_element_type=F32,
        )
        for j in range(NX):
            rows = slice(16 * j, 16 * j + 16)
            part3[j, :, 0:384] = terms[rows].astype(BF16)
            part3[j, :, 384:768] = terms[64 + 16 * j : 80 + 16 * j].astype(BF16)
            if half == 0:
                part3[j, :, 768:896] = squares[rows]
        got3[x] = part3[x]
        for d, peer in ring_x:
            scatter3[half].send(part3.at[at_x(d)], got3.at[x], peer)
    with jax.named_scope("wait_down_y"):
        down_y.arrive()
    for d in range(1, NY):
        other = along_y(d)
        down_core.send(down_all.at[other], down_all.at[other], partner)
    gather3 = [Exchange(hid.at[half, 0:3]) for half in range(2)]
    inv = None
    for half, got3 in enumerate(gots3):
        with jax.named_scope(f"wait_scatter3_{half}"):
            scatter3[half].arrive()
        total = got3[0].astype(F32)
        for j in range(1, NX):
            total += got3[j].astype(F32)
        if half == 0:
            inv = lax.rsqrt(of_pair(total[:, 768:896]) / D + EPS)
        gate = total[:, 0:384] * inv
        hid[half, x] = (gate * sigmoid(gate) * (total[:, 384:768] * inv)).astype(BF16)
        for d, peer in ring_x:
            gather3[half].send(hid.at[half, x], hid.at[half, x], peer)
    with jax.named_scope("wait_down_core"):
        down_core.arrive()

    weights = down_all[...].reshape(NT * 48, 1024)
    products = []
    for half in range(2):
        with jax.named_scope(f"wait_gather3_{half}"):
            gather3[half].arrive()
        products.append(
            jnp.dot(hid[half].reshape(64, 384), weights, preferred_element_type=F32)
        )
    for j, block in enumerate(packed_products(*products, lane32)):
        part4[j] = block.astype(BF16)
    got4[z] = part4[z]
    scatter4 = Exchange(got4.at[0:7])
    for d, peer in ring_z:
        scatter4.send(part4.at[at_z(d)], got4.at[z], peer)
    with jax.named_scope("wait_scatter4"):
        scatter4.arrive()
    total = got4[0].astype(F32)
    for j in range(1, NZ):
        total += got4[j].astype(F32)
    res_own[...] = (middle[z].astype(F32) + total).astype(BF16)
    res_all[t] = res_own[...]
    gather4 = Exchange(res_all.at[0:7])
    for d, peer in ring_t:
        gather4.send(res_own, res_all.at[t], peer)
    with jax.named_scope("wait_gather4"):
        gather4.arrive()
    rows = []
    for j in range(NT):
        block = res_all[j].astype(F32)
        rows += [block, pltpu.roll(block, 64, 1)]
    rows = jnp.concatenate(rows, axis=0)
    result[...] = jnp.transpose(rows, (1, 0))[0:64].astype(BF16)
    with jax.named_scope("wait_sends"):
        for exchange in unsent:
            if exchange is spread:
                spread_wait(send_sems)
            else:
                exchange.leave()

def finish(result_in, state_in, result_out, state_out, sems):
    result = pltpu.make_async_copy(result_in, result_out, sems.at[0])
    states = pltpu.make_async_copy(state_in, state_out, sems.at[1])
    parts = [pl.ds(2 * i, 2) for i in range(8)]
    result.start()
    for part in parts:
        pltpu.make_async_copy(state_in.at[part], state_out.at[part], sems.at[1]).start()
    result.wait()
    states.wait()


def body(
    tokens,
    norm_gain,
    w_query,
    w_key,
    w_value,
    w_gate,
    w_decay,
    log_decay,
    state,
    out_gain,
    w_out,
    mixer_gain,
    w_ffgate,
    w_ffup,
    w_down,
):
    vmem = pl.BlockSpec(memory_space=pltpu.VMEM)
    hbm = pl.BlockSpec(memory_space=pltpu.HBM)
    shape = state.shape
    arguments = (
        tokens.T,
        norm_gain.reshape(1, 64),
        w_query,
        w_key,
        w_value,
        w_gate,
        w_decay,
        log_decay,
        state.reshape(shape[0], DK, DV),
        out_gain.reshape(1, DV),
        w_out.T,
        mixer_gain.reshape(1, 64),
        w_ffgate,
        w_ffup,
        w_down.T,
    )
    arguments = [pltpu.with_memory_space_constraint(value, pltpu.HBM) for value in arguments]
    result, new_state = pl.pallas_call(
        kernel,
        out_shape=(
            pltpu.VMEM((64, 512), BF16),
            pltpu.VMEM((shape[0], DK, DV), F32),
        ),
        in_specs=[hbm] * 15,
        out_specs=(vmem, vmem),
        scratch_shapes=[pltpu.VMEM(value.shape, value.dtype) for value in arguments]
        + [
            pltpu.VMEM((16, DV), F32),
            pltpu.VMEM((NX, 64, 256), BF16),
            pltpu.VMEM((NX, 4, 64, 128), BF16),
            pltpu.VMEM((NX, 64, 256), BF16),
            pltpu.VMEM((NX, 128, 512), BF16),
            pltpu.VMEM((NZ * NX, 16, 256), BF16),
            pltpu.VMEM((NX * NZ, 16, 256), BF16),
            pltpu.VMEM((NX, 16, 256), BF16),
            pltpu.VMEM((128, 1024), BF16),
            pltpu.VMEM((NT, 32, 128), BF16),
            pltpu.VMEM((NT, 32, 128), BF16),
            pltpu.VMEM((32, 128), BF16),
            pltpu.VMEM((NT, 32, 128), BF16),
            pltpu.VMEM((32, 128), BF16),
            pltpu.VMEM((NZ, 32, 128), BF16),
            pltpu.VMEM((NZ, 32, 128), BF16),
            pltpu.VMEM((NZ, 2, 48, 128), BF16),
            pltpu.VMEM((2, NT, 48, 1024), BF16),
            pltpu.VMEM((NZ, 48, 128), BF16),
            pltpu.VMEM((NT, 48, 1024), BF16),
            pltpu.VMEM((NX, 16, 896), BF16),
            pltpu.VMEM((NX, 16, 896), BF16),
            pltpu.VMEM((NX, 16, 768), BF16),
            pltpu.VMEM((NX, 16, 768), BF16),
            pltpu.VMEM((2, NX, 16, 384), BF16),
            pltpu.VMEM((NZ, 32, 128), BF16),
            pltpu.VMEM((NZ, 32, 128), BF16),
            pltpu.VMEM((32, 128), BF16),
            pltpu.VMEM((NT, 32, 128), BF16),
            pltpu.SemaphoreType.DMA((COPIES,)),
            pltpu.SemaphoreType.DMA((COPIES,)),
            pltpu.SemaphoreType.DMA((8,)),
        ],
        compiler_params=pltpu.CompilerParams(
            collective_id=0, has_side_effects=True, vmem_limit_bytes=40 * 1024 * 1024
        ),
    )(*arguments)
    result, new_state = pl.pallas_call(
        finish,
        out_shape=(
            jax.ShapeDtypeStruct((64, 512), BF16),
            jax.ShapeDtypeStruct((shape[0], DK, DV), F32),
        ),
        in_specs=[vmem, vmem],
        out_specs=(hbm, hbm),
        scratch_shapes=[pltpu.SemaphoreType.DMA((2,))],
        compiler_params=pltpu.CompilerParams(vmem_limit_bytes=8 * 1024 * 1024),
    )(result, new_state)
    return (result.T, new_state.reshape(shape))


def solution(mesh):
    return jax.shard_map(
        body,
        mesh=mesh,
        in_specs=(
            P(None, "kv"),
            P("kv"),
            P("kv", "tp"),
            P("kv", "tp"),
            P("kv", "tp"),
            P("kv", "tp"),
            P("kv", "tp"),
            P("kv", "tp"),
            P("kv", "tp", None, None),
            P(),
            P("tp", "kv"),
            P("kv"),
            P("kv", "tp"),
            P("kv", "tp"),
            P("tp", "kv"),
        ),
        out_specs=(P(None, "kv"), P("kv", "tp", None, None)),
        check_vma=False,
    )
```

```python
import functools

import jax
import jax.numpy as jnp
from jax import lax
from jax.experimental import pallas as pl
from jax.experimental.pallas import tpu as pltpu
from jax.sharding import PartitionSpec as P

MESH = pl.DeviceIdType.MESH
F32 = jnp.float32
BF16 = jnp.bfloat16

D = 2048
DK = 128
DV = 256
EPS = 1e-06
GATE_NORM = 16.0

NX, NY, NZ = 4, 4, 8
NT = 2 * NY
COPIES = 32
FAR_X = [2, 1, 3]
FAR_Y = [2, 1, 3]
FAR_Z = [4, 3, 5, 2, 6, 1, 7]
FAR_T = [4, 5, 2, 3, 6, 7, 1]
X_ORDER = [(0, 4), (2, 6), (3, 7), (1, 5)]
PLANE = [(dz, dx) for dz in FAR_Z + [0] for dx in FAR_X + [0] if (dz, dx) != (0, 0)]
LOADS = [(0, 0), (1, 1), (2, 0), (3, 0), (4, 0), (5, 0), (6, 0)]
LOADS += [(10, 3), (12, 2), (13, 2), (14, 2), (11, 4), (7, 5), (9, 6), (8, 7)]


def sigmoid(value):
    return 1.0 / (1.0 + jnp.exp(-value))


def halves(low, high):
    return jnp.concatenate([low, high], axis=1)


def as_pair(total):
    high = jnp.broadcast_to(total, (total.shape[0], 128)).astype(BF16).astype(F32)
    low = jnp.broadcast_to(total, (total.shape[0], 128)) - high
    lane = lax.broadcasted_iota(jnp.int32, high.shape, 1)
    return jnp.where(lane < 64, high, low).astype(BF16)


def of_pair(pair):
    return pair[:, 0:1] + pair[:, 64:65]


def packed_products(first, second, lane):
    blocks = []
    for j in range(8):
        low = first[:, 128 * j : 128 * j + 128]
        high = second[:, 128 * j : 128 * j + 128]
        top = low[0:32] + pltpu.roll(high[0:32], 64, 1)
        bottom = pltpu.roll(low[32:64], 64, 1) + high[32:64]
        blocks.append(jnp.where(lane < 64, top, bottom))
    return blocks


def kernel(*refs):
    inputs, (result, new_state), refs = refs[:15], refs[15:17], refs[17:]
    held, refs = refs[:15], refs[15:]
    (
        tokens,
        norm_gain,
        w_query,
        w_key,
        w_value,
        w_gate,
        w_decay,
        log_decay,
        state,
        out_gain,
        w_out,
        mixer_gain,
        w_ffgate,
        w_ffup,
        w_down,
    ) = held
    (
        att,
        w_own,
        x_all,
        w_all,
        w_diag,
        part1,
        got1,
        mix,
        w_mix,
        part2,
        got2,
        attn_own,
        attn_all,
        tok_own,
        tok_all,
        middle,
        up_own,
        up_all,
        down_own,
        down_all,
        part3a,
        got3a,
        part3b,
        got3b,
        hid,
        part4,
        got4,
        res_own,
        res_all,
        send_sems,
        recv_sems,
        local_sems,
    ) = refs
    kv = lax.axis_index("kv")
    t = lax.axis_index("tp")
    z, x = lax.div(kv, NX), lax.rem(kv, NX)
    y, core = lax.div(t, 2), lax.rem(t, 2)

    def at_x(d):
        return lax.rem(x + d, NX)

    def at_z(d):
        return lax.rem(z + d, NZ)

    def at_t(d):
        return lax.rem(t + d, NT)

    counter = [0]
    unsent = []

    class Exchange:
        def __init__(self, size):
            self.number = counter[0]
            self.size = size
            counter[0] += 1
            unsent.append(self)

        def send(self, src, dst, peer):
            pltpu.make_async_remote_copy(
                src_ref=src,
                dst_ref=dst,
                send_sem=send_sems.at[self.number],
                recv_sem=recv_sems.at[self.number],
                device_id=peer,
                device_id_type=MESH,
            ).start()

        def wait(self, sems, size):
            pltpu.make_async_copy(size, size, sems.at[self.number]).wait()

        def arrive(self):
            self.wait(recv_sems, self.size)

        def leave(self):
            self.wait(send_sems, self.size)

    for i, sem in LOADS:
        pltpu.make_async_copy(inputs[i], held[i], local_sems.at[sem]).start()

    barrier = pltpu.get_barrier_semaphore()

    def greet(peer):
        pl.semaphore_signal(barrier, inc=1, device_id=peer, device_id_type=MESH)

    for dz, dx in PLANE:
        greet((at_z(dz) * NX + at_x(dx), t))
    for d in FAR_T:
        greet((kv, at_t(d)))
    for d in FAR_Z:
        greet((at_z(d) * NX + x, z))

    @pl.when(t != z)
    def _():
        greet((kv, z))

    def loaded(sem, size):
        pltpu.make_async_copy(size, size, local_sems.at[sem]).wait()

    with jax.named_scope("wait_first"):
        loaded(0, part1.at[0:22])
        loaded(1, norm_gain)
    square = (64, 64)
    row = lax.broadcasted_iota(jnp.int32, square, 0)
    column = lax.broadcasted_iota(jnp.int32, square, 1)
    gain = jnp.sum(
        jnp.where(row == column, jnp.broadcast_to(norm_gain[...].astype(F32), square), 0.0),
        axis=1,
        keepdims=True,
    )

    def gained(weight):
        return (weight[...].astype(F32) * gain).astype(BF16)

    w_own[0, :, 0:128] = gained(w_query)
    w_own[0, :, 128:256] = gained(w_key)
    w_own[1] = gained(w_value)
    w_own[2] = gained(w_gate)
    w_own[3, :, 0:128] = gained(w_decay)
    w_own[3, :, 128:256] = jnp.zeros((64, 128), BF16)
    own = jnp.concatenate([tokens[:, 0:256], tokens[:, 256:512]], axis=0).astype(F32)
    x_all[x] = jnp.transpose(own, (1, 0)).astype(BF16).reshape(4, 64, 128)
    w_all[x] = w_own[x]

    greetings = len(PLANE) + len(FAR_T) + len(FAR_Z)
    with jax.named_scope("wait_barrier"):
        pl.semaphore_wait(barrier, greetings + jnp.where(t != z, 1, 0))

    tile_z = w_mix.at[:, 0:128]

    def lanes_of(block):
        return pl.ds(pl.multiple_of(block * 128, 128), 128)

    ring_x = [(d, (z * NX + at_x(d), t)) for d in FAR_X]
    ring_z = [(d, (at_z(d) * NX + x, t)) for d in FAR_Z]
    ring_t = [(d, (kv, at_t(d))) for d in FAR_T]
    gather_w = Exchange(w_all.at[0:3])
    gather_x = [Exchange(x_all.at[0:3, 0]) for _ in X_ORDER]
    x_blocks = [lax.rem(z + steps[0], 4) for steps in X_ORDER]
    for d, peer in ring_x:
        gather_w.send(w_own.at[at_x(d)], w_all.at[x], peer)
    for exchange, r in zip(gather_x, x_blocks):
        for d, peer in ring_x:
            exchange.send(x_all.at[x, r], x_all.at[x, r], peer)

    with jax.named_scope("wait_later"):
        loaded(3, w_out)
    out_rows = jnp.concatenate([w_out[:, 0:128], w_out[:, 128:256]], axis=0).astype(F32)
    w_mix[:, lanes_of(z)] = jnp.transpose(out_rows, (1, 0)).astype(BF16)
    mix_steps = []

    def mix_step(step):
        if step > 1:
            for exchange in mix_steps[-1]:
                exchange.arrive()
        exchanges = []
        for way in (1, -1):
            if step <= (4 if way > 0 else 3):
                lanes = lanes_of(at_z(NZ - way * (step - 1)))
                exchange = Exchange(tile_z)
                exchange.send(
                    w_mix.at[:, lanes], w_mix.at[:, lanes], (at_z(NZ + way) * NX + x, t)
                )
                exchanges.append(exchange)
        mix_steps.append(exchanges)

    mix_step(1)

    with jax.named_scope("wait_later"):
        loaded(2, up_all.at[0, 0:3])
        loaded(4, mixer_gain)
        loaded(5, log_decay)
        loaded(6, out_gain)
    gains = mixer_gain[...].astype(F32)
    units = jnp.transpose(
        jnp.concatenate([w_ffgate[...], w_ffup[...]], axis=0).astype(F32), (1, 0)
    )
    units = (units * jnp.concatenate([gains, gains], axis=1)).astype(BF16)
    down = w_down[...].astype(F32)
    down = jnp.concatenate([down, pltpu.roll(down, 768 - 48, 1)], axis=0)
    down = jnp.transpose(down, (1, 0)).astype(BF16)
    for j in range(NZ):
        up_own[0, j] = units[96 * j : 96 * j + 48]
        up_own[1, j] = units[96 * j + 48 : 96 * j + 96]
        down_own[j] = down[96 * j : 96 * j + 48]
    lanes_z = lanes_of(z)
    for half in range(2):
        up_all[half, t, :, lanes_z] = up_own[half, z]
    down_all[t, :, lanes_z] = down_own[z]
    up_blocks = [Exchange(up_own.at[half, 0:7]) for half in range(2)]
    up_y = [Exchange(up_all.at[half, 0:3]) for half in range(2)]
    up_core = [Exchange(up_all.at[half, 0:4]) for half in range(2)]
    partner = (kv, t + 1 - 2 * core)

    def along_y(d):
        return lax.rem(y + d, NY) * 2 + core

    def up_along_z(half):
        for d, peer in ring_z:
            up_blocks[half].send(
                up_own.at[half, at_z(d)], up_all.at[half, t, :, lanes_z], peer
            )

    def up_along_y(half):
        with jax.named_scope(f"wait_up_blocks_{half}"):
            up_blocks[half].arrive()
        for d in FAR_Y:
            up_y[half].send(up_all.at[half, t], up_all.at[half, t], (kv, along_y(d)))
        up_core[half].send(up_all.at[half, t], up_all.at[half, t], partner)

    up_along_z(0)
    lane32 = lax.broadcasted_iota(jnp.int32, (32, 128), 1)
    own = x_all[x, lax.rem(t, 4)].astype(F32)
    own = jnp.where(t < 4, own, pltpu.roll(own, 64, 1))
    tok_own[...] = jnp.where(lane32 < 64, own[0:32], pltpu.roll(own[32:64], 64, 1)).astype(BF16)
    tok_all[z] = tok_own[...]
    w_diag[...] = jnp.zeros(w_diag.shape, BF16)

    with jax.named_scope("wait_mix_step"):
        mix_step(2)

    with jax.named_scope("wait_gather1_w"):
        gather_w.arrive()
    for j in range(NX):
        w_diag[j, 0:64, 0:256] = w_all[j]
        w_diag[j, 64:128, 256:512] = w_all[j]
    lane64 = lax.broadcasted_iota(jnp.int32, (64, 128), 1)
    has_sums = x == NX - 1
    scatter1 = Exchange(got1.at[0:31])
    for number, (r, steps) in enumerate(zip(x_blocks, X_ORDER)):
        with jax.named_scope(f"wait_gather1_{number}"):
            gather_x[number].arrive()
        total = jnp.zeros((64, 512), F32)
        squares = jnp.zeros((64, 128), F32)
        for j in range(NX):
            block = x_all[j, r]
            total += jnp.dot(block, w_diag[j], preferred_element_type=F32)
            wide = block.astype(F32)
            squares += wide * wide
        for side in range(2):
            ours = (lane64 < 64) if side == 0 else (lane64 >= 64)
            sums = as_pair(jnp.sum(jnp.where(ours, squares, 0.0), axis=1, keepdims=True))
            first = 256 * side
            for k in range(NX):
                rows = slice(16 * k, 16 * k + 16)
                owner = NX * (r + 4 * side) + k
                part1[owner, :, 0:128] = total[rows, first : first + 128].astype(BF16)
                part1[owner, :, 128:256] = jnp.where(
                    has_sums, sums[rows].astype(F32), total[rows, first + 128 : first + 256]
                ).astype(BF16)
        for dz in sorted(steps, key=lambda step: -min(step, NZ - step)):
            for dx in FAR_X + [0]:
                if (dz, dx) != (0, 0):
                    peer = at_z(dz) * NX + at_x(dx)
                    scatter1.send(part1.at[peer], got1.at[x * NZ + z], (peer, t))
    got1[x * NZ + z] = part1[kv]

    up_along_z(1)
    up_along_y(0)
    mix_step(3)

    with jax.named_scope("wait_scatter1"):
        scatter1.arrive()
    mix_step(4)
    proj = []
    for j in range(NX):
        total = got1[NZ * j].astype(F32)
        for k in range(1, NZ):
            total += got1[NZ * j + k].astype(F32)
        proj.append(total)
    loaded(7, state)

    inv = lax.rsqrt(of_pair(proj[3][:, 128:256]) / D + EPS)
    query = proj[0][:, 0:128] * (inv * DK ** (-0.5))
    keys = proj[0][:, 128:256] * inv
    values = proj[1] * inv
    gate = proj[2] * inv
    decay_pre = proj[3][:, 0:128] * inv
    log_sigmoid = jnp.minimum(decay_pre, 0.0) - jnp.log1p(jnp.exp(-jnp.abs(decay_pre)))
    decay = jnp.exp(log_sigmoid / GATE_NORM + log_decay[...])
    columns = jnp.transpose(
        jnp.concatenate([query * decay, keys, decay, jnp.zeros((80, 128), F32)], axis=0), (1, 0)
    )
    for b in range(16):
        att[b : b + 1, :] = jnp.sum(state[b] * columns[:, b : b + 1], axis=0, keepdims=True)
    attended = att[...] + jnp.sum(query * keys, axis=1, keepdims=True) * values
    normed = (
        attended
        * lax.rsqrt(jnp.mean(attended * attended, axis=1, keepdims=True) + EPS)
        * out_gain[...]
    )
    mix[x] = (normed * (gate * sigmoid(gate))).astype(BF16)
    gather2 = Exchange(mix.at[0:3])
    for d, peer in ring_x:
        gather2.send(mix.at[x], mix.at[x], peer)
    down_blocks = Exchange(down_own.at[0:7])
    for d, peer in ring_z:
        down_blocks.send(down_own.at[at_z(d)], down_all.at[t, :, lanes_z], peer)
    tok_blocks = Exchange(tok_all.at[0:7])
    for d, peer in ring_z:
        tok_blocks.send(tok_own, tok_all.at[z], peer)
    for b in range(16):
        k_col = columns[:, 16 + b : 17 + b]
        a_col = columns[:, 32 + b : 33 + b]
        new_state[b] = state[b] * a_col + k_col * values[b : b + 1, :]

    with jax.named_scope("wait_mix_blocks"):
        for exchange in mix_steps[-1]:
            exchange.arrive()
    with jax.named_scope("wait_gather2"):
        gather2.arrive()
    mixed = mix[...].reshape(64, DV)
    stacked = jnp.concatenate([mixed[:, 0:128], mixed[:, 128:256]], axis=0)
    total = jnp.dot(stacked, w_mix[...], preferred_element_type=F32)
    for j, block in enumerate(packed_products(total[0:64], total[64:128], lane32)):
        part2[j] = block.astype(BF16)
    got2[t] = part2[t]
    scatter2 = Exchange(got2.at[0:7])
    for d, peer in ring_t:
        scatter2.send(part2.at[at_t(d)], got2.at[t], peer)
    up_along_y(1)
    with jax.named_scope("wait_scatter2"):
        scatter2.arrive()
    total = got2[0].astype(F32)
    for j in range(1, NT):
        total += got2[j].astype(F32)
    attn_own[...] = total.astype(BF16)

    spread = Exchange(attn_all)
    diagonal = t == z
    for d in FAR_Z:
        spread.send(attn_own, attn_all.at[t], (at_z(d) * NX + x, z))

    @pl.when(jnp.logical_not(diagonal))
    def _():
        spread.send(attn_own, attn_all.at[t], (kv, z))

    @pl.when(diagonal)
    def _():
        attn_all[t] = attn_own[...]

    def spread_wait(sems):
        @pl.when(diagonal)
        def _():
            spread.wait(sems, attn_all.at[0:7])

        @pl.when(jnp.logical_not(diagonal))
        def _():
            spread.wait(sems, attn_all)

    with jax.named_scope("wait_down_blocks"):
        down_blocks.arrive()
    down_y, down_core = Exchange(down_all.at[0:3]), Exchange(down_all.at[0:4])
    for d in FAR_Y:
        down_y.send(down_all.at[t], down_all.at[t], (kv, along_y(d)))
    for half in range(2):
        with jax.named_scope(f"wait_up_y_{half}"):
            up_y[half].arrive()
        for d in range(1, NY):
            other = along_y(d)
            up_core[half].send(up_all.at[half, other], up_all.at[half, other], partner)
    down_core.send(down_all.at[t], down_all.at[t], partner)

    with jax.named_scope("wait_tok_blocks"):
        tok_blocks.arrive()
    with jax.named_scope("wait_spread"):
        spread_wait(recv_sems)

    top = jnp.zeros((32, 128), F32)
    bottom = jnp.zeros((32, 128), F32)
    pieces = []
    for j in range(NZ):
        block = (tok_all[j].astype(F32) + attn_all[j].astype(F32)).astype(BF16)
        middle[j] = block
        wide = block.astype(F32)
        low = jnp.where(lane32 < 64, wide, 0.0)
        high = jnp.where(lane32 < 64, 0.0, wide)
        top += low * low
        bottom += high * high
        pieces.append(
            jnp.concatenate(
                [low, pltpu.roll(high, 64, 1), pltpu.roll(low, 64, 1), high], axis=0
            ).astype(BF16)
        )
    left = jnp.concatenate(pieces, axis=1)
    squares = as_pair(
        jnp.concatenate(
            [jnp.sum(top, axis=1, keepdims=True), jnp.sum(bottom, axis=1, keepdims=True)], axis=0
        )
    )
    parts3, gots3 = (part3a, part3b), (got3a, got3b)
    scatter3 = [Exchange(got3.at[0:3]) for got3 in gots3]
    for half, (part3, got3) in enumerate(zip(parts3, gots3)):
        with jax.named_scope(f"wait_up_core_{half}"):
            up_core[half].arrive()
        terms = lax.dot_general(
            left,
            up_all[half].reshape(384, 1024),
            (((1,), (1,)), ((), ())),
            preferred_element_type=F32,
        )
        for j in range(NX):
            rows = slice(16 * j, 16 * j + 16)
            part3[j, :, 0:384] = terms[rows].astype(BF16)
            part3[j, :, 384:768] = terms[64 + 16 * j : 80 + 16 * j].astype(BF16)
            if half == 0:
                part3[j, :, 768:896] = squares[rows]
        got3[x] = part3[x]
        for d, peer in ring_x:
            scatter3[half].send(part3.at[at_x(d)], got3.at[x], peer)
    with jax.named_scope("wait_down_y"):
        down_y.arrive()
    for d in range(1, NY):
        other = along_y(d)
        down_core.send(down_all.at[other], down_all.at[other], partner)
    gather3 = [Exchange(hid.at[half, 0:3]) for half in range(2)]
    inv = None
    for half, got3 in enumerate(gots3):
        with jax.named_scope(f"wait_scatter3_{half}"):
            scatter3[half].arrive()
        total = got3[0].astype(F32)
        for j in range(1, NX):
            total += got3[j].astype(F32)
        if half == 0:
            inv = lax.rsqrt(of_pair(total[:, 768:896]) / D + EPS)
        gate = total[:, 0:384] * inv
        hid[half, x] = (gate * sigmoid(gate) * (total[:, 384:768] * inv)).astype(BF16)
        for d, peer in ring_x:
            gather3[half].send(hid.at[half, x], hid.at[half, x], peer)
    with jax.named_scope("wait_down_core"):
        down_core.arrive()

    weights = down_all[...].reshape(NT * 48, 1024)
    products = []
    for half in range(2):
        with jax.named_scope(f"wait_gather3_{half}"):
            gather3[half].arrive()
        products.append(
            jnp.dot(hid[half].reshape(64, 384), weights, preferred_element_type=F32)
        )
    for j, block in enumerate(packed_products(*products, lane32)):
        part4[j] = block.astype(BF16)
    got4[z] = part4[z]
    scatter4 = Exchange(got4.at[0:7])
    for d, peer in ring_z:
        scatter4.send(part4.at[at_z(d)], got4.at[z], peer)
    with jax.named_scope("wait_scatter4"):
        scatter4.arrive()
    total = got4[0].astype(F32)
    for j in range(1, NZ):
        total += got4[j].astype(F32)
    res_own[...] = (middle[z].astype(F32) + total).astype(BF16)
    res_all[t] = res_own[...]
    gather4 = Exchange(res_all.at[0:7])
    for d, peer in ring_t:
        gather4.send(res_own, res_all.at[t], peer)
    with jax.named_scope("wait_gather4"):
        gather4.arrive()
    rows = []
    for j in range(NT):
        block = res_all[j].astype(F32)
        rows += [block, pltpu.roll(block, 64, 1)]
    rows = jnp.concatenate(rows, axis=0)
    result[...] = jnp.transpose(rows, (1, 0))[0:64].astype(BF16)
    with jax.named_scope("wait_sends"):
        for exchange in unsent:
            if exchange is spread:
                spread_wait(send_sems)
            else:
                exchange.leave()

def finish(result_in, state_in, result_out, state_out, sems):
    result = pltpu.make_async_copy(result_in, result_out, sems.at[0])
    states = pltpu.make_async_copy(state_in, state_out, sems.at[1])
    parts = [pl.ds(2 * i, 2) for i in range(8)]
    result.start()
    for part in parts:
        pltpu.make_async_copy(state_in.at[part], state_out.at[part], sems.at[1]).start()
    result.wait()
    states.wait()


def body(
    tokens,
    norm_gain,
    w_query,
    w_key,
    w_value,
    w_gate,
    w_decay,
    log_decay,
    state,
    out_gain,
    w_out,
    mixer_gain,
    w_ffgate,
    w_ffup,
    w_down,
):
    vmem = pl.BlockSpec(memory_space=pltpu.VMEM)
    hbm = pl.BlockSpec(memory_space=pltpu.HBM)
    shape = state.shape
    arguments = (
        tokens.T,
        norm_gain.reshape(1, 64),
        w_query,
        w_key,
        w_value,
        w_gate,
        w_decay,
        log_decay,
        state.reshape(shape[0], DK, DV),
        out_gain.reshape(1, DV),
        w_out.T,
        mixer_gain.reshape(1, 64),
        w_ffgate,
        w_ffup,
        w_down.T,
    )
    arguments = [pltpu.with_memory_space_constraint(value, pltpu.HBM) for value in arguments]
    result, new_state = pl.pallas_call(
        kernel,
        out_shape=(
            pltpu.VMEM((64, 512), BF16),
            pltpu.VMEM((shape[0], DK, DV), F32),
        ),
        in_specs=[hbm] * 15,
        out_specs=(vmem, vmem),
        scratch_shapes=[pltpu.VMEM(value.shape, value.dtype) for value in arguments]
        + [
            pltpu.VMEM((16, DV), F32),
            pltpu.VMEM((NX, 64, 256), BF16),
            pltpu.VMEM((NX, 4, 64, 128), BF16),
            pltpu.VMEM((NX, 64, 256), BF16),
            pltpu.VMEM((NX, 128, 512), BF16),
            pltpu.VMEM((NZ * NX, 16, 256), BF16),
            pltpu.VMEM((NX * NZ, 16, 256), BF16),
            pltpu.VMEM((NX, 16, 256), BF16),
            pltpu.VMEM((128, 1024), BF16),
            pltpu.VMEM((NT, 32, 128), BF16),
            pltpu.VMEM((NT, 32, 128), BF16),
            pltpu.VMEM((32, 128), BF16),
            pltpu.VMEM((NT, 32, 128), BF16),
            pltpu.VMEM((32, 128), BF16),
            pltpu.VMEM((NZ, 32, 128), BF16),
            pltpu.VMEM((NZ, 32, 128), BF16),
            pltpu.VMEM((2, NZ, 48, 128), BF16),
            pltpu.VMEM((2, NT, 48, 1024), BF16),
            pltpu.VMEM((NZ, 48, 128), BF16),
            pltpu.VMEM((NT, 48, 1024), BF16),
            pltpu.VMEM((NX, 16, 896), BF16),
            pltpu.VMEM((NX, 16, 896), BF16),
            pltpu.VMEM((NX, 16, 768), BF16),
            pltpu.VMEM((NX, 16, 768), BF16),
            pltpu.VMEM((2, NX, 16, 384), BF16),
            pltpu.VMEM((NZ, 32, 128), BF16),
            pltpu.VMEM((NZ, 32, 128), BF16),
            pltpu.VMEM((32, 128), BF16),
            pltpu.VMEM((NT, 32, 128), BF16),
            pltpu.SemaphoreType.DMA((COPIES,)),
            pltpu.SemaphoreType.DMA((COPIES,)),
            pltpu.SemaphoreType.DMA((8,)),
        ],
        compiler_params=pltpu.CompilerParams(
            collective_id=0, has_side_effects=True, vmem_limit_bytes=40 * 1024 * 1024
        ),
    )(*arguments)
    result, new_state = pl.pallas_call(
        finish,
        out_shape=(
            jax.ShapeDtypeStruct((64, 512), BF16),
            jax.ShapeDtypeStruct((shape[0], DK, DV), F32),
        ),
        in_specs=[vmem, vmem],
        out_specs=(hbm, hbm),
        scratch_shapes=[pltpu.SemaphoreType.DMA((2,))],
        compiler_params=pltpu.CompilerParams(vmem_limit_bytes=8 * 1024 * 1024),
    )(result, new_state)
    return (result.T, new_state.reshape(shape))


def solution(mesh):
    return jax.shard_map(
        body,
        mesh=mesh,
        in_specs=(
            P(None, "kv"),
            P("kv"),
            P("kv", "tp"),
            P("kv", "tp"),
            P("kv", "tp"),
            P("kv", "tp"),
            P("kv", "tp"),
            P("kv", "tp"),
            P("kv", "tp", None, None),
            P(),
            P("tp", "kv"),
            P("kv"),
            P("kv", "tp"),
            P("kv", "tp"),
            P("tp", "kv"),
        ),
        out_specs=(P(None, "kv"), P("kv", "tp", None, None)),
        check_vma=False,
    )
```

```python
import functools

import jax
import jax.numpy as jnp
from jax import lax
from jax.experimental import pallas as pl
from jax.experimental.pallas import tpu as pltpu
from jax.sharding import PartitionSpec as P

MESH = pl.DeviceIdType.MESH
F32 = jnp.float32
BF16 = jnp.bfloat16

D = 2048
DK = 128
DV = 256
EPS = 1e-06
GATE_NORM = 16.0

NX, NY, NZ = 4, 4, 8
NT = 2 * NY
COPIES = 32
FAR_X = [2, 1, 3]
FAR_Y = [2, 1, 3]
FAR_Z = [4, 3, 5, 2, 6, 1, 7]
FAR_T = [4, 5, 2, 3, 6, 7, 1]
X_ORDER = [(0, 4), (2, 6), (3, 7), (1, 5)]
PLANE = [(dz, dx) for dz in FAR_Z + [0] for dx in FAR_X + [0] if (dz, dx) != (0, 0)]
LOADS = [(0, 0), (1, 1), (2, 0), (3, 0), (4, 0), (5, 0), (6, 0)]
LOADS += [(10, 3), (12, 2), (13, 2), (14, 2), (11, 4), (7, 5), (9, 6), (8, 7)]


def sigmoid(value):
    return 1.0 / (1.0 + jnp.exp(-value))


def as_pair(total):
    high = jnp.broadcast_to(total, (total.shape[0], 128)).astype(BF16).astype(F32)
    low = jnp.broadcast_to(total, (total.shape[0], 128)) - high
    lane = lax.broadcasted_iota(jnp.int32, high.shape, 1)
    return jnp.where(lane < 64, high, low).astype(BF16)


def of_pair(pair):
    return pair[:, 0:1] + pair[:, 64:65]


def packed_products(first, second, lane):
    blocks = []
    for j in range(8):
        low = first[:, 128 * j : 128 * j + 128]
        high = second[:, 128 * j : 128 * j + 128]
        top = low[0:32] + pltpu.roll(high[0:32], 64, 1)
        bottom = pltpu.roll(low[32:64], 64, 1) + high[32:64]
        blocks.append(jnp.where(lane < 64, top, bottom))
    return blocks


def kernel(*refs):
    inputs, (result, new_state), refs = refs[:15], refs[15:17], refs[17:]
    held, refs = refs[:15], refs[15:]
    (
        tokens,
        norm_gain,
        w_query,
        w_key,
        w_value,
        w_gate,
        w_decay,
        log_decay,
        state,
        out_gain,
        w_out,
        mixer_gain,
        w_ffgate,
        w_ffup,
        w_down,
    ) = held
    (
        att,
        w_own,
        x_own,
        x_all,
        w_all,
        w_diag,
        part1,
        got1,
        mix,
        w_mix,
        part2,
        got2,
        attn_own,
        attn_all,
        tok_own,
        tok_all,
        middle,
        up_own,
        up_all,
        down_own,
        down_all,
        part3a,
        got3a,
        part3b,
        got3b,
        hid,
        part4,
        got4,
        res_own,
        res_all,
        send_sems,
        recv_sems,
        local_sems,
    ) = refs
    kv = lax.axis_index("kv")
    t = lax.axis_index("tp")
    z, x = lax.div(kv, NX), lax.rem(kv, NX)
    y, core = lax.div(t, 2), lax.rem(t, 2)

    def at_x(d):
        return lax.rem(x + d, NX)

    def at_z(d):
        return lax.rem(z + d, NZ)

    def at_t(d):
        return lax.rem(t + d, NT)

    counter = [0]
    unsent = []

    class Exchange:
        def __init__(self, size):
            self.number = counter[0]
            self.size = size
            counter[0] += 1
            unsent.append(self)

        def send(self, src, dst, peer):
            pltpu.make_async_remote_copy(
                src_ref=src,
                dst_ref=dst,
                send_sem=send_sems.at[self.number],
                recv_sem=recv_sems.at[self.number],
                device_id=peer,
                device_id_type=MESH,
            ).start()

        def wait(self, sems, size):
            pltpu.make_async_copy(size, size, sems.at[self.number]).wait()

        def arrive(self):
            self.wait(recv_sems, self.size)

        def leave(self):
            self.wait(send_sems, self.size)

    for i, sem in LOADS:
        pltpu.make_async_copy(inputs[i], held[i], local_sems.at[sem]).start()

    barrier = pltpu.get_barrier_semaphore()

    def greet(peer):
        pl.semaphore_signal(barrier, inc=1, device_id=peer, device_id_type=MESH)

    for dz, dx in PLANE:
        greet((at_z(dz) * NX + at_x(dx), t))
    for d in FAR_T:
        greet((kv, at_t(d)))
    def loaded(sem, size):
        pltpu.make_async_copy(size, size, local_sems.at[sem]).wait()

    with jax.named_scope("wait_first"):
        loaded(0, part1.at[0:22])
        loaded(1, norm_gain)
    square = (64, 64)
    row = lax.broadcasted_iota(jnp.int32, square, 0)
    column = lax.broadcasted_iota(jnp.int32, square, 1)
    gain = jnp.sum(
        jnp.where(row == column, jnp.broadcast_to(norm_gain[...].astype(F32), square), 0.0),
        axis=1,
        keepdims=True,
    )

    def gained(weight):
        return (weight[...].astype(F32) * gain).astype(BF16)

    w_own[0, :, 0:128] = gained(w_query)
    w_own[0, :, 128:256] = gained(w_key)
    w_own[1] = gained(w_value)
    w_own[2] = gained(w_gate)
    w_own[3, :, 0:128] = gained(w_decay)
    w_own[3, :, 128:256] = jnp.zeros((64, 128), BF16)
    own = jnp.concatenate([tokens[:, 0:256], tokens[:, 256:512]], axis=0).astype(F32)
    own = jnp.transpose(own, (1, 0))
    x_own[...] = own.reshape(4, 64, 128)
    x_all[x] = own.astype(BF16).reshape(4, 64, 128)
    w_all[x] = w_own[x]

    with jax.named_scope("wait_barrier"):
        pl.semaphore_wait(barrier, len(PLANE) + len(FAR_T))

    tile_z = w_mix.at[:, 0:128]

    def lanes_of(block):
        return pl.ds(pl.multiple_of(block * 128, 128), 128)

    ring_x = [(d, (z * NX + at_x(d), t)) for d in FAR_X]
    ring_z = [(d, (at_z(d) * NX + x, t)) for d in FAR_Z]
    ring_t = [(d, (kv, at_t(d))) for d in FAR_T]
    gather_w = Exchange(w_all.at[0:3])
    gather_x = [Exchange(x_all.at[0:3, 0]) for _ in X_ORDER]
    x_blocks = [lax.rem(z + steps[0], 4) for steps in X_ORDER]
    for d, peer in ring_x:
        gather_w.send(w_own.at[at_x(d)], w_all.at[x], peer)
    for exchange, r in zip(gather_x, x_blocks):
        for d, peer in ring_x:
            exchange.send(x_all.at[x, r], x_all.at[x, r], peer)

    with jax.named_scope("wait_later"):
        loaded(3, w_out)
    out_rows = jnp.concatenate([w_out[:, 0:128], w_out[:, 128:256]], axis=0).astype(F32)
    w_mix[:, lanes_of(z)] = jnp.transpose(out_rows, (1, 0)).astype(BF16)
    mix_steps = []

    def mix_step(step):
        if step > 1:
            for exchange in mix_steps[-1]:
                exchange.arrive()
        exchanges = []
        for way in (1, -1):
            if step <= (4 if way > 0 else 3):
                lanes = lanes_of(at_z(NZ - way * (step - 1)))
                exchange = Exchange(tile_z)
                exchange.send(
                    w_mix.at[:, lanes], w_mix.at[:, lanes], (at_z(NZ + way) * NX + x, t)
                )
                exchanges.append(exchange)
        mix_steps.append(exchanges)

    mix_step(1)

    with jax.named_scope("wait_later"):
        loaded(2, up_all.at[0, 0:3])
        loaded(4, mixer_gain)
        loaded(5, log_decay)
        loaded(6, out_gain)
    gains = mixer_gain[...].astype(F32)
    units = jnp.transpose(
        jnp.concatenate([w_ffgate[...], w_ffup[...]], axis=0).astype(F32), (1, 0)
    )
    units = (units * jnp.concatenate([gains, gains], axis=1)).astype(BF16)
    down = w_down[...].astype(F32)
    down = jnp.concatenate([down, pltpu.roll(down, 768 - 48, 1)], axis=0)
    down = jnp.transpose(down, (1, 0)).astype(BF16)
    for j in range(NZ):
        up_own[0, j] = units[96 * j : 96 * j + 48]
        up_own[1, j] = units[96 * j + 48 : 96 * j + 96]
        down_own[j] = down[96 * j : 96 * j + 48]
    lanes_z = lanes_of(z)
    for half in range(2):
        up_all[half, t, :, lanes_z] = up_own[half, z]
    down_all[t, :, lanes_z] = down_own[z]
    up_blocks = [Exchange(up_own.at[half, 0:7]) for half in range(2)]
    up_y = [Exchange(up_all.at[half, 0:3]) for half in range(2)]
    up_core = [Exchange(up_all.at[half, 0:4]) for half in range(2)]
    partner = (kv, t + 1 - 2 * core)

    def along_y(d):
        return lax.rem(y + d, NY) * 2 + core

    def up_along_z(half):
        for d, peer in ring_z:
            up_blocks[half].send(
                up_own.at[half, at_z(d)], up_all.at[half, t, :, lanes_z], peer
            )

    def up_along_y(half):
        with jax.named_scope(f"wait_up_blocks_{half}"):
            up_blocks[half].arrive()
        for d in FAR_Y:
            up_y[half].send(up_all.at[half, t], up_all.at[half, t], (kv, along_y(d)))
        up_core[half].send(up_all.at[half, t], up_all.at[half, t], partner)

    up_along_z(0)
    lane32 = lax.broadcasted_iota(jnp.int32, (32, 128), 1)
    ours = x_own[:, pl.ds(pl.multiple_of(8 * t, 8), 8), :]
    tok_own[...] = ours.reshape(32, 128).astype(BF16)
    tok_all[z] = tok_own[...]
    w_diag[...] = jnp.zeros(w_diag.shape, BF16)

    with jax.named_scope("wait_mix_step"):
        mix_step(2)

    with jax.named_scope("wait_gather1_w"):
        gather_w.arrive()
    for j in range(NX):
        w_diag[j, 0:64, 0:256] = w_all[j]
        w_diag[j, 64:128, 256:512] = w_all[j]
    lane64 = lax.broadcasted_iota(jnp.int32, (64, 128), 1)
    has_sums = x == NX - 1
    scatter1 = Exchange(got1.at[0:31])
    for number, (r, steps) in enumerate(zip(x_blocks, X_ORDER)):
        with jax.named_scope(f"wait_gather1_{number}"):
            gather_x[number].arrive()
        total = jnp.zeros((64, 512), F32)
        squares = jnp.zeros((64, 128), F32)
        for j in range(NX):
            block = x_all[j, r]
            total += jnp.dot(block, w_diag[j], preferred_element_type=F32)
            wide = block.astype(F32)
            squares += wide * wide
        for side in range(2):
            ours = (lane64 < 64) if side == 0 else (lane64 >= 64)
            sums = as_pair(jnp.sum(jnp.where(ours, squares, 0.0), axis=1, keepdims=True))
            first = 256 * side
            for k in range(NX):
                rows = slice(16 * k, 16 * k + 16)
                owner = NX * (r + 4 * side) + k
                part1[owner, :, 0:128] = total[rows, first : first + 128].astype(BF16)
                part1[owner, :, 128:256] = jnp.where(
                    has_sums, sums[rows].astype(F32), total[rows, first + 128 : first + 256]
                ).astype(BF16)
        for dz in sorted(steps, key=lambda step: -min(step, NZ - step)):
            for dx in FAR_X + [0]:
                if (dz, dx) != (0, 0):
                    peer = at_z(dz) * NX + at_x(dx)
                    scatter1.send(part1.at[peer], got1.at[x * NZ + z], (peer, t))
    got1[x * NZ + z] = part1[kv]

    with jax.named_scope("wait_mix_step"):
        mix_step(3)
    up_along_z(1)
    up_along_y(0)

    with jax.named_scope("wait_scatter1"):
        scatter1.arrive()
    proj = []
    for j in range(NX):
        total = got1[NZ * j].astype(F32)
        for k in range(1, NZ):
            total += got1[NZ * j + k].astype(F32)
        proj.append(total)
    loaded(7, state)

    inv = lax.rsqrt(of_pair(proj[3][:, 128:256]) / D + EPS)
    query = proj[0][:, 0:128] * (inv * DK ** (-0.5))
    keys = proj[0][:, 128:256] * inv
    values = proj[1] * inv
    gate = proj[2] * inv
    decay_pre = proj[3][:, 0:128] * inv
    log_sigmoid = jnp.minimum(decay_pre, 0.0) - jnp.log1p(jnp.exp(-jnp.abs(decay_pre)))
    decay = jnp.exp(log_sigmoid / GATE_NORM + log_decay[...])
    columns = jnp.transpose(
        jnp.concatenate([query * decay, keys, decay, jnp.zeros((80, 128), F32)], axis=0), (1, 0)
    )
    for b in range(16):
        att[b : b + 1, :] = jnp.sum(state[b] * columns[:, b : b + 1], axis=0, keepdims=True)
    attended = att[...] + jnp.sum(query * keys, axis=1, keepdims=True) * values
    normed = (
        attended
        * lax.rsqrt(jnp.mean(attended * attended, axis=1, keepdims=True) + EPS)
        * out_gain[...]
    )
    mix[x] = (normed * (gate * sigmoid(gate))).astype(BF16)
    gather2 = Exchange(mix.at[0:3])
    for d, peer in ring_x:
        gather2.send(mix.at[x], mix.at[x], peer)
    with jax.named_scope("wait_mix_step"):
        mix_step(4)
    down_blocks = Exchange(down_own.at[0:7])
    for d, peer in ring_z:
        down_blocks.send(down_own.at[at_z(d)], down_all.at[t, :, lanes_z], peer)
    tok_blocks = Exchange(tok_all.at[0:7])
    for d, peer in ring_z:
        tok_blocks.send(tok_own, tok_all.at[z], peer)
    for b in range(16):
        k_col = columns[:, 16 + b : 17 + b]
        a_col = columns[:, 32 + b : 33 + b]
        new_state[b] = state[b] * a_col + k_col * values[b : b + 1, :]

    with jax.named_scope("wait_mix_blocks"):
        for exchange in mix_steps[-1]:
            exchange.arrive()
    with jax.named_scope("wait_gather2"):
        gather2.arrive()
    mixed = mix[...].reshape(64, DV)
    stacked = jnp.concatenate([mixed[:, 0:128], mixed[:, 128:256]], axis=0)
    total = jnp.dot(stacked, w_mix[...], preferred_element_type=F32)
    lane64 = lax.broadcasted_iota(jnp.int32, (64, 128), 1)
    pairs = []
    for p in range(4):
        low, high = [
            (total[0:64, first : first + 128], total[64:128, first : first + 128])
            for first in (256 * p, 256 * p + 128)
        ]
        pairs.append(
            jnp.where(
                lane64 < 64,
                low[0] + pltpu.roll(low[1], 64, 1),
                pltpu.roll(high[0], 64, 1) + high[1],
            )
        )
    for j in range(NT):
        rows = slice(8 * j, 8 * j + 8)
        part2[j] = jnp.concatenate([pair[rows] for pair in pairs], axis=0).astype(BF16)
    got2[t] = part2[t]
    scatter2 = Exchange(got2.at[0:7])
    for d, peer in ring_t:
        scatter2.send(part2.at[at_t(d)], got2.at[t], peer)
    up_along_y(1)
    with jax.named_scope("wait_scatter2"):
        scatter2.arrive()
    total = got2[0].astype(F32)
    for j in range(1, NT):
        total += got2[j].astype(F32)
    attn_own[...] = total.astype(BF16)

    attn_all[z] = attn_own[...]
    spread = Exchange(attn_all.at[0:7])
    for d, peer in ring_z:
        spread.send(attn_own, attn_all.at[z], peer)

    with jax.named_scope("wait_down_blocks"):
        down_blocks.arrive()
    down_y, down_core = Exchange(down_all.at[0:3]), Exchange(down_all.at[0:4])
    for d in FAR_Y:
        down_y.send(down_all.at[t], down_all.at[t], (kv, along_y(d)))
    for half in range(2):
        with jax.named_scope(f"wait_up_y_{half}"):
            up_y[half].arrive()
        for d in range(1, NY):
            other = along_y(d)
            up_core[half].send(up_all.at[half, other], up_all.at[half, other], partner)
    down_core.send(down_all.at[t], down_all.at[t], partner)

    with jax.named_scope("wait_tok_blocks"):
        tok_blocks.arrive()
    with jax.named_scope("wait_spread"):
        spread.arrive()

    squares = jnp.zeros((64, 128), F32)
    pieces = []
    sums = [attn_all[j].astype(F32) for j in range(NZ)]
    middles = []
    for p in range(4):
        low, high = tok_all[2 * p].astype(F32), tok_all[2 * p + 1].astype(F32)
        residual = jnp.concatenate(
            [
                jnp.where(lane32 < 64, low, pltpu.roll(high, 64, 1)),
                jnp.where(lane32 < 64, pltpu.roll(low, 64, 1), high),
            ],
            axis=0,
        )
        added = jnp.concatenate([total[8 * p : 8 * p + 8] for total in sums], axis=0)
        wide = (residual + added).astype(BF16).astype(F32)
        middles.append(wide)
        squares += wide * wide
        turned = pltpu.roll(wide, 64, 1)
        for here, there in ((wide, turned), (turned, wide)):
            pieces.append(
                jnp.concatenate(
                    [jnp.where(lane64 < 64, here, 0.0), jnp.where(lane64 < 64, 0.0, there)], axis=0
                ).astype(BF16)
            )
    left = jnp.concatenate(pieces, axis=1)
    squares = as_pair(jnp.sum(squares, axis=1, keepdims=True))
    parts3, gots3 = (part3a, part3b), (got3a, got3b)
    scatter3 = [Exchange(got3.at[0:3]) for got3 in gots3]
    for half, (part3, got3) in enumerate(zip(parts3, gots3)):
        with jax.named_scope(f"wait_up_core_{half}"):
            up_core[half].arrive()
        terms = lax.dot_general(
            left,
            up_all[half].reshape(384, 1024),
            (((1,), (1,)), ((), ())),
            preferred_element_type=F32,
        )
        for j in range(NX):
            rows = slice(16 * j, 16 * j + 16)
            part3[j, :, 0:384] = terms[rows].astype(BF16)
            part3[j, :, 384:768] = terms[64 + 16 * j : 80 + 16 * j].astype(BF16)
            if half == 0:
                part3[j, :, 768:896] = squares[rows]
        got3[x] = part3[x]
        for d, peer in ring_x:
            scatter3[half].send(part3.at[at_x(d)], got3.at[x], peer)
    for p, wide in enumerate(middles):
        turned = pltpu.roll(wide, 64, 1)
        middle[2 * p] = jnp.where(lane32 < 64, wide[0:32], turned[32:64]).astype(BF16)
        middle[2 * p + 1] = jnp.where(lane32 < 64, turned[0:32], wide[32:64]).astype(BF16)
    with jax.named_scope("wait_down_y"):
        down_y.arrive()
    for d in range(1, NY):
        other = along_y(d)
        down_core.send(down_all.at[other], down_all.at[other], partner)
    gather3 = [Exchange(hid.at[half, 0:3]) for half in range(2)]
    inv = None
    for half, got3 in enumerate(gots3):
        with jax.named_scope(f"wait_scatter3_{half}"):
            scatter3[half].arrive()
        total = got3[0].astype(F32)
        for j in range(1, NX):
            total += got3[j].astype(F32)
        if half == 0:
            inv = lax.rsqrt(of_pair(total[:, 768:896]) / D + EPS)
        gate = total[:, 0:384] * inv
        hid[half, x] = (gate * sigmoid(gate) * (total[:, 384:768] * inv)).astype(BF16)
        for d, peer in ring_x:
            gather3[half].send(hid.at[half, x], hid.at[half, x], peer)
    with jax.named_scope("wait_down_core"):
        down_core.arrive()

    weights = down_all[...].reshape(NT * 48, 1024)
    products = []
    for half in range(2):
        with jax.named_scope(f"wait_gather3_{half}"):
            gather3[half].arrive()
        products.append(
            jnp.dot(hid[half].reshape(64, 384), weights, preferred_element_type=F32)
        )
    for j, block in enumerate(packed_products(*products, lane32)):
        part4[j] = block.astype(BF16)
    got4[z] = part4[z]
    scatter4 = Exchange(got4.at[0:7])
    for d, peer in ring_z:
        scatter4.send(part4.at[at_z(d)], got4.at[z], peer)
    with jax.named_scope("wait_scatter4"):
        scatter4.arrive()
    total = got4[0].astype(F32)
    for j in range(1, NZ):
        total += got4[j].astype(F32)
    res_own[...] = (middle[z].astype(F32) + total).astype(BF16)
    res_all[t] = res_own[...]
    gather4 = Exchange(res_all.at[0:7])
    for d, peer in ring_t:
        gather4.send(res_own, res_all.at[t], peer)
    with jax.named_scope("wait_gather4"):
        gather4.arrive()
    blocks = [res_all[j].astype(F32) for j in range(NT)]
    blocks = [blocks, [pltpu.roll(block, 64, 1) for block in blocks]]
    rows = jnp.concatenate(
        [
            blocks[j // 4][k][8 * (j % 4) : 8 * (j % 4) + 8]
            for j in range(NZ)
            for k in range(NT)
        ],
        axis=0,
    )
    result[...] = jnp.transpose(rows, (1, 0))[0:64].astype(BF16)
    with jax.named_scope("wait_sends"):
        for exchange in unsent:
            exchange.leave()


def finish(result_in, state_in, result_out, state_out, sems):
    result = pltpu.make_async_copy(result_in, result_out, sems.at[0])
    states = pltpu.make_async_copy(state_in, state_out, sems.at[1])
    parts = [pl.ds(2 * i, 2) for i in range(8)]
    result.start()
    for part in parts:
        pltpu.make_async_copy(state_in.at[part], state_out.at[part], sems.at[1]).start()
    result.wait()
    states.wait()


def body(
    tokens,
    norm_gain,
    w_query,
    w_key,
    w_value,
    w_gate,
    w_decay,
    log_decay,
    state,
    out_gain,
    w_out,
    mixer_gain,
    w_ffgate,
    w_ffup,
    w_down,
):
    vmem = pl.BlockSpec(memory_space=pltpu.VMEM)
    hbm = pl.BlockSpec(memory_space=pltpu.HBM)
    shape = state.shape
    arguments = (
        tokens.T,
        norm_gain.reshape(1, 64),
        w_query,
        w_key,
        w_value,
        w_gate,
        w_decay,
        log_decay,
        state.reshape(shape[0], DK, DV),
        out_gain.reshape(1, DV),
        w_out.T,
        mixer_gain.reshape(1, 64),
        w_ffgate,
        w_ffup,
        w_down.T,
    )
    arguments = [pltpu.with_memory_space_constraint(value, pltpu.HBM) for value in arguments]
    result, new_state = pl.pallas_call(
        kernel,
        out_shape=(
            pltpu.VMEM((64, 512), BF16),
            pltpu.VMEM((shape[0], DK, DV), F32),
        ),
        in_specs=[hbm] * 15,
        out_specs=(vmem, vmem),
        scratch_shapes=[pltpu.VMEM(value.shape, value.dtype) for value in arguments]
        + [
            pltpu.VMEM((16, DV), F32),
            pltpu.VMEM((NX, 64, 256), BF16),
            pltpu.VMEM((4, 64, 128), F32),
            pltpu.VMEM((NX, 4, 64, 128), BF16),
            pltpu.VMEM((NX, 64, 256), BF16),
            pltpu.VMEM((NX, 128, 512), BF16),
            pltpu.VMEM((NZ * NX, 16, 256), BF16),
            pltpu.VMEM((NX * NZ, 16, 256), BF16),
            pltpu.VMEM((NX, 16, 256), BF16),
            pltpu.VMEM((128, 1024), BF16),
            pltpu.VMEM((NT, 32, 128), BF16),
            pltpu.VMEM((NT, 32, 128), BF16),
            pltpu.VMEM((32, 128), BF16),
            pltpu.VMEM((NT, 32, 128), BF16),
            pltpu.VMEM((32, 128), BF16),
            pltpu.VMEM((NZ, 32, 128), BF16),
            pltpu.VMEM((NZ, 32, 128), BF16),
            pltpu.VMEM((2, NZ, 48, 128), BF16),
            pltpu.VMEM((2, NT, 48, 1024), BF16),
            pltpu.VMEM((NZ, 48, 128), BF16),
            pltpu.VMEM((NT, 48, 1024), BF16),
            pltpu.VMEM((NX, 16, 896), BF16),
            pltpu.VMEM((NX, 16, 896), BF16),
            pltpu.VMEM((NX, 16, 768), BF16),
            pltpu.VMEM((NX, 16, 768), BF16),
            pltpu.VMEM((2, NX, 16, 384), BF16),
            pltpu.VMEM((NZ, 32, 128), BF16),
            pltpu.VMEM((NZ, 32, 128), BF16),
            pltpu.VMEM((32, 128), BF16),
            pltpu.VMEM((NT, 32, 128), BF16),
            pltpu.SemaphoreType.DMA((COPIES,)),
            pltpu.SemaphoreType.DMA((COPIES,)),
            pltpu.SemaphoreType.DMA((8,)),
        ],
        compiler_params=pltpu.CompilerParams(
            collective_id=0, has_side_effects=True, vmem_limit_bytes=40 * 1024 * 1024
        ),
    )(*arguments)
    result, new_state = pl.pallas_call(
        finish,
        out_shape=(
            jax.ShapeDtypeStruct((64, 512), BF16),
            jax.ShapeDtypeStruct((shape[0], DK, DV), F32),
        ),
        in_specs=[vmem, vmem],
        out_specs=(hbm, hbm),
        scratch_shapes=[pltpu.SemaphoreType.DMA((2,))],
        compiler_params=pltpu.CompilerParams(vmem_limit_bytes=8 * 1024 * 1024),
    )(result, new_state)
    return (result.T, new_state.reshape(shape))


def solution(mesh):
    return jax.shard_map(
        body,
        mesh=mesh,
        in_specs=(
            P(None, "kv"),
            P("kv"),
            P("kv", "tp"),
            P("kv", "tp"),
            P("kv", "tp"),
            P("kv", "tp"),
            P("kv", "tp"),
            P("kv", "tp"),
            P("kv", "tp", None, None),
            P(),
            P("tp", "kv"),
            P("kv"),
            P("kv", "tp"),
            P("kv", "tp"),
            P("tp", "kv"),
        ),
        out_specs=(P(None, "kv"), P("kv", "tp", None, None)),
        check_vma=False,
    )
```

```python
import functools

import jax
import jax.numpy as jnp
from jax import lax
from jax.experimental import pallas as pl
from jax.experimental.pallas import tpu as pltpu
from jax.sharding import PartitionSpec as P

MESH = pl.DeviceIdType.MESH
F32 = jnp.float32
BF16 = jnp.bfloat16

D = 2048
DK = 128
DV = 256
EPS = 1e-06
GATE_NORM = 16.0

NX, NY, NZ = 4, 4, 8
NT = 2 * NY
COPIES = 32
SMALL, UP, DOWN, LAST = range(4)
FAR_X = [2, 1, 3]
FAR_Y = [2, 1, 3]
FAR_Z = [4, 3, 5, 2, 6, 1, 7]
FAR_T = [4, 5, 2, 3, 6, 7, 1]
X_ORDER = [(0, 4), (2, 6), (3, 7), (1, 5)]
PLANE = [(dz, dx) for dz in FAR_Z + [0] for dx in FAR_X + [0] if (dz, dx) != (0, 0)]
LOADS = [(0, 0), (1, 1), (2, 0), (3, 0), (4, 0), (5, 0), (6, 0)]
LOADS += [(10, 3), (12, 2), (13, 2), (14, 2), (11, 4), (7, 5), (9, 6), (8, 7)]


def sigmoid(value):
    return 1.0 / (1.0 + jnp.exp(-value))


def as_pair(total):
    high = jnp.broadcast_to(total, (total.shape[0], 128)).astype(BF16).astype(F32)
    low = jnp.broadcast_to(total, (total.shape[0], 128)) - high
    lane = lax.broadcasted_iota(jnp.int32, high.shape, 1)
    return jnp.where(lane < 64, high, low).astype(BF16)


def of_pair(pair):
    return pair[:, 0:1] + pair[:, 64:65]


def packed_products(first, second, lane):
    blocks = []
    for j in range(8):
        low = first[:, 128 * j : 128 * j + 128]
        high = second[:, 128 * j : 128 * j + 128]
        top = low[0:32] + pltpu.roll(high[0:32], 64, 1)
        bottom = pltpu.roll(low[32:64], 64, 1) + high[32:64]
        blocks.append(jnp.where(lane < 64, top, bottom))
    return blocks


def kernel(*refs):
    inputs, (result, new_state), refs = refs[:15], refs[15:17], refs[17:]
    held, refs = refs[:15], refs[15:]
    (
        tokens,
        norm_gain,
        w_query,
        w_key,
        w_value,
        w_gate,
        w_decay,
        log_decay,
        state,
        out_gain,
        w_out,
        mixer_gain,
        w_ffgate,
        w_ffup,
        w_down,
    ) = held
    (
        att,
        w_own,
        x_own,
        x_all,
        w_all,
        w_diag,
        part1,
        got1,
        mix,
        w_mix,
        part2,
        got2,
        attn_own,
        attn_all,
        tok_own,
        tok_all,
        middle,
        up_own,
        up_all,
        down_own,
        down_all,
        part3a,
        got3a,
        part3b,
        got3b,
        hid,
        part4,
        got4,
        res_own,
        res_all,
        send_sems,
        recv_sems,
        local_sems,
    ) = refs
    kv = lax.axis_index("kv")
    t = lax.axis_index("tp")
    z, x = lax.div(kv, NX), lax.rem(kv, NX)
    y, core = lax.div(t, 2), lax.rem(t, 2)

    def at_x(d):
        return lax.rem(x + d, NX)

    def at_z(d):
        return lax.rem(z + d, NZ)

    def at_t(d):
        return lax.rem(t + d, NT)

    counter = [0]

    class Exchange:
        def __init__(self, size, group=SMALL):
            self.number, self.group, self.size = counter[0], group, size
            counter[0] += 1

        def send(self, src, dst, peer):
            pltpu.make_async_remote_copy(
                src_ref=src,
                dst_ref=dst,
                send_sem=send_sems.at[self.group],
                recv_sem=recv_sems.at[self.number],
                device_id=peer,
                device_id_type=MESH,
            ).start()

        def arrive(self):
            pltpu.make_async_copy(self.size, self.size, recv_sems.at[self.number]).wait()

    for i, sem in LOADS:
        pltpu.make_async_copy(inputs[i], held[i], local_sems.at[sem]).start()

    barrier = pltpu.get_barrier_semaphore()

    def greet(peer):
        pl.semaphore_signal(barrier, inc=1, device_id=peer, device_id_type=MESH)

    for dz, dx in PLANE:
        greet((at_z(dz) * NX + at_x(dx), t))
    for d in FAR_T:
        greet((kv, at_t(d)))
    def loaded(sem, size):
        pltpu.make_async_copy(size, size, local_sems.at[sem]).wait()

    with jax.named_scope("wait_first"):
        loaded(0, part1.at[0:22])
        loaded(1, norm_gain)
    square = (64, 64)
    row = lax.broadcasted_iota(jnp.int32, square, 0)
    column = lax.broadcasted_iota(jnp.int32, square, 1)
    gain = jnp.sum(
        jnp.where(row == column, jnp.broadcast_to(norm_gain[...].astype(F32), square), 0.0),
        axis=1,
        keepdims=True,
    )

    def gained(weight):
        return (weight[...].astype(F32) * gain).astype(BF16)

    w_own[0, :, 0:128] = gained(w_query)
    w_own[0, :, 128:256] = gained(w_key)
    w_own[1] = gained(w_value)
    w_own[2] = gained(w_gate)
    w_own[3, :, 0:128] = gained(w_decay)
    w_own[3, :, 128:256] = jnp.zeros((64, 128), BF16)
    own = jnp.concatenate([tokens[:, 0:256], tokens[:, 256:512]], axis=0).astype(F32)
    own = jnp.transpose(own, (1, 0))
    x_own[...] = own.reshape(4, 64, 128)
    x_all[x] = own.astype(BF16).reshape(4, 64, 128)
    w_all[x] = w_own[x]

    with jax.named_scope("wait_barrier"):
        pl.semaphore_wait(barrier, len(PLANE) + len(FAR_T))

    tile_z = w_mix.at[:, 0:128]

    def lanes_of(block):
        return pl.ds(pl.multiple_of(block * 128, 128), 128)

    ring_x = [(d, (z * NX + at_x(d), t)) for d in FAR_X]
    ring_z = [(d, (at_z(d) * NX + x, t)) for d in FAR_Z]
    ring_t = [(d, (kv, at_t(d))) for d in FAR_T]
    gather_w = Exchange(w_all.at[0:3], DOWN)
    gather_x = [Exchange(x_all.at[0:3, 0], UP) for _ in X_ORDER]
    x_blocks = [lax.rem(z + steps[0], 4) for steps in X_ORDER]
    for d, peer in ring_x:
        gather_w.send(w_own.at[at_x(d)], w_all.at[x], peer)
    for exchange, r in zip(gather_x, x_blocks):
        for d, peer in ring_x:
            exchange.send(x_all.at[x, r], x_all.at[x, r], peer)

    with jax.named_scope("wait_later"):
        loaded(3, w_out)
    out_rows = jnp.concatenate([w_out[:, 0:128], w_out[:, 128:256]], axis=0).astype(F32)
    w_mix[:, lanes_of(z)] = jnp.transpose(out_rows, (1, 0)).astype(BF16)
    mix_steps = []

    def mix_step(step):
        if step > 1:
            for exchange in mix_steps[-1]:
                exchange.arrive()
        exchanges = []
        for way in (1, -1):
            if step <= (4 if way > 0 else 3):
                lanes = lanes_of(at_z(NZ - way * (step - 1)))
                exchange = Exchange(tile_z)
                exchange.send(
                    w_mix.at[:, lanes], w_mix.at[:, lanes], (at_z(NZ + way) * NX + x, t)
                )
                exchanges.append(exchange)
        mix_steps.append(exchanges)

    mix_step(1)

    with jax.named_scope("wait_later"):
        loaded(2, up_all.at[0, 0:3])
        loaded(4, mixer_gain)
        loaded(5, log_decay)
        loaded(6, out_gain)
    gains = mixer_gain[...].astype(F32)
    units = jnp.transpose(
        jnp.concatenate([w_ffgate[...], w_ffup[...]], axis=0).astype(F32), (1, 0)
    )
    units = (units * jnp.concatenate([gains, gains], axis=1)).astype(BF16)
    down = w_down[...].astype(F32)
    down = jnp.concatenate([down, pltpu.roll(down, 768 - 48, 1)], axis=0)
    down = jnp.transpose(down, (1, 0)).astype(BF16)
    for j in range(NZ):
        up_own[0, j] = units[96 * j : 96 * j + 48]
        up_own[1, j] = units[96 * j + 48 : 96 * j + 96]
        down_own[j] = down[96 * j : 96 * j + 48]
    lanes_z = lanes_of(z)
    for half in range(2):
        up_all[half, t, :, lanes_z] = up_own[half, z]
    down_all[t, :, lanes_z] = down_own[z]
    up_blocks = [Exchange(up_own.at[half, 0:7]) for half in range(2)]
    up_y = [Exchange(up_all.at[half, 0:3], UP) for half in range(2)]
    up_core = [Exchange(up_all.at[half, 0:4], UP) for half in range(2)]
    partner = (kv, t + 1 - 2 * core)

    def along_y(d):
        return lax.rem(y + d, NY) * 2 + core

    def up_along_z(half):
        for d, peer in ring_z:
            up_blocks[half].send(
                up_own.at[half, at_z(d)], up_all.at[half, t, :, lanes_z], peer
            )

    def up_along_y(half):
        with jax.named_scope(f"wait_up_blocks_{half}"):
            up_blocks[half].arrive()
        for d in FAR_Y:
            up_y[half].send(up_all.at[half, t], up_all.at[half, t], (kv, along_y(d)))
        up_core[half].send(up_all.at[half, t], up_all.at[half, t], partner)

    up_along_z(0)
    lane32 = lax.broadcasted_iota(jnp.int32, (32, 128), 1)
    ours = x_own[:, pl.ds(pl.multiple_of(8 * t, 8), 8), :]
    tok_own[...] = ours.reshape(32, 128).astype(BF16)
    tok_all[z] = tok_own[...]
    w_diag[...] = jnp.zeros(w_diag.shape, BF16)

    with jax.named_scope("wait_mix_step"):
        mix_step(2)

    with jax.named_scope("wait_gather1_w"):
        gather_w.arrive()
    for j in range(NX):
        w_diag[j, 0:64, 0:256] = w_all[j]
        w_diag[j, 64:128, 256:512] = w_all[j]
    lane64 = lax.broadcasted_iota(jnp.int32, (64, 128), 1)
    has_sums = x == NX - 1
    scatter1 = Exchange(got1.at[0:31])
    for number, (r, steps) in enumerate(zip(x_blocks, X_ORDER)):
        if number == 3:
            with jax.named_scope("wait_mix_step3"):
                mix_step(3)
        with jax.named_scope(f"wait_gather1_{number}"):
            gather_x[number].arrive()
        total = jnp.zeros((64, 512), F32)
        squares = jnp.zeros((64, 128), F32)
        for j in range(NX):
            block = x_all[j, r]
            total += jnp.dot(block, w_diag[j], preferred_element_type=F32)
            wide = block.astype(F32)
            squares += wide * wide
        for side in range(2):
            ours = (lane64 < 64) if side == 0 else (lane64 >= 64)
            sums = as_pair(jnp.sum(jnp.where(ours, squares, 0.0), axis=1, keepdims=True))
            first = 256 * side
            for k in range(NX):
                rows = slice(16 * k, 16 * k + 16)
                owner = NX * (r + 4 * side) + k
                part1[owner, :, 0:128] = total[rows, first : first + 128].astype(BF16)
                part1[owner, :, 128:256] = jnp.where(
                    has_sums, sums[rows].astype(F32), total[rows, first + 128 : first + 256]
                ).astype(BF16)
        for dz in sorted(steps, key=lambda step: -min(step, NZ - step)):
            for dx in FAR_X + [0]:
                if (dz, dx) != (0, 0):
                    peer = at_z(dz) * NX + at_x(dx)
                    scatter1.send(part1.at[peer], got1.at[x * NZ + z], (peer, t))
    got1[x * NZ + z] = part1[kv]

    up_along_y(0)
    with jax.named_scope("wait_mix_step4"):
        mix_step(4)
    up_along_z(1)

    with jax.named_scope("wait_scatter1"):
        scatter1.arrive()
    proj = []
    for j in range(NX):
        total = got1[NZ * j].astype(F32)
        for k in range(1, NZ):
            total += got1[NZ * j + k].astype(F32)
        proj.append(total)
    loaded(7, state)

    inv = lax.rsqrt(of_pair(proj[3][:, 128:256]) / D + EPS)
    query = proj[0][:, 0:128] * (inv * DK ** (-0.5))
    keys = proj[0][:, 128:256] * inv
    values = proj[1] * inv
    gate = proj[2] * inv
    decay_pre = proj[3][:, 0:128] * inv
    log_sigmoid = jnp.minimum(decay_pre, 0.0) - jnp.log1p(jnp.exp(-jnp.abs(decay_pre)))
    decay = jnp.exp(log_sigmoid / GATE_NORM + log_decay[...])
    columns = jnp.transpose(
        jnp.concatenate([query * decay, keys, decay, jnp.zeros((80, 128), F32)], axis=0), (1, 0)
    )
    for b in range(16):
        att[b : b + 1, :] = jnp.sum(state[b] * columns[:, b : b + 1], axis=0, keepdims=True)
    attended = att[...] + jnp.sum(query * keys, axis=1, keepdims=True) * values
    normed = (
        attended
        * lax.rsqrt(jnp.mean(attended * attended, axis=1, keepdims=True) + EPS)
        * out_gain[...]
    )
    mix[x] = (normed * (gate * sigmoid(gate))).astype(BF16)
    gather2 = Exchange(mix.at[0:3])
    for d, peer in ring_x:
        gather2.send(mix.at[x], mix.at[x], peer)
    down_blocks = Exchange(down_own.at[0:7])
    for d, peer in ring_z:
        down_blocks.send(down_own.at[at_z(d)], down_all.at[t, :, lanes_z], peer)
    tok_blocks = Exchange(tok_all.at[0:7])
    for d, peer in ring_z:
        tok_blocks.send(tok_own, tok_all.at[z], peer)
    for b in range(16):
        k_col = columns[:, 16 + b : 17 + b]
        a_col = columns[:, 32 + b : 33 + b]
        new_state[b] = state[b] * a_col + k_col * values[b : b + 1, :]

    with jax.named_scope("wait_mix_blocks"):
        for exchange in mix_steps[-1]:
            exchange.arrive()
    with jax.named_scope("wait_gather2"):
        gather2.arrive()
    mixed = mix[...].reshape(64, DV)
    stacked = jnp.concatenate([mixed[:, 0:128], mixed[:, 128:256]], axis=0)
    total = jnp.dot(stacked, w_mix[...], preferred_element_type=F32)
    lane64 = lax.broadcasted_iota(jnp.int32, (64, 128), 1)
    pairs = []
    for p in range(4):
        low, high = [
            (total[0:64, first : first + 128], total[64:128, first : first + 128])
            for first in (256 * p, 256 * p + 128)
        ]
        pairs.append(
            jnp.where(
                lane64 < 64,
                low[0] + pltpu.roll(low[1], 64, 1),
                pltpu.roll(high[0], 64, 1) + high[1],
            )
        )
    for j in range(NT):
        rows = slice(8 * j, 8 * j + 8)
        part2[j] = jnp.concatenate([pair[rows] for pair in pairs], axis=0).astype(BF16)
    got2[t] = part2[t]
    scatter2 = Exchange(got2.at[0:7])
    for d, peer in ring_t:
        scatter2.send(part2.at[at_t(d)], got2.at[t], peer)
    up_along_y(1)
    with jax.named_scope("wait_scatter2"):
        scatter2.arrive()
    total = got2[0].astype(F32)
    for j in range(1, NT):
        total += got2[j].astype(F32)
    attn_own[...] = total.astype(BF16)

    attn_all[z] = attn_own[...]
    spread = Exchange(attn_all.at[0:7])
    for d, peer in ring_z:
        spread.send(attn_own, attn_all.at[z], peer)

    with jax.named_scope("wait_down_blocks"):
        down_blocks.arrive()
    down_y, down_core = Exchange(down_all.at[0:3], DOWN), Exchange(down_all.at[0:4], DOWN)
    for d in FAR_Y:
        down_y.send(down_all.at[t], down_all.at[t], (kv, along_y(d)))
    for half in range(2):
        with jax.named_scope(f"wait_up_y_{half}"):
            up_y[half].arrive()
        for d in range(1, NY):
            other = along_y(d)
            up_core[half].send(up_all.at[half, other], up_all.at[half, other], partner)
    down_core.send(down_all.at[t], down_all.at[t], partner)

    with jax.named_scope("wait_tok_blocks"):
        tok_blocks.arrive()
    with jax.named_scope("wait_spread"):
        spread.arrive()

    squares = jnp.zeros((64, 128), F32)
    pieces = []
    sums = [attn_all[j].astype(F32) for j in range(NZ)]
    middles = []
    for p in range(4):
        low, high = tok_all[2 * p].astype(F32), tok_all[2 * p + 1].astype(F32)
        residual = jnp.concatenate(
            [
                jnp.where(lane32 < 64, low, pltpu.roll(high, 64, 1)),
                jnp.where(lane32 < 64, pltpu.roll(low, 64, 1), high),
            ],
            axis=0,
        )
        added = jnp.concatenate([total[8 * p : 8 * p + 8] for total in sums], axis=0)
        wide = (residual + added).astype(BF16).astype(F32)
        middles.append(wide)
        squares += wide * wide
        turned = pltpu.roll(wide, 64, 1)
        for here, there in ((wide, turned), (turned, wide)):
            pieces.append(
                jnp.concatenate(
                    [jnp.where(lane64 < 64, here, 0.0), jnp.where(lane64 < 64, 0.0, there)], axis=0
                ).astype(BF16)
            )
    left = jnp.concatenate(pieces, axis=1)
    squares = as_pair(jnp.sum(squares, axis=1, keepdims=True))
    parts3, gots3 = (part3a, part3b), (got3a, got3b)
    scatter3 = [Exchange(got3.at[0:3]) for got3 in gots3]
    for half, (part3, got3) in enumerate(zip(parts3, gots3)):
        with jax.named_scope(f"wait_up_core_{half}"):
            up_core[half].arrive()
        terms = lax.dot_general(
            left,
            up_all[half].reshape(384, 1024),
            (((1,), (1,)), ((), ())),
            preferred_element_type=F32,
        )
        for j in range(NX):
            rows = slice(16 * j, 16 * j + 16)
            part3[j, :, 0:384] = terms[rows].astype(BF16)
            part3[j, :, 384:768] = terms[64 + 16 * j : 80 + 16 * j].astype(BF16)
            if half == 0:
                part3[j, :, 768:896] = squares[rows]
        got3[x] = part3[x]
        for d, peer in ring_x:
            scatter3[half].send(part3.at[at_x(d)], got3.at[x], peer)
    for p, wide in enumerate(middles):
        turned = pltpu.roll(wide, 64, 1)
        middle[2 * p] = jnp.where(lane32 < 64, wide[0:32], turned[32:64]).astype(BF16)
        middle[2 * p + 1] = jnp.where(lane32 < 64, turned[0:32], wide[32:64]).astype(BF16)
    with jax.named_scope("wait_down_y"):
        down_y.arrive()
    for d in range(1, NY):
        other = along_y(d)
        down_core.send(down_all.at[other], down_all.at[other], partner)
    gather3 = [Exchange(hid.at[half, 0:3]) for half in range(2)]
    inv = None
    for half, got3 in enumerate(gots3):
        with jax.named_scope(f"wait_scatter3_{half}"):
            scatter3[half].arrive()
        total = got3[0].astype(F32)
        for j in range(1, NX):
            total += got3[j].astype(F32)
        if half == 0:
            inv = lax.rsqrt(of_pair(total[:, 768:896]) / D + EPS)
        gate = total[:, 0:384] * inv
        hid[half, x] = (gate * sigmoid(gate) * (total[:, 384:768] * inv)).astype(BF16)
        for d, peer in ring_x:
            gather3[half].send(hid.at[half, x], hid.at[half, x], peer)
    with jax.named_scope("wait_down_core"):
        down_core.arrive()

    weights = down_all[...].reshape(NT * 48, 1024)
    products = []
    for half in range(2):
        with jax.named_scope(f"wait_gather3_{half}"):
            gather3[half].arrive()
        products.append(
            jnp.dot(hid[half].reshape(64, 384), weights, preferred_element_type=F32)
        )
    for j, block in enumerate(packed_products(*products, lane32)):
        part4[j] = block.astype(BF16)
    got4[z] = part4[z]
    scatter4 = Exchange(got4.at[0:7])
    for d, peer in ring_z:
        scatter4.send(part4.at[at_z(d)], got4.at[z], peer)
    with jax.named_scope("wait_scatter4"):
        scatter4.arrive()
    total = got4[0].astype(F32)
    for j in range(1, NZ):
        total += got4[j].astype(F32)
    res_own[...] = (middle[z].astype(F32) + total).astype(BF16)
    res_all[t] = res_own[...]
    gather4 = Exchange(res_all.at[0:7], LAST)
    for d, peer in ring_t:
        gather4.send(res_own, res_all.at[t], peer)
    with jax.named_scope("wait_gather4"):
        gather4.arrive()
    blocks = [res_all[j].astype(F32) for j in range(NT)]
    blocks = [blocks, [pltpu.roll(block, 64, 1) for block in blocks]]
    rows = jnp.concatenate(
        [
            blocks[j // 4][k][8 * (j % 4) : 8 * (j % 4) + 8]
            for j in range(NZ)
            for k in range(NT)
        ],
        axis=0,
    )
    result[...] = jnp.transpose(rows, (1, 0))[0:64].astype(BF16)
    with jax.named_scope("wait_sends"):
        everything = (state.at[0:15, 0:80], up_all, up_all.at[0], res_all.at[0:7])
        for group, size in enumerate(everything):
            pltpu.make_async_copy(size, size, send_sems.at[group]).wait()


def finish(result_in, state_in, result_out, state_out, sems):
    result = pltpu.make_async_copy(result_in, result_out, sems.at[0])
    states = pltpu.make_async_copy(state_in, state_out, sems.at[1])
    parts = [pl.ds(2 * i, 2) for i in range(8)]
    result.start()
    for part in parts:
        pltpu.make_async_copy(state_in.at[part], state_out.at[part], sems.at[1]).start()
    result.wait()
    states.wait()


def body(
    tokens,
    norm_gain,
    w_query,
    w_key,
    w_value,
    w_gate,
    w_decay,
    log_decay,
    state,
    out_gain,
    w_out,
    mixer_gain,
    w_ffgate,
    w_ffup,
    w_down,
):
    vmem = pl.BlockSpec(memory_space=pltpu.VMEM)
    hbm = pl.BlockSpec(memory_space=pltpu.HBM)
    shape = state.shape
    arguments = (
        tokens.T,
        norm_gain.reshape(1, 64),
        w_query,
        w_key,
        w_value,
        w_gate,
        w_decay,
        log_decay,
        state.reshape(shape[0], DK, DV),
        out_gain.reshape(1, DV),
        w_out.T,
        mixer_gain.reshape(1, 64),
        w_ffgate,
        w_ffup,
        w_down.T,
    )
    arguments = [pltpu.with_memory_space_constraint(value, pltpu.HBM) for value in arguments]
    result, new_state = pl.pallas_call(
        kernel,
        out_shape=(
            pltpu.VMEM((64, 512), BF16),
            pltpu.VMEM((shape[0], DK, DV), F32),
        ),
        in_specs=[hbm] * 15,
        out_specs=(vmem, vmem),
        scratch_shapes=[pltpu.VMEM(value.shape, value.dtype) for value in arguments]
        + [
            pltpu.VMEM((16, DV), F32),
            pltpu.VMEM((NX, 64, 256), BF16),
            pltpu.VMEM((4, 64, 128), F32),
            pltpu.VMEM((NX, 4, 64, 128), BF16),
            pltpu.VMEM((NX, 64, 256), BF16),
            pltpu.VMEM((NX, 128, 512), BF16),
            pltpu.VMEM((NZ * NX, 16, 256), BF16),
            pltpu.VMEM((NX * NZ, 16, 256), BF16),
            pltpu.VMEM((NX, 16, 256), BF16),
            pltpu.VMEM((128, 1024), BF16),
            pltpu.VMEM((NT, 32, 128), BF16),
            pltpu.VMEM((NT, 32, 128), BF16),
            pltpu.VMEM((32, 128), BF16),
            pltpu.VMEM((NT, 32, 128), BF16),
            pltpu.VMEM((32, 128), BF16),
            pltpu.VMEM((NZ, 32, 128), BF16),
            pltpu.VMEM((NZ, 32, 128), BF16),
            pltpu.VMEM((2, NZ, 48, 128), BF16),
            pltpu.VMEM((2, NT, 48, 1024), BF16),
            pltpu.VMEM((NZ, 48, 128), BF16),
            pltpu.VMEM((NT, 48, 1024), BF16),
            pltpu.VMEM((NX, 16, 896), BF16),
            pltpu.VMEM((NX, 16, 896), BF16),
            pltpu.VMEM((NX, 16, 768), BF16),
            pltpu.VMEM((NX, 16, 768), BF16),
            pltpu.VMEM((2, NX, 16, 384), BF16),
            pltpu.VMEM((NZ, 32, 128), BF16),
            pltpu.VMEM((NZ, 32, 128), BF16),
            pltpu.VMEM((32, 128), BF16),
            pltpu.VMEM((NT, 32, 128), BF16),
            pltpu.SemaphoreType.DMA((4,)),
            pltpu.SemaphoreType.DMA((COPIES,)),
            pltpu.SemaphoreType.DMA((8,)),
        ],
        compiler_params=pltpu.CompilerParams(
            collective_id=0, has_side_effects=True, vmem_limit_bytes=40 * 1024 * 1024
        ),
    )(*arguments)
    result, new_state = pl.pallas_call(
        finish,
        out_shape=(
            jax.ShapeDtypeStruct((64, 512), BF16),
            jax.ShapeDtypeStruct((shape[0], DK, DV), F32),
        ),
        in_specs=[vmem, vmem],
        out_specs=(hbm, hbm),
        scratch_shapes=[pltpu.SemaphoreType.DMA((2,))],
        compiler_params=pltpu.CompilerParams(vmem_limit_bytes=8 * 1024 * 1024),
    )(result, new_state)
    return (result.T, new_state.reshape(shape))


def solution(mesh):
    return jax.shard_map(
        body,
        mesh=mesh,
        in_specs=(
            P(None, "kv"),
            P("kv"),
            P("kv", "tp"),
            P("kv", "tp"),
            P("kv", "tp"),
            P("kv", "tp"),
            P("kv", "tp"),
            P("kv", "tp"),
            P("kv", "tp", None, None),
            P(),
            P("tp", "kv"),
            P("kv"),
            P("kv", "tp"),
            P("kv", "tp"),
            P("tp", "kv"),
        ),
        out_specs=(P(None, "kv"), P("kv", "tp", None, None)),
        check_vma=False,
    )
```

```python
import functools

import jax
import jax.numpy as jnp
from jax import lax
from jax.experimental import pallas as pl
from jax.experimental.pallas import tpu as pltpu
from jax.sharding import PartitionSpec as P

MESH = pl.DeviceIdType.MESH
F32 = jnp.float32
BF16 = jnp.bfloat16

D = 2048
DK = 128
DV = 256
EPS = 1e-06
GATE_NORM = 16.0

NX, NY, NZ = 4, 4, 8
NT = 2 * NY
COPIES = 32
SMALL, UP, DOWN, LAST = range(4)
FAR_X = [2, 1, 3]
FAR_Y = [2, 1, 3]
FAR_Z = [4, 3, 5, 2, 6, 1, 7]
FAR_T = [4, 5, 2, 3, 6, 7, 1]
X_ORDER = [(0, 4), (2, 6), (3, 7), (1, 5)]
PLANE = [(dz, dx) for dz in FAR_Z + [0] for dx in FAR_X + [0] if (dz, dx) != (0, 0)]
LOADS = [(0, 0), (1, 1), (2, 0), (3, 0), (4, 0), (5, 0), (6, 0)]
LOADS += [(10, 3), (12, 2), (13, 2), (14, 2), (11, 4), (7, 5), (9, 6), (8, 7)]


def sigmoid(value):
    return 1.0 / (1.0 + jnp.exp(-value))


def as_pair(total):
    high = jnp.broadcast_to(total, (total.shape[0], 128)).astype(BF16).astype(F32)
    low = jnp.broadcast_to(total, (total.shape[0], 128)) - high
    lane = lax.broadcasted_iota(jnp.int32, high.shape, 1)
    return jnp.where(lane < 64, high, low).astype(BF16)


def of_pair(pair):
    return pair[:, 0:1] + pair[:, 64:65]


def packed_products(first, second, lane):
    blocks = []
    for j in range(8):
        low = first[:, 128 * j : 128 * j + 128]
        high = second[:, 128 * j : 128 * j + 128]
        top = low[0:32] + pltpu.roll(high[0:32], 64, 1)
        bottom = pltpu.roll(low[32:64], 64, 1) + high[32:64]
        blocks.append(jnp.where(lane < 64, top, bottom))
    return blocks


def kernel(*refs):
    inputs, (result, new_state), refs = refs[:15], refs[15:17], refs[17:]
    held, refs = refs[:15], refs[15:]
    (
        tokens,
        norm_gain,
        w_query,
        w_key,
        w_value,
        w_gate,
        w_decay,
        log_decay,
        state,
        out_gain,
        w_out,
        mixer_gain,
        w_ffgate,
        w_ffup,
        w_down,
    ) = held
    (
        att,
        w_own,
        x_own,
        x_all,
        w_all,
        w_diag,
        part1,
        got1,
        mix,
        w_mix,
        part2,
        got2,
        attn_own,
        attn_all,
        tok_own,
        tok_all,
        middle,
        up_own,
        up_all,
        down_own,
        down_all,
        part3a,
        got3a,
        part3b,
        got3b,
        hid,
        part4,
        got4,
        res_own,
        res_all,
        send_sems,
        recv_sems,
        local_sems,
    ) = refs
    kv = lax.axis_index("kv")
    t = lax.axis_index("tp")
    z, x = lax.div(kv, NX), lax.rem(kv, NX)
    y, core = lax.div(t, 2), lax.rem(t, 2)

    def at_x(d):
        return lax.rem(x + d, NX)

    def at_z(d):
        return lax.rem(z + d, NZ)

    def at_t(d):
        return lax.rem(t + d, NT)

    counter = [0]

    class Exchange:
        def __init__(self, size, group=SMALL):
            self.number, self.group, self.size = counter[0], group, size
            counter[0] += 1

        def send(self, src, dst, peer):
            pltpu.make_async_remote_copy(
                src_ref=src,
                dst_ref=dst,
                send_sem=send_sems.at[self.group],
                recv_sem=recv_sems.at[self.number],
                device_id=peer,
                device_id_type=MESH,
            ).start()

        def arrive(self):
            pltpu.make_async_copy(self.size, self.size, recv_sems.at[self.number]).wait()

    for i, sem in LOADS:
        pltpu.make_async_copy(inputs[i], held[i], local_sems.at[sem]).start()

    barrier = pltpu.get_barrier_semaphore()

    def greet(peer):
        pl.semaphore_signal(barrier, inc=1, device_id=peer, device_id_type=MESH)

    for dz, dx in PLANE:
        greet((at_z(dz) * NX + at_x(dx), t))
    for d in FAR_T:
        greet((kv, at_t(d)))
    def loaded(sem, size):
        pltpu.make_async_copy(size, size, local_sems.at[sem]).wait()

    with jax.named_scope("wait_first"):
        loaded(0, part1.at[0:22])
        loaded(1, norm_gain)
    square = (64, 64)
    row = lax.broadcasted_iota(jnp.int32, square, 0)
    column = lax.broadcasted_iota(jnp.int32, square, 1)
    gain = jnp.sum(
        jnp.where(row == column, jnp.broadcast_to(norm_gain[...].astype(F32), square), 0.0),
        axis=1,
        keepdims=True,
    )

    def gained(weight):
        return (weight[...].astype(F32) * gain).astype(BF16)

    w_own[0, :, 0:128] = gained(w_query)
    w_own[0, :, 128:256] = gained(w_key)
    w_own[1] = gained(w_value)
    w_own[2] = gained(w_gate)
    w_own[3, :, 0:128] = gained(w_decay)
    w_own[3, :, 128:256] = jnp.zeros((64, 128), BF16)
    own = jnp.concatenate([tokens[:, 0:256], tokens[:, 256:512]], axis=0).astype(F32)
    own = jnp.transpose(own, (1, 0))
    x_own[...] = own.reshape(4, 64, 128)
    x_all[x] = own.astype(BF16).reshape(4, 64, 128)
    w_all[x] = w_own[x]

    with jax.named_scope("wait_barrier"):
        pl.semaphore_wait(barrier, len(PLANE) + len(FAR_T))

    tile_z = w_mix.at[:, 0:128]

    def lanes_of(block):
        return pl.ds(pl.multiple_of(block * 128, 128), 128)

    ring_x = [(d, (z * NX + at_x(d), t)) for d in FAR_X]
    ring_z = [(d, (at_z(d) * NX + x, t)) for d in FAR_Z]
    ring_t = [(d, (kv, at_t(d))) for d in FAR_T]
    gather_w = Exchange(w_all.at[0:3], DOWN)
    gather_x = [Exchange(x_all.at[0:3, 0], UP) for _ in X_ORDER]
    x_blocks = [lax.rem(z + steps[0], 4) for steps in X_ORDER]
    for d, peer in ring_x:
        gather_w.send(w_own.at[at_x(d)], w_all.at[x], peer)
    for exchange, r in zip(gather_x, x_blocks):
        for d, peer in ring_x:
            exchange.send(x_all.at[x, r], x_all.at[x, r], peer)

    with jax.named_scope("wait_later"):
        loaded(3, w_out)
    out_rows = jnp.concatenate([w_out[:, 0:128], w_out[:, 128:256]], axis=0).astype(F32)
    w_mix[:, lanes_of(z)] = jnp.transpose(out_rows, (1, 0)).astype(BF16)
    mix_steps = []

    def mix_step(step):
        if step > 1:
            for exchange in mix_steps[-1]:
                exchange.arrive()
        exchanges = []
        for way in (1, -1):
            if step <= (4 if way > 0 else 3):
                lanes = lanes_of(at_z(NZ - way * (step - 1)))
                exchange = Exchange(tile_z)
                exchange.send(
                    w_mix.at[:, lanes], w_mix.at[:, lanes], (at_z(NZ + way) * NX + x, t)
                )
                exchanges.append(exchange)
        mix_steps.append(exchanges)

    mix_step(1)

    with jax.named_scope("wait_later"):
        loaded(2, up_all.at[0, 0:3])
        loaded(4, mixer_gain)
        loaded(5, log_decay)
        loaded(6, out_gain)
    gains = mixer_gain[...].astype(F32)
    units = jnp.transpose(
        jnp.concatenate([w_ffgate[...], w_ffup[...]], axis=0).astype(F32), (1, 0)
    )
    units = (units * jnp.concatenate([gains, gains], axis=1)).astype(BF16)
    down = w_down[...].astype(F32)
    down = jnp.concatenate([down, pltpu.roll(down, 768 - 48, 1)], axis=0)
    down = jnp.transpose(down, (1, 0)).astype(BF16)
    for j in range(NZ):
        up_own[0, j] = units[96 * j : 96 * j + 48]
        up_own[1, j] = units[96 * j + 48 : 96 * j + 96]
        down_own[j] = down[96 * j : 96 * j + 48]
    lanes_z = lanes_of(z)
    for half in range(2):
        up_all[half, t, :, lanes_z] = up_own[half, z]
    down_all[t, :, lanes_z] = down_own[z]
    up_blocks = [Exchange(up_own.at[half, 0:7]) for half in range(2)]
    up_y = [Exchange(up_all.at[half, 0:3], UP) for half in range(2)]
    up_core = [Exchange(up_all.at[half, 0:4], UP) for half in range(2)]
    partner = (kv, t + 1 - 2 * core)

    def along_y(d):
        return lax.rem(y + d, NY) * 2 + core

    def up_along_z(half):
        for d, peer in ring_z:
            up_blocks[half].send(
                up_own.at[half, at_z(d)], up_all.at[half, t, :, lanes_z], peer
            )

    def up_along_y(half):
        with jax.named_scope(f"wait_up_blocks_{half}"):
            up_blocks[half].arrive()
        for d in FAR_Y:
            up_y[half].send(up_all.at[half, t], up_all.at[half, t], (kv, along_y(d)))
        up_core[half].send(up_all.at[half, t], up_all.at[half, t], partner)

    up_along_z(0)
    lane32 = lax.broadcasted_iota(jnp.int32, (32, 128), 1)
    ours = x_own[:, pl.ds(pl.multiple_of(8 * t, 8), 8), :]
    tok_own[...] = ours.reshape(32, 128).astype(BF16)
    tok_all[z] = tok_own[...]
    w_diag[...] = jnp.zeros(w_diag.shape, BF16)

    with jax.named_scope("wait_mix_step"):
        mix_step(2)

    with jax.named_scope("wait_gather1_w"):
        gather_w.arrive()
    for j in range(NX):
        w_diag[j, 0:64, 0:256] = w_all[j]
        w_diag[j, 64:128, 256:512] = w_all[j]
    lane64 = lax.broadcasted_iota(jnp.int32, (64, 128), 1)
    has_sums = x == NX - 1
    scatter1 = Exchange(got1.at[0:31])
    for number, (r, steps) in enumerate(zip(x_blocks, X_ORDER)):
        with jax.named_scope(f"wait_gather1_{number}"):
            gather_x[number].arrive()
        total = jnp.zeros((64, 512), F32)
        squares = jnp.zeros((64, 128), F32)
        for j in range(NX):
            block = x_all[j, r]
            total += jnp.dot(block, w_diag[j], preferred_element_type=F32)
            wide = block.astype(F32)
            squares += wide * wide
        for side in range(2):
            ours = (lane64 < 64) if side == 0 else (lane64 >= 64)
            sums = as_pair(jnp.sum(jnp.where(ours, squares, 0.0), axis=1, keepdims=True))
            first = 256 * side
            for k in range(NX):
                rows = slice(16 * k, 16 * k + 16)
                owner = NX * (r + 4 * side) + k
                part1[owner, :, 0:128] = total[rows, first : first + 128].astype(BF16)
                part1[owner, :, 128:256] = jnp.where(
                    has_sums, sums[rows].astype(F32), total[rows, first + 128 : first + 256]
                ).astype(BF16)
        for dz in sorted(steps, key=lambda step: -min(step, NZ - step)):
            for dx in FAR_X + [0]:
                if (dz, dx) != (0, 0):
                    peer = at_z(dz) * NX + at_x(dx)
                    scatter1.send(part1.at[peer], got1.at[x * NZ + z], (peer, t))
    got1[x * NZ + z] = part1[kv]

    with jax.named_scope("wait_mix_step3"):
        mix_step(3)
    up_along_y(0)
    with jax.named_scope("wait_mix_step4"):
        mix_step(4)
    up_along_z(1)

    with jax.named_scope("wait_scatter1"):
        scatter1.arrive()
    proj = []
    for j in range(NX):
        total = got1[NZ * j].astype(F32)
        for k in range(1, NZ):
            total += got1[NZ * j + k].astype(F32)
        proj.append(total)
    loaded(7, state)

    inv = lax.rsqrt(of_pair(proj[3][:, 128:256]) / D + EPS)
    query = proj[0][:, 0:128] * (inv * DK ** (-0.5))
    keys = proj[0][:, 128:256] * inv
    values = proj[1] * inv
    gate = proj[2] * inv
    decay_pre = proj[3][:, 0:128] * inv
    log_sigmoid = jnp.minimum(decay_pre, 0.0) - jnp.log1p(jnp.exp(-jnp.abs(decay_pre)))
    decay = jnp.exp(log_sigmoid / GATE_NORM + log_decay[...])
    columns = jnp.transpose(
        jnp.concatenate([query * decay, keys, decay, jnp.zeros((80, 128), F32)], axis=0), (1, 0)
    )
    for b in range(16):
        att[b : b + 1, :] = jnp.sum(state[b] * columns[:, b : b + 1], axis=0, keepdims=True)
    attended = att[...] + jnp.sum(query * keys, axis=1, keepdims=True) * values
    normed = (
        attended
        * lax.rsqrt(jnp.mean(attended * attended, axis=1, keepdims=True) + EPS)
        * out_gain[...]
    )
    mix[x] = (normed * (gate * sigmoid(gate))).astype(BF16)
    gather2 = Exchange(mix.at[0:3])
    for d, peer in ring_x:
        gather2.send(mix.at[x], mix.at[x], peer)
    down_blocks = Exchange(down_own.at[0:7])
    for d, peer in ring_z:
        down_blocks.send(down_own.at[at_z(d)], down_all.at[t, :, lanes_z], peer)
    tok_blocks = Exchange(tok_all.at[0:7])
    for d, peer in ring_z:
        tok_blocks.send(tok_own, tok_all.at[z], peer)
    for b in range(16):
        k_col = columns[:, 16 + b : 17 + b]
        a_col = columns[:, 32 + b : 33 + b]
        new_state[b] = state[b] * a_col + k_col * values[b : b + 1, :]

    with jax.named_scope("wait_mix_blocks"):
        for exchange in mix_steps[-1]:
            exchange.arrive()
    with jax.named_scope("wait_gather2"):
        gather2.arrive()
    mixed = mix[...].reshape(64, DV)
    stacked = jnp.concatenate([mixed[:, 0:128], mixed[:, 128:256]], axis=0)
    total = jnp.dot(stacked, w_mix[...], preferred_element_type=F32)
    lane64 = lax.broadcasted_iota(jnp.int32, (64, 128), 1)
    pairs = []
    for p in range(4):
        low, high = [
            (total[0:64, first : first + 128], total[64:128, first : first + 128])
            for first in (256 * p, 256 * p + 128)
        ]
        pairs.append(
            jnp.where(
                lane64 < 64,
                low[0] + pltpu.roll(low[1], 64, 1),
                pltpu.roll(high[0], 64, 1) + high[1],
            )
        )
    for j in range(NT):
        rows = slice(8 * j, 8 * j + 8)
        part2[j] = jnp.concatenate([pair[rows] for pair in pairs], axis=0).astype(BF16)
    got2[t] = part2[t]
    scatter2 = Exchange(got2.at[0:7])
    for d, peer in ring_t:
        scatter2.send(part2.at[at_t(d)], got2.at[t], peer)
    up_along_y(1)
    with jax.named_scope("wait_scatter2"):
        scatter2.arrive()
    total = got2[0].astype(F32)
    for j in range(1, NT):
        total += got2[j].astype(F32)
    attn_own[...] = total.astype(BF16)

    attn_all[z] = attn_own[...]
    spread = Exchange(attn_all.at[0:7])
    for d, peer in ring_z:
        spread.send(attn_own, attn_all.at[z], peer)

    with jax.named_scope("wait_down_blocks"):
        down_blocks.arrive()
    down_y, down_core = Exchange(down_all.at[0:3], DOWN), Exchange(down_all.at[0:4], DOWN)
    for d in FAR_Y:
        down_y.send(down_all.at[t], down_all.at[t], (kv, along_y(d)))
    for half in range(2):
        with jax.named_scope(f"wait_up_y_{half}"):
            up_y[half].arrive()
        for d in range(1, NY):
            other = along_y(d)
            up_core[half].send(up_all.at[half, other], up_all.at[half, other], partner)
    down_core.send(down_all.at[t], down_all.at[t], partner)

    with jax.named_scope("wait_tok_blocks"):
        tok_blocks.arrive()
    with jax.named_scope("wait_spread"):
        spread.arrive()

    squares = jnp.zeros((64, 128), F32)
    pieces = []
    sums = [attn_all[j].astype(F32) for j in range(NZ)]
    middles = []
    for p in range(4):
        low, high = tok_all[2 * p].astype(F32), tok_all[2 * p + 1].astype(F32)
        residual = jnp.concatenate(
            [
                jnp.where(lane32 < 64, low, pltpu.roll(high, 64, 1)),
                jnp.where(lane32 < 64, pltpu.roll(low, 64, 1), high),
            ],
            axis=0,
        )
        added = jnp.concatenate([total[8 * p : 8 * p + 8] for total in sums], axis=0)
        wide = (residual + added).astype(BF16).astype(F32)
        middles.append(wide)
        squares += wide * wide
        turned = pltpu.roll(wide, 64, 1)
        for here, there in ((wide, turned), (turned, wide)):
            pieces.append(
                jnp.concatenate(
                    [jnp.where(lane64 < 64, here, 0.0), jnp.where(lane64 < 64, 0.0, there)], axis=0
                ).astype(BF16)
            )
    left = jnp.concatenate(pieces, axis=1)
    squares = as_pair(jnp.sum(squares, axis=1, keepdims=True))
    parts3, gots3 = (part3a, part3b), (got3a, got3b)
    scatter3 = [Exchange(got3.at[0:3]) for got3 in gots3]
    for half, (part3, got3) in enumerate(zip(parts3, gots3)):
        with jax.named_scope(f"wait_up_core_{half}"):
            up_core[half].arrive()
        terms = lax.dot_general(
            left,
            up_all[half].reshape(384, 1024),
            (((1,), (1,)), ((), ())),
            preferred_element_type=F32,
        )
        for j in range(NX):
            rows = slice(16 * j, 16 * j + 16)
            part3[j, :, 0:384] = terms[rows].astype(BF16)
            part3[j, :, 384:768] = terms[64 + 16 * j : 80 + 16 * j].astype(BF16)
            if half == 0:
                part3[j, :, 768:896] = squares[rows]
        got3[x] = part3[x]
        for d, peer in ring_x:
            scatter3[half].send(part3.at[at_x(d)], got3.at[x], peer)
    for p, wide in enumerate(middles):
        turned = pltpu.roll(wide, 64, 1)
        middle[2 * p] = jnp.where(lane32 < 64, wide[0:32], turned[32:64]).astype(BF16)
        middle[2 * p + 1] = jnp.where(lane32 < 64, turned[0:32], wide[32:64]).astype(BF16)
    with jax.named_scope("wait_down_y"):
        down_y.arrive()
    for d in range(1, NY):
        other = along_y(d)
        down_core.send(down_all.at[other], down_all.at[other], partner)
    gather3 = [Exchange(hid.at[half, 0:3]) for half in range(2)]
    inv = None
    for half, got3 in enumerate(gots3):
        with jax.named_scope(f"wait_scatter3_{half}"):
            scatter3[half].arrive()
        total = got3[0].astype(F32)
        for j in range(1, NX):
            total += got3[j].astype(F32)
        if half == 0:
            inv = lax.rsqrt(of_pair(total[:, 768:896]) / D + EPS)
        gate = total[:, 0:384] * inv
        hid[half, x] = (gate * sigmoid(gate) * (total[:, 384:768] * inv)).astype(BF16)
        for d, peer in ring_x:
            gather3[half].send(hid.at[half, x], hid.at[half, x], peer)
    with jax.named_scope("wait_down_core"):
        down_core.arrive()

    weights = down_all[...].reshape(NT * 48, 1024)
    products = []
    for half in range(2):
        with jax.named_scope(f"wait_gather3_{half}"):
            gather3[half].arrive()
        products.append(
            jnp.dot(hid[half].reshape(64, 384), weights, preferred_element_type=F32)
        )
    for j, block in enumerate(packed_products(*products, lane32)):
        part4[j] = block.astype(BF16)
    got4[z] = part4[z]
    scatter4 = Exchange(got4.at[0:7])
    for d, peer in ring_z:
        scatter4.send(part4.at[at_z(d)], got4.at[z], peer)
    with jax.named_scope("wait_scatter4"):
        scatter4.arrive()
    total = got4[0].astype(F32)
    for j in range(1, NZ):
        total += got4[j].astype(F32)
    res_own[...] = (middle[z].astype(F32) + total).astype(BF16)
    res_all[t] = res_own[...]
    gather4 = Exchange(res_all.at[0:7], LAST)
    for d, peer in ring_t:
        gather4.send(res_own, res_all.at[t], peer)
    with jax.named_scope("wait_gather4"):
        gather4.arrive()
    blocks = [res_all[j].astype(F32) for j in range(NT)]
    blocks = [blocks, [pltpu.roll(block, 64, 1) for block in blocks]]
    rows = jnp.concatenate(
        [
            blocks[j // 4][k][8 * (j % 4) : 8 * (j % 4) + 8]
            for j in range(NZ)
            for k in range(NT)
        ],
        axis=0,
    )
    result[...] = jnp.transpose(rows, (1, 0))[0:64].astype(BF16)
    with jax.named_scope("wait_sends"):
        everything = (state.at[0:15, 0:80], up_all, up_all.at[0], res_all.at[0:7])
        for group, size in enumerate(everything):
            pltpu.make_async_copy(size, size, send_sems.at[group]).wait()


def finish(result_in, state_in, result_out, state_out, sems):
    result = pltpu.make_async_copy(result_in, result_out, sems.at[0])
    states = pltpu.make_async_copy(state_in, state_out, sems.at[1])
    parts = [pl.ds(2 * i, 2) for i in range(8)]
    result.start()
    for part in parts:
        pltpu.make_async_copy(state_in.at[part], state_out.at[part], sems.at[1]).start()
    result.wait()
    states.wait()


def body(
    tokens,
    norm_gain,
    w_query,
    w_key,
    w_value,
    w_gate,
    w_decay,
    log_decay,
    state,
    out_gain,
    w_out,
    mixer_gain,
    w_ffgate,
    w_ffup,
    w_down,
):
    vmem = pl.BlockSpec(memory_space=pltpu.VMEM)
    hbm = pl.BlockSpec(memory_space=pltpu.HBM)
    shape = state.shape
    arguments = (
        tokens.T,
        norm_gain.reshape(1, 64),
        w_query,
        w_key,
        w_value,
        w_gate,
        w_decay,
        log_decay,
        state.reshape(shape[0], DK, DV),
        out_gain.reshape(1, DV),
        w_out.T,
        mixer_gain.reshape(1, 64),
        w_ffgate,
        w_ffup,
        w_down.T,
    )
    arguments = [pltpu.with_memory_space_constraint(value, pltpu.HBM) for value in arguments]
    result, new_state = pl.pallas_call(
        kernel,
        out_shape=(
            pltpu.VMEM((64, 512), BF16),
            pltpu.VMEM((shape[0], DK, DV), F32),
        ),
        in_specs=[hbm] * 15,
        out_specs=(vmem, vmem),
        scratch_shapes=[pltpu.VMEM(value.shape, value.dtype) for value in arguments]
        + [
            pltpu.VMEM((16, DV), F32),
            pltpu.VMEM((NX, 64, 256), BF16),
            pltpu.VMEM((4, 64, 128), F32),
            pltpu.VMEM((NX, 4, 64, 128), BF16),
            pltpu.VMEM((NX, 64, 256), BF16),
            pltpu.VMEM((NX, 128, 512), BF16),
            pltpu.VMEM((NZ * NX, 16, 256), BF16),
            pltpu.VMEM((NX * NZ, 16, 256), BF16),
            pltpu.VMEM((NX, 16, 256), BF16),
            pltpu.VMEM((128, 1024), BF16),
            pltpu.VMEM((NT, 32, 128), BF16),
            pltpu.VMEM((NT, 32, 128), BF16),
            pltpu.VMEM((32, 128), BF16),
            pltpu.VMEM((NT, 32, 128), BF16),
            pltpu.VMEM((32, 128), BF16),
            pltpu.VMEM((NZ, 32, 128), BF16),
            pltpu.VMEM((NZ, 32, 128), BF16),
            pltpu.VMEM((2, NZ, 48, 128), BF16),
            pltpu.VMEM((2, NT, 48, 1024), BF16),
            pltpu.VMEM((NZ, 48, 128), BF16),
            pltpu.VMEM((NT, 48, 1024), BF16),
            pltpu.VMEM((NX, 16, 896), BF16),
            pltpu.VMEM((NX, 16, 896), BF16),
            pltpu.VMEM((NX, 16, 768), BF16),
            pltpu.VMEM((NX, 16, 768), BF16),
            pltpu.VMEM((2, NX, 16, 384), BF16),
            pltpu.VMEM((NZ, 32, 128), BF16),
            pltpu.VMEM((NZ, 32, 128), BF16),
            pltpu.VMEM((32, 128), BF16),
            pltpu.VMEM((NT, 32, 128), BF16),
            pltpu.SemaphoreType.DMA((4,)),
            pltpu.SemaphoreType.DMA((COPIES,)),
            pltpu.SemaphoreType.DMA((8,)),
        ],
        compiler_params=pltpu.CompilerParams(
            collective_id=0, has_side_effects=True, vmem_limit_bytes=40 * 1024 * 1024
        ),
    )(*arguments)
    result, new_state = pl.pallas_call(
        finish,
        out_shape=(
            jax.ShapeDtypeStruct((64, 512), BF16),
            jax.ShapeDtypeStruct((shape[0], DK, DV), F32),
        ),
        in_specs=[vmem, vmem],
        out_specs=(hbm, hbm),
        scratch_shapes=[pltpu.SemaphoreType.DMA((2,))],
        compiler_params=pltpu.CompilerParams(vmem_limit_bytes=8 * 1024 * 1024),
    )(result, new_state)
    return (result.T, new_state.reshape(shape))


def solution(mesh):
    return jax.shard_map(
        body,
        mesh=mesh,
        in_specs=(
            P(None, "kv"),
            P("kv"),
            P("kv", "tp"),
            P("kv", "tp"),
            P("kv", "tp"),
            P("kv", "tp"),
            P("kv", "tp"),
            P("kv", "tp"),
            P("kv", "tp", None, None),
            P(),
            P("tp", "kv"),
            P("kv"),
            P("kv", "tp"),
            P("kv", "tp"),
            P("tp", "kv"),
        ),
        out_specs=(P(None, "kv"), P("kv", "tp", None, None)),
        check_vma=False,
    )
```

```python
import functools

import jax
import jax.numpy as jnp
from jax import lax
from jax.experimental import pallas as pl
from jax.experimental.pallas import tpu as pltpu
from jax.sharding import PartitionSpec as P

MESH = pl.DeviceIdType.MESH
F32 = jnp.float32
BF16 = jnp.bfloat16

D = 2048
DK = 128
DV = 256
EPS = 1e-06
GATE_NORM = 16.0

NX, NY, NZ = 4, 4, 8
NT = 2 * NY
COPIES = 35
PARTS = (32, 16)
SMALL, UP, DOWN, LAST = range(4)
FAR_X = [2, 1, 3]
FAR_Y = [2, 1, 3]
FAR_Z = [4, 3, 5, 2, 6, 1, 7]
FAR_T = [4, 5, 2, 3, 6, 7, 1]
X_ORDER = [(0, 4), (2, 6), (3, 7), (1, 5)]
PLANE = [(dz, dx) for dz in FAR_Z + [0] for dx in FAR_X + [0] if (dz, dx) != (0, 0)]
LOADS = [(0, 0), (1, 1), (2, 0), (3, 0), (4, 0), (5, 0), (6, 0)]
LOADS += [(10, 3), (12, 2), (13, 2), (14, 2), (11, 4), (7, 5), (9, 6), (8, 7)]


def sigmoid(value):
    return 1.0 / (1.0 + jnp.exp(-value))


def as_pair(total):
    high = jnp.broadcast_to(total, (total.shape[0], 128)).astype(BF16).astype(F32)
    low = jnp.broadcast_to(total, (total.shape[0], 128)) - high
    lane = lax.broadcasted_iota(jnp.int32, high.shape, 1)
    return jnp.where(lane < 64, high, low).astype(BF16)


def of_pair(pair):
    return pair[:, 0:1] + pair[:, 64:65]


def packed_products(first, second, lane):
    blocks = []
    for j in range(8):
        low = first[:, 128 * j : 128 * j + 128]
        high = second[:, 128 * j : 128 * j + 128]
        top = low[0:32] + pltpu.roll(high[0:32], 64, 1)
        bottom = pltpu.roll(low[32:64], 64, 1) + high[32:64]
        blocks.append(jnp.where(lane < 64, top, bottom))
    return blocks


def kernel(*refs):
    inputs, (result, new_state), refs = refs[:15], refs[15:17], refs[17:]
    held, refs = refs[:15], refs[15:]
    (
        tokens,
        norm_gain,
        w_query,
        w_key,
        w_value,
        w_gate,
        w_decay,
        log_decay,
        state,
        out_gain,
        w_out,
        mixer_gain,
        w_ffgate,
        w_ffup,
        w_down,
    ) = held
    (
        att,
        w_own,
        x_own,
        x_all,
        w_all,
        w_diag,
        part1,
        got1,
        mix,
        w_mix,
        part2,
        got2,
        attn_own,
        attn_all,
        tok_own,
        tok_all,
        middle,
        up_own0,
        up_own1,
        up_all0,
        up_all1,
        down_own0,
        down_own1,
        down_all0,
        down_all1,
        part3a,
        got3a,
        part3b,
        got3b,
        hid0,
        hid1,
        part4,
        got4,
        res_own,
        res_all,
        send_sems,
        recv_sems,
        local_sems,
    ) = refs
    kv = lax.axis_index("kv")
    t = lax.axis_index("tp")
    z, x = lax.div(kv, NX), lax.rem(kv, NX)
    y, core = lax.div(t, 2), lax.rem(t, 2)

    def at_x(d):
        return lax.rem(x + d, NX)

    def at_z(d):
        return lax.rem(z + d, NZ)

    def at_t(d):
        return lax.rem(t + d, NT)

    counter = [0]

    class Exchange:
        def __init__(self, size, group=SMALL):
            self.number, self.group, self.size = counter[0], group, size
            counter[0] += 1

        def send(self, src, dst, peer):
            pltpu.make_async_remote_copy(
                src_ref=src,
                dst_ref=dst,
                send_sem=send_sems.at[self.group],
                recv_sem=recv_sems.at[self.number],
                device_id=peer,
                device_id_type=MESH,
            ).start()

        def arrive(self):
            pltpu.make_async_copy(self.size, self.size, recv_sems.at[self.number]).wait()

    for i, sem in LOADS:
        pltpu.make_async_copy(inputs[i], held[i], local_sems.at[sem]).start()

    barrier = pltpu.get_barrier_semaphore()

    def greet(peer):
        pl.semaphore_signal(barrier, inc=1, device_id=peer, device_id_type=MESH)

    for dz, dx in PLANE:
        greet((at_z(dz) * NX + at_x(dx), t))
    for d in FAR_T:
        greet((kv, at_t(d)))
    def loaded(sem, size):
        pltpu.make_async_copy(size, size, local_sems.at[sem]).wait()

    with jax.named_scope("wait_first"):
        loaded(0, part1.at[0:22])
        loaded(1, norm_gain)
    square = (64, 64)
    row = lax.broadcasted_iota(jnp.int32, square, 0)
    column = lax.broadcasted_iota(jnp.int32, square, 1)
    gain = jnp.sum(
        jnp.where(row == column, jnp.broadcast_to(norm_gain[...].astype(F32), square), 0.0),
        axis=1,
        keepdims=True,
    )

    def gained(weight):
        return (weight[...].astype(F32) * gain).astype(BF16)

    w_own[0, :, 0:128] = gained(w_query)
    w_own[0, :, 128:256] = gained(w_key)
    w_own[1] = gained(w_value)
    w_own[2] = gained(w_gate)
    w_own[3, :, 0:128] = gained(w_decay)
    w_own[3, :, 128:256] = jnp.zeros((64, 128), BF16)
    own = jnp.concatenate([tokens[:, 0:256], tokens[:, 256:512]], axis=0).astype(F32)
    own = jnp.transpose(own, (1, 0))
    x_own[...] = own.reshape(4, 64, 128)
    x_all[x] = own.astype(BF16).reshape(4, 64, 128)
    w_all[x] = w_own[x]

    with jax.named_scope("wait_barrier"):
        pl.semaphore_wait(barrier, len(PLANE) + len(FAR_T))

    tile_z = w_mix.at[:, 0:128]

    def lanes_of(block):
        return pl.ds(pl.multiple_of(block * 128, 128), 128)

    ring_x = [(d, (z * NX + at_x(d), t)) for d in FAR_X]
    ring_z = [(d, (at_z(d) * NX + x, t)) for d in FAR_Z]
    ring_t = [(d, (kv, at_t(d))) for d in FAR_T]
    gather_w = Exchange(w_all.at[0:3], DOWN)
    gather_x = [Exchange(x_all.at[0:3, 0], UP) for _ in X_ORDER]
    x_blocks = [lax.rem(z + steps[0], 4) for steps in X_ORDER]
    for d, peer in ring_x:
        gather_w.send(w_own.at[at_x(d)], w_all.at[x], peer)
    for exchange, r in zip(gather_x, x_blocks):
        for d, peer in ring_x:
            exchange.send(x_all.at[x, r], x_all.at[x, r], peer)

    with jax.named_scope("wait_later"):
        loaded(3, w_out)
    out_rows = jnp.concatenate([w_out[:, 0:128], w_out[:, 128:256]], axis=0).astype(F32)
    w_mix[:, lanes_of(z)] = jnp.transpose(out_rows, (1, 0)).astype(BF16)
    mix_steps = []

    def mix_step(step):
        if step > 1:
            for exchange in mix_steps[-1]:
                exchange.arrive()
        exchanges = []
        for way in (1, -1):
            if step <= (4 if way > 0 else 3):
                lanes = lanes_of(at_z(NZ - way * (step - 1)))
                exchange = Exchange(tile_z)
                exchange.send(
                    w_mix.at[:, lanes], w_mix.at[:, lanes], (at_z(NZ + way) * NX + x, t)
                )
                exchanges.append(exchange)
        mix_steps.append(exchanges)

    mix_step(1)

    with jax.named_scope("wait_later"):
        loaded(2, new_state.at[0:9, 0:32])
        loaded(4, mixer_gain)
        loaded(5, log_decay)
        loaded(6, out_gain)
    gains = mixer_gain[...].astype(F32)
    units = jnp.transpose(
        jnp.concatenate([w_ffgate[...], w_ffup[...]], axis=0).astype(F32), (1, 0)
    )
    units = (units * jnp.concatenate([gains, gains], axis=1)).astype(BF16)
    down = w_down[...].astype(F32)
    down = jnp.concatenate([down, pltpu.roll(down, 768 - 48, 1)], axis=0)
    down = jnp.transpose(down, (1, 0)).astype(BF16)
    up_own, up_all = (up_own0, up_own1), (up_all0, up_all1)
    down_own, down_all = (down_own0, down_own1), (down_all0, down_all1)
    for j in range(NZ):
        for part, skip in ((0, 0), (1, 32)):
            count = PARTS[part]
            low, high = 96 * j + skip, 96 * j + 48 + skip
            up_own[part][j, 0] = units[low : low + count]
            up_own[part][j, 1] = units[high : high + count]
            down_own[part][j] = down[low : low + count]
    lanes_z = lanes_of(z)
    for part in range(2):
        up_all[part][:, t, :, lanes_z] = up_own[part][z]
        down_all[part][t, :, lanes_z] = down_own[part][z]
    up_blocks = [Exchange(up_own[part].at[0:7]) for part in range(2)]
    up_y = [Exchange(up_all[part].at[:, 0:3], UP) for part in range(2)]
    up_core = [Exchange(up_all[part].at[:, 0:4], UP) for part in range(2)]
    partner = (kv, t + 1 - 2 * core)

    def along_y(d):
        return lax.rem(y + d, NY) * 2 + core

    def up_along_z(half):
        for d, peer in ring_z:
            up_blocks[half].send(
                up_own[half].at[at_z(d)], up_all[half].at[:, t, :, lanes_z], peer
            )

    def up_along_y(half):
        with jax.named_scope(f"wait_up_blocks_{half}"):
            up_blocks[half].arrive()
        for d in FAR_Y:
            up_y[half].send(up_all[half].at[:, t], up_all[half].at[:, t], (kv, along_y(d)))
        up_core[half].send(up_all[half].at[:, t], up_all[half].at[:, t], partner)

    up_along_z(0)
    lane32 = lax.broadcasted_iota(jnp.int32, (32, 128), 1)
    ours = x_own[:, pl.ds(pl.multiple_of(8 * t, 8), 8), :]
    tok_own[...] = ours.reshape(32, 128).astype(BF16)
    tok_all[z] = tok_own[...]
    w_diag[...] = jnp.zeros(w_diag.shape, BF16)

    with jax.named_scope("wait_mix_step"):
        mix_step(2)

    with jax.named_scope("wait_gather1_w"):
        gather_w.arrive()
    for j in range(NX):
        w_diag[j, 0:64, 0:256] = w_all[j]
        w_diag[j, 64:128, 256:512] = w_all[j]
    lane64 = lax.broadcasted_iota(jnp.int32, (64, 128), 1)
    has_sums = x == NX - 1
    scatter1 = Exchange(got1.at[0:31])
    for number, (r, steps) in enumerate(zip(x_blocks, X_ORDER)):
        with jax.named_scope(f"wait_gather1_{number}"):
            gather_x[number].arrive()
        total = jnp.zeros((64, 512), F32)
        squares = jnp.zeros((64, 128), F32)
        for j in range(NX):
            block = x_all[j, r]
            total += jnp.dot(block, w_diag[j], preferred_element_type=F32)
            wide = block.astype(F32)
            squares += wide * wide
        for side in range(2):
            ours = (lane64 < 64) if side == 0 else (lane64 >= 64)
            sums = as_pair(jnp.sum(jnp.where(ours, squares, 0.0), axis=1, keepdims=True))
            first = 256 * side
            for k in range(NX):
                rows = slice(16 * k, 16 * k + 16)
                owner = NX * (r + 4 * side) + k
                part1[owner, :, 0:128] = total[rows, first : first + 128].astype(BF16)
                part1[owner, :, 128:256] = jnp.where(
                    has_sums, sums[rows].astype(F32), total[rows, first + 128 : first + 256]
                ).astype(BF16)
        for dz in sorted(steps, key=lambda step: -min(step, NZ - step)):
            for dx in FAR_X + [0]:
                if (dz, dx) != (0, 0):
                    peer = at_z(dz) * NX + at_x(dx)
                    scatter1.send(part1.at[peer], got1.at[x * NZ + z], (peer, t))
    got1[x * NZ + z] = part1[kv]

    with jax.named_scope("wait_mix_step3"):
        mix_step(3)
    up_along_y(0)
    with jax.named_scope("wait_mix_step4"):
        mix_step(4)
    up_along_z(1)

    with jax.named_scope("wait_scatter1"):
        scatter1.arrive()
    proj = []
    for j in range(NX):
        total = got1[NZ * j].astype(F32)
        for k in range(1, NZ):
            total += got1[NZ * j + k].astype(F32)
        proj.append(total)
    loaded(7, state)

    inv = lax.rsqrt(of_pair(proj[3][:, 128:256]) / D + EPS)
    query = proj[0][:, 0:128] * (inv * DK ** (-0.5))
    keys = proj[0][:, 128:256] * inv
    values = proj[1] * inv
    gate = proj[2] * inv
    decay_pre = proj[3][:, 0:128] * inv
    log_sigmoid = jnp.minimum(decay_pre, 0.0) - jnp.log1p(jnp.exp(-jnp.abs(decay_pre)))
    decay = jnp.exp(log_sigmoid / GATE_NORM + log_decay[...])
    columns = jnp.transpose(
        jnp.concatenate([query * decay, keys, decay, jnp.zeros((80, 128), F32)], axis=0), (1, 0)
    )
    for b in range(16):
        att[b : b + 1, :] = jnp.sum(state[b] * columns[:, b : b + 1], axis=0, keepdims=True)
    attended = att[...] + jnp.sum(query * keys, axis=1, keepdims=True) * values
    normed = (
        attended
        * lax.rsqrt(jnp.mean(attended * attended, axis=1, keepdims=True) + EPS)
        * out_gain[...]
    )
    mix[x] = (normed * (gate * sigmoid(gate))).astype(BF16)
    gather2 = Exchange(mix.at[0:3])
    for d, peer in ring_x:
        gather2.send(mix.at[x], mix.at[x], peer)
    down_blocks = [Exchange(down_own[part].at[0:7]) for part in range(2)]
    for part in range(2):
        for d, peer in ring_z:
            down_blocks[part].send(
                down_own[part].at[at_z(d)], down_all[part].at[t, :, lanes_z], peer
            )
    tok_blocks = Exchange(tok_all.at[0:7])
    for d, peer in ring_z:
        tok_blocks.send(tok_own, tok_all.at[z], peer)
    for b in range(16):
        k_col = columns[:, 16 + b : 17 + b]
        a_col = columns[:, 32 + b : 33 + b]
        new_state[b] = state[b] * a_col + k_col * values[b : b + 1, :]

    with jax.named_scope("wait_mix_blocks"):
        for exchange in mix_steps[-1]:
            exchange.arrive()
    with jax.named_scope("wait_gather2"):
        gather2.arrive()
    mixed = mix[...].reshape(64, DV)
    stacked = jnp.concatenate([mixed[:, 0:128], mixed[:, 128:256]], axis=0)
    total = jnp.dot(stacked, w_mix[...], preferred_element_type=F32)
    lane64 = lax.broadcasted_iota(jnp.int32, (64, 128), 1)
    pairs = []
    for p in range(4):
        low, high = [
            (total[0:64, first : first + 128], total[64:128, first : first + 128])
            for first in (256 * p, 256 * p + 128)
        ]
        pairs.append(
            jnp.where(
                lane64 < 64,
                low[0] + pltpu.roll(low[1], 64, 1),
                pltpu.roll(high[0], 64, 1) + high[1],
            )
        )
    for j in range(NT):
        rows = slice(8 * j, 8 * j + 8)
        part2[j] = jnp.concatenate([pair[rows] for pair in pairs], axis=0).astype(BF16)
    got2[t] = part2[t]
    scatter2 = Exchange(got2.at[0:7])
    for d, peer in ring_t:
        scatter2.send(part2.at[at_t(d)], got2.at[t], peer)
    up_along_y(1)
    with jax.named_scope("wait_scatter2"):
        scatter2.arrive()
    total = got2[0].astype(F32)
    for j in range(1, NT):
        total += got2[j].astype(F32)
    attn_own[...] = total.astype(BF16)

    attn_all[z] = attn_own[...]
    spread = Exchange(attn_all.at[0:7])
    for d, peer in ring_z:
        spread.send(attn_own, attn_all.at[z], peer)

    with jax.named_scope("wait_down_blocks"):
        for exchange in down_blocks:
            exchange.arrive()
    down_y = [Exchange(down_all[part].at[0:3], DOWN) for part in range(2)]
    down_core = [Exchange(down_all[part].at[0:4], DOWN) for part in range(2)]

    def down_send(exchanges, block, peer):
        for exchange, ref in zip(exchanges, down_all):
            exchange.send(ref.at[block], ref.at[block], peer)

    for d in FAR_Y:
        down_send(down_y, t, (kv, along_y(d)))
    for half in range(2):
        with jax.named_scope(f"wait_up_y_{half}"):
            up_y[half].arrive()
        for d in range(1, NY):
            other = along_y(d)
            up_core[half].send(up_all[half].at[:, other], up_all[half].at[:, other], partner)
    down_send(down_core, t, partner)

    with jax.named_scope("wait_tok_blocks"):
        tok_blocks.arrive()
    with jax.named_scope("wait_spread"):
        spread.arrive()

    squares = jnp.zeros((64, 128), F32)
    pieces = []
    sums = [attn_all[j].astype(F32) for j in range(NZ)]
    middles = []
    for p in range(4):
        low, high = tok_all[2 * p].astype(F32), tok_all[2 * p + 1].astype(F32)
        residual = jnp.concatenate(
            [
                jnp.where(lane32 < 64, low, pltpu.roll(high, 64, 1)),
                jnp.where(lane32 < 64, pltpu.roll(low, 64, 1), high),
            ],
            axis=0,
        )
        added = jnp.concatenate([total[8 * p : 8 * p + 8] for total in sums], axis=0)
        wide = (residual + added).astype(BF16).astype(F32)
        middles.append(wide)
        squares += wide * wide
        turned = pltpu.roll(wide, 64, 1)
        for here, there in ((wide, turned), (turned, wide)):
            pieces.append(
                jnp.concatenate(
                    [jnp.where(lane64 < 64, here, 0.0), jnp.where(lane64 < 64, 0.0, there)], axis=0
                ).astype(BF16)
            )
    left = jnp.concatenate(pieces, axis=1)
    squares = as_pair(jnp.sum(squares, axis=1, keepdims=True))
    parts3, gots3 = (part3a, part3b), (got3a, got3b)
    scatter3 = [Exchange(got3.at[0:3]) for got3 in gots3]
    for half, (part3, got3) in enumerate(zip(parts3, gots3)):
        with jax.named_scope(f"wait_up_core_{half}"):
            up_core[half].arrive()
        terms = lax.dot_general(
            left,
            up_all[half][...].reshape(16 * PARTS[half], 1024),
            (((1,), (1,)), ((), ())),
            preferred_element_type=F32,
        )
        for j in range(NX):
            rows = slice(16 * j, 16 * j + 16)
            width = 16 * PARTS[half]
            part3[j, :, 0:width] = terms[rows].astype(BF16)
            part3[j, :, width : 2 * width] = terms[64 + 16 * j : 80 + 16 * j].astype(BF16)
            if half == 0:
                part3[j, :, 2 * width : 2 * width + 128] = squares[rows]
        got3[x] = part3[x]
        for d, peer in ring_x:
            scatter3[half].send(part3.at[at_x(d)], got3.at[x], peer)
    for p, wide in enumerate(middles):
        turned = pltpu.roll(wide, 64, 1)
        middle[2 * p] = jnp.where(lane32 < 64, wide[0:32], turned[32:64]).astype(BF16)
        middle[2 * p + 1] = jnp.where(lane32 < 64, turned[0:32], wide[32:64]).astype(BF16)
    with jax.named_scope("wait_down_y"):
        for exchange in down_y:
            exchange.arrive()
    for d in range(1, NY):
        down_send(down_core, along_y(d), partner)
    hid = (hid0, hid1)
    gather3 = [Exchange(ref.at[0:3]) for ref in hid]
    inv = None
    for half, got3 in enumerate(gots3):
        with jax.named_scope(f"wait_scatter3_{half}"):
            scatter3[half].arrive()
        total = got3[0].astype(F32)
        for j in range(1, NX):
            total += got3[j].astype(F32)
        width = 16 * PARTS[half]
        if half == 0:
            inv = lax.rsqrt(of_pair(total[:, 2 * width : 2 * width + 128]) / D + EPS)
        gate = total[:, 0:width] * inv
        hid[half][x] = (gate * sigmoid(gate) * (total[:, width : 2 * width] * inv)).astype(BF16)
        for d, peer in ring_x:
            gather3[half].send(hid[half].at[x], hid[half].at[x], peer)
    with jax.named_scope("wait_down_core"):
        for exchange in down_core:
            exchange.arrive()

    total = jnp.zeros((128, 1024), F32)
    for half in range(2):
        with jax.named_scope(f"wait_gather3_{half}"):
            gather3[half].arrive()
        width = 8 * PARTS[half]
        hidden = hid[half][...].reshape(64, 2 * width)
        stacked = jnp.concatenate([hidden[:, 0:width], hidden[:, width:]], axis=0)
        weights = down_all[half][...].reshape(width, 1024)
        total += jnp.dot(stacked, weights, preferred_element_type=F32)
    products = (total[0:64], total[64:128])
    for j, block in enumerate(packed_products(*products, lane32)):
        part4[j] = block.astype(BF16)
    got4[z] = part4[z]
    scatter4 = Exchange(got4.at[0:7])
    for d, peer in ring_z:
        scatter4.send(part4.at[at_z(d)], got4.at[z], peer)
    with jax.named_scope("wait_scatter4"):
        scatter4.arrive()
    total = got4[0].astype(F32)
    for j in range(1, NZ):
        total += got4[j].astype(F32)
    res_own[...] = (middle[z].astype(F32) + total).astype(BF16)
    res_all[t] = res_own[...]
    gather4 = Exchange(res_all.at[0:7], LAST)
    for d, peer in ring_t:
        gather4.send(res_own, res_all.at[t], peer)
    with jax.named_scope("wait_gather4"):
        gather4.arrive()
    blocks = [res_all[j].astype(F32) for j in range(NT)]
    blocks = [blocks, [pltpu.roll(block, 64, 1) for block in blocks]]
    rows = jnp.concatenate(
        [
            blocks[j // 4][k][8 * (j % 4) : 8 * (j % 4) + 8]
            for j in range(NZ)
            for k in range(NT)
        ],
        axis=0,
    )
    result[...] = jnp.transpose(rows, (1, 0))[0:64].astype(BF16)
    with jax.named_scope("wait_sends"):
        everything = (state.at[0:15, 0:80], state.at[0:12], state.at[0:6], res_all.at[0:7])
        for group, size in enumerate(everything):
            pltpu.make_async_copy(size, size, send_sems.at[group]).wait()


def finish(result_in, state_in, result_out, state_out, sems):
    result = pltpu.make_async_copy(result_in, result_out, sems.at[0])
    states = pltpu.make_async_copy(state_in, state_out, sems.at[1])
    parts = [pl.ds(2 * i, 2) for i in range(8)]
    result.start()
    for part in parts:
        pltpu.make_async_copy(state_in.at[part], state_out.at[part], sems.at[1]).start()
    result.wait()
    states.wait()


def body(
    tokens,
    norm_gain,
    w_query,
    w_key,
    w_value,
    w_gate,
    w_decay,
    log_decay,
    state,
    out_gain,
    w_out,
    mixer_gain,
    w_ffgate,
    w_ffup,
    w_down,
):
    vmem = pl.BlockSpec(memory_space=pltpu.VMEM)
    hbm = pl.BlockSpec(memory_space=pltpu.HBM)
    shape = state.shape
    arguments = (
        tokens.T,
        norm_gain.reshape(1, 64),
        w_query,
        w_key,
        w_value,
        w_gate,
        w_decay,
        log_decay,
        state.reshape(shape[0], DK, DV),
        out_gain.reshape(1, DV),
        w_out.T,
        mixer_gain.reshape(1, 64),
        w_ffgate,
        w_ffup,
        w_down.T,
    )
    arguments = [pltpu.with_memory_space_constraint(value, pltpu.HBM) for value in arguments]
    result, new_state = pl.pallas_call(
        kernel,
        out_shape=(
            pltpu.VMEM((64, 512), BF16),
            pltpu.VMEM((shape[0], DK, DV), F32),
        ),
        in_specs=[hbm] * 15,
        out_specs=(vmem, vmem),
        scratch_shapes=[pltpu.VMEM(value.shape, value.dtype) for value in arguments]
        + [
            pltpu.VMEM((16, DV), F32),
            pltpu.VMEM((NX, 64, 256), BF16),
            pltpu.VMEM((4, 64, 128), F32),
            pltpu.VMEM((NX, 4, 64, 128), BF16),
            pltpu.VMEM((NX, 64, 256), BF16),
            pltpu.VMEM((NX, 128, 512), BF16),
            pltpu.VMEM((NZ * NX, 16, 256), BF16),
            pltpu.VMEM((NX * NZ, 16, 256), BF16),
            pltpu.VMEM((NX, 16, 256), BF16),
            pltpu.VMEM((128, 1024), BF16),
            pltpu.VMEM((NT, 32, 128), BF16),
            pltpu.VMEM((NT, 32, 128), BF16),
            pltpu.VMEM((32, 128), BF16),
            pltpu.VMEM((NT, 32, 128), BF16),
            pltpu.VMEM((32, 128), BF16),
            pltpu.VMEM((NZ, 32, 128), BF16),
            pltpu.VMEM((NZ, 32, 128), BF16),
            *(pltpu.VMEM((NZ, 2, units, 128), BF16) for units in PARTS),
            *(pltpu.VMEM((2, NT, units, 1024), BF16) for units in PARTS),
            *(pltpu.VMEM((NZ, units, 128), BF16) for units in PARTS),
            *(pltpu.VMEM((NT, units, 1024), BF16) for units in PARTS),
            pltpu.VMEM((NX, 16, 1152), BF16),
            pltpu.VMEM((NX, 16, 1152), BF16),
            pltpu.VMEM((NX, 16, 512), BF16),
            pltpu.VMEM((NX, 16, 512), BF16),
            pltpu.VMEM((NX, 16, 512), BF16),
            pltpu.VMEM((NX, 16, 256), BF16),
            pltpu.VMEM((NZ, 32, 128), BF16),
            pltpu.VMEM((NZ, 32, 128), BF16),
            pltpu.VMEM((32, 128), BF16),
            pltpu.VMEM((NT, 32, 128), BF16),
            pltpu.SemaphoreType.DMA((4,)),
            pltpu.SemaphoreType.DMA((COPIES,)),
            pltpu.SemaphoreType.DMA((8,)),
        ],
        compiler_params=pltpu.CompilerParams(
            collective_id=0, has_side_effects=True, vmem_limit_bytes=40 * 1024 * 1024
        ),
    )(*arguments)
    result, new_state = pl.pallas_call(
        finish,
        out_shape=(
            jax.ShapeDtypeStruct((64, 512), BF16),
            jax.ShapeDtypeStruct((shape[0], DK, DV), F32),
        ),
        in_specs=[vmem, vmem],
        out_specs=(hbm, hbm),
        scratch_shapes=[pltpu.SemaphoreType.DMA((2,))],
        compiler_params=pltpu.CompilerParams(vmem_limit_bytes=8 * 1024 * 1024),
    )(result, new_state)
    return (result.T, new_state.reshape(shape))


def solution(mesh):
    return jax.shard_map(
        body,
        mesh=mesh,
        in_specs=(
            P(None, "kv"),
            P("kv"),
            P("kv", "tp"),
            P("kv", "tp"),
            P("kv", "tp"),
            P("kv", "tp"),
            P("kv", "tp"),
            P("kv", "tp"),
            P("kv", "tp", None, None),
            P(),
            P("tp", "kv"),
            P("kv"),
            P("kv", "tp"),
            P("kv", "tp"),
            P("tp", "kv"),
        ),
        out_specs=(P(None, "kv"), P("kv", "tp", None, None)),
        check_vma=False,
    )
```

```python
import functools

import jax
import jax.numpy as jnp
from jax import lax
from jax.experimental import pallas as pl
from jax.experimental.pallas import tpu as pltpu
from jax.sharding import PartitionSpec as P

MESH = pl.DeviceIdType.MESH
F32 = jnp.float32
BF16 = jnp.bfloat16

D = 2048
DK = 128
DV = 256
EPS = 1e-06
GATE_NORM = 16.0

NX, NY, NZ = 4, 4, 8
NT = 2 * NY
COPIES = 32
SMALL, UP, DOWN, LAST = range(4)
FAR_X = [2, 1, 3]
FAR_Y = [2, 1, 3]
FAR_Z = [4, 3, 5, 2, 6, 1, 7]
FAR_T = [(dy, dc) for dy in FAR_Y + [0] for dc in range(2) if (dy, dc) != (0, 0)]
X_ORDER = [(0, 4), (2, 6), (3, 7), (1, 5)]
PLANE = [(dz, dx) for dz in FAR_Z + [0] for dx in FAR_X + [0] if (dz, dx) != (0, 0)]
LOADS = [(0, 0), (1, 1), (2, 0), (3, 0), (4, 0), (5, 0), (6, 0)]
LOADS += [(10, 3), (12, 2), (13, 2), (14, 2), (11, 4), (7, 5), (9, 6), (8, 7)]


def sigmoid(value):
    return 1.0 / (1.0 + jnp.exp(-value))


def as_pair(total):
    high = jnp.broadcast_to(total, (total.shape[0], 128)).astype(BF16).astype(F32)
    low = jnp.broadcast_to(total, (total.shape[0], 128)) - high
    lane = lax.broadcasted_iota(jnp.int32, high.shape, 1)
    return jnp.where(lane < 64, high, low).astype(BF16)


def of_pair(pair):
    return pair[:, 0:1] + pair[:, 64:65]


def packed_products(first, second, lane):
    blocks = []
    for j in range(8):
        low = first[:, 128 * j : 128 * j + 128]
        high = second[:, 128 * j : 128 * j + 128]
        top = low[0:32] + pltpu.roll(high[0:32], 64, 1)
        bottom = pltpu.roll(low[32:64], 64, 1) + high[32:64]
        blocks.append(jnp.where(lane < 64, top, bottom))
    return blocks


def kernel(*refs):
    inputs, (result, new_state), refs = refs[:15], refs[15:17], refs[17:]
    held, refs = refs[:15], refs[15:]
    (
        tokens,
        norm_gain,
        w_query,
        w_key,
        w_value,
        w_gate,
        w_decay,
        log_decay,
        state,
        out_gain,
        w_out,
        mixer_gain,
        w_ffgate,
        w_ffup,
        w_down,
    ) = held
    (
        att,
        w_own,
        x_own,
        x_all,
        w_all,
        w_diag,
        part1,
        got1,
        mix,
        w_mix,
        part2,
        got2,
        attn_own,
        attn_all,
        tok_own,
        tok_all,
        middle,
        up_own,
        up_all,
        down_own,
        down_all,
        part3a,
        got3a,
        part3b,
        got3b,
        hid,
        part4,
        got4,
        res_own,
        res_all,
        send_sems,
        recv_sems,
        local_sems,
    ) = refs
    kv = lax.axis_index("kv")
    t = lax.axis_index("tp")
    z, x = lax.div(kv, NX), lax.rem(kv, NX)
    y, core = lax.div(t, 2), lax.rem(t, 2)

    def at_x(d):
        return lax.rem(x + d, NX)

    def at_z(d):
        return lax.rem(z + d, NZ)

    counter = [0]

    class Exchange:
        def __init__(self, size, group=SMALL):
            self.number, self.group, self.size = counter[0], group, size
            counter[0] += 1

        def send(self, src, dst, peer):
            pltpu.make_async_remote_copy(
                src_ref=src,
                dst_ref=dst,
                send_sem=send_sems.at[self.group],
                recv_sem=recv_sems.at[self.number],
                device_id=peer,
                device_id_type=MESH,
            ).start()

        def arrive(self):
            pltpu.make_async_copy(self.size, self.size, recv_sems.at[self.number]).wait()

    for i, sem in LOADS:
        pltpu.make_async_copy(inputs[i], held[i], local_sems.at[sem]).start()

    barrier = pltpu.get_barrier_semaphore()

    def greet(peer):
        pl.semaphore_signal(barrier, inc=1, device_id=peer, device_id_type=MESH)

    for dz, dx in PLANE:
        greet((at_z(dz) * NX + at_x(dx), t))
    for dy, dc in FAR_T:
        greet((kv, lax.rem(y + dy, NY) * 2 + (core if dc == 0 else 1 - core)))
    def loaded(sem, size):
        pltpu.make_async_copy(size, size, local_sems.at[sem]).wait()

    with jax.named_scope("wait_first"):
        loaded(0, part1.at[0:22])
        loaded(1, norm_gain)
    square = (64, 64)
    row = lax.broadcasted_iota(jnp.int32, square, 0)
    column = lax.broadcasted_iota(jnp.int32, square, 1)
    gain = jnp.sum(
        jnp.where(row == column, jnp.broadcast_to(norm_gain[...].astype(F32), square), 0.0),
        axis=1,
        keepdims=True,
    )

    def gained(weight):
        return (weight[...].astype(F32) * gain).astype(BF16)

    w_own[0, :, 0:128] = gained(w_query)
    w_own[0, :, 128:256] = gained(w_key)
    w_own[1] = gained(w_value)
    w_own[2] = gained(w_gate)
    w_own[3, :, 0:128] = gained(w_decay)
    w_own[3, :, 128:256] = jnp.zeros((64, 128), BF16)
    own = jnp.concatenate([tokens[:, 0:256], tokens[:, 256:512]], axis=0).astype(F32)
    own = jnp.transpose(own, (1, 0))
    x_own[...] = own.reshape(4, 64, 128)
    x_all[x] = own.astype(BF16).reshape(4, 64, 128)
    w_all[x] = w_own[x]

    with jax.named_scope("wait_barrier"):
        pl.semaphore_wait(barrier, len(PLANE) + len(FAR_T))

    tile_z = w_mix.at[:, 0:128]

    def lanes_of(block):
        return pl.ds(pl.multiple_of(block * 128, 128), 128)

    ring_x = [(d, (z * NX + at_x(d), t)) for d in FAR_X]
    ring_z = [(d, (at_z(d) * NX + x, t)) for d in FAR_Z]
    ring_t = [
        lax.rem(y + dy, NY) * 2 + (core if dc == 0 else 1 - core) for dy, dc in FAR_T
    ]
    gather_w = Exchange(w_all.at[0:3], DOWN)
    gather_x = [Exchange(x_all.at[0:3, 0], UP) for _ in X_ORDER]
    x_blocks = [lax.rem(z + steps[0], 4) for steps in X_ORDER]
    for d, peer in ring_x:
        gather_w.send(w_own.at[at_x(d)], w_all.at[x], peer)
    for exchange, r in zip(gather_x, x_blocks):
        for d, peer in ring_x:
            exchange.send(x_all.at[x, r], x_all.at[x, r], peer)

    with jax.named_scope("wait_later"):
        loaded(3, w_out)
    out_rows = jnp.concatenate([w_out[:, 0:128], w_out[:, 128:256]], axis=0).astype(F32)
    w_mix[:, lanes_of(z)] = jnp.transpose(out_rows, (1, 0)).astype(BF16)
    mix_steps = []

    def mix_step(step):
        if step > 1:
            for exchange in mix_steps[-1]:
                exchange.arrive()
        exchanges = []
        for way in (1, -1):
            if step <= (4 if way > 0 else 3):
                lanes = lanes_of(at_z(NZ - way * (step - 1)))
                exchange = Exchange(tile_z)
                exchange.send(
                    w_mix.at[:, lanes], w_mix.at[:, lanes], (at_z(NZ + way) * NX + x, t)
                )
                exchanges.append(exchange)
        mix_steps.append(exchanges)

    mix_step(1)

    with jax.named_scope("wait_later"):
        loaded(2, up_all.at[0, 0:3])
        loaded(4, mixer_gain)
        loaded(5, log_decay)
        loaded(6, out_gain)
    gains = mixer_gain[...].astype(F32)
    units = jnp.transpose(
        jnp.concatenate([w_ffgate[...], w_ffup[...]], axis=0).astype(F32), (1, 0)
    )
    units = (units * jnp.concatenate([gains, gains], axis=1)).astype(BF16)
    down = w_down[...].astype(F32)
    down = jnp.concatenate([down, pltpu.roll(down, 768 - 48, 1)], axis=0)
    down = jnp.transpose(down, (1, 0)).astype(BF16)
    for j in range(NZ):
        up_own[0, j] = units[96 * j : 96 * j + 48]
        up_own[1, j] = units[96 * j + 48 : 96 * j + 96]
        down_own[j] = down[96 * j : 96 * j + 48]
    lanes_z = lanes_of(z)
    for half in range(2):
        up_all[half, t, :, lanes_z] = up_own[half, z]
    down_all[t, :, lanes_z] = down_own[z]
    up_blocks = [Exchange(up_own.at[half, 0:7]) for half in range(2)]
    up_y = [Exchange(up_all.at[half, 0:3], UP) for half in range(2)]
    up_core = [Exchange(up_all.at[half, 0:4], UP) for half in range(2)]
    partner = (kv, t + 1 - 2 * core)

    def along_y(d):
        return lax.rem(y + d, NY) * 2 + core

    def up_along_z(half):
        for d, peer in ring_z:
            up_blocks[half].send(
                up_own.at[half, at_z(d)], up_all.at[half, t, :, lanes_z], peer
            )

    def up_along_y(half):
        with jax.named_scope(f"wait_up_blocks_{half}"):
            up_blocks[half].arrive()
        for d in FAR_Y:
            up_y[half].send(up_all.at[half, t], up_all.at[half, t], (kv, along_y(d)))
        up_core[half].send(up_all.at[half, t], up_all.at[half, t], partner)

    up_along_z(0)
    lane32 = lax.broadcasted_iota(jnp.int32, (32, 128), 1)
    ours = x_own[:, pl.ds(pl.multiple_of(8 * t, 8), 8), :]
    tok_own[...] = ours.reshape(32, 128).astype(BF16)
    tok_all[z] = tok_own[...]
    w_diag[...] = jnp.zeros(w_diag.shape, BF16)

    with jax.named_scope("wait_mix_step"):
        mix_step(2)

    with jax.named_scope("wait_gather1_w"):
        gather_w.arrive()
    for j in range(NX):
        w_diag[j, 0:64, 0:256] = w_all[j]
        w_diag[j, 64:128, 256:512] = w_all[j]
    lane64 = lax.broadcasted_iota(jnp.int32, (64, 128), 1)
    has_sums = x == NX - 1
    scatter1 = Exchange(got1.at[0:31])
    for number, (r, steps) in enumerate(zip(x_blocks, X_ORDER)):
        with jax.named_scope(f"wait_gather1_{number}"):
            gather_x[number].arrive()
        total = jnp.zeros((64, 512), F32)
        squares = jnp.zeros((64, 128), F32)
        for j in range(NX):
            block = x_all[j, r]
            total += jnp.dot(block, w_diag[j], preferred_element_type=F32)
            wide = block.astype(F32)
            squares += wide * wide
        for side in range(2):
            ours = (lane64 < 64) if side == 0 else (lane64 >= 64)
            sums = as_pair(jnp.sum(jnp.where(ours, squares, 0.0), axis=1, keepdims=True))
            first = 256 * side
            for k in range(NX):
                rows = slice(16 * k, 16 * k + 16)
                owner = NX * (r + 4 * side) + k
                part1[owner, :, 0:128] = total[rows, first : first + 128].astype(BF16)
                part1[owner, :, 128:256] = jnp.where(
                    has_sums, sums[rows].astype(F32), total[rows, first + 128 : first + 256]
                ).astype(BF16)
        for dz in sorted(steps, key=lambda step: -min(step, NZ - step)):
            for dx in FAR_X + [0]:
                if (dz, dx) != (0, 0):
                    peer = at_z(dz) * NX + at_x(dx)
                    scatter1.send(part1.at[peer], got1.at[x * NZ + z], (peer, t))
    got1[x * NZ + z] = part1[kv]

    with jax.named_scope("wait_mix_step3"):
        mix_step(3)
    up_along_y(0)
    with jax.named_scope("wait_mix_step4"):
        mix_step(4)
    up_along_z(1)

    with jax.named_scope("wait_scatter1"):
        scatter1.arrive()
    proj = []
    for j in range(NX):
        total = got1[NZ * j].astype(F32)
        for k in range(1, NZ):
            total += got1[NZ * j + k].astype(F32)
        proj.append(total)
    loaded(7, state)

    inv = lax.rsqrt(of_pair(proj[3][:, 128:256]) / D + EPS)
    query = proj[0][:, 0:128] * (inv * DK ** (-0.5))
    keys = proj[0][:, 128:256] * inv
    values = proj[1] * inv
    gate = proj[2] * inv
    decay_pre = proj[3][:, 0:128] * inv
    log_sigmoid = jnp.minimum(decay_pre, 0.0) - jnp.log1p(jnp.exp(-jnp.abs(decay_pre)))
    decay = jnp.exp(log_sigmoid / GATE_NORM + log_decay[...])
    columns = jnp.transpose(
        jnp.concatenate([query * decay, keys, decay, jnp.zeros((80, 128), F32)], axis=0), (1, 0)
    )
    for b in range(16):
        att[b : b + 1, :] = jnp.sum(state[b] * columns[:, b : b + 1], axis=0, keepdims=True)
    attended = att[...] + jnp.sum(query * keys, axis=1, keepdims=True) * values
    normed = (
        attended
        * lax.rsqrt(jnp.mean(attended * attended, axis=1, keepdims=True) + EPS)
        * out_gain[...]
    )
    mix[x] = (normed * (gate * sigmoid(gate))).astype(BF16)
    gather2 = Exchange(mix.at[0:3])
    for d, peer in ring_x:
        gather2.send(mix.at[x], mix.at[x], peer)
    down_blocks = Exchange(down_own.at[0:7])
    for d, peer in ring_z:
        down_blocks.send(down_own.at[at_z(d)], down_all.at[t, :, lanes_z], peer)
    tok_blocks = Exchange(tok_all.at[0:7])
    for d, peer in ring_z:
        tok_blocks.send(tok_own, tok_all.at[z], peer)
    for b in range(16):
        k_col = columns[:, 16 + b : 17 + b]
        a_col = columns[:, 32 + b : 33 + b]
        new_state[b] = state[b] * a_col + k_col * values[b : b + 1, :]

    with jax.named_scope("wait_mix_blocks"):
        for exchange in mix_steps[-1]:
            exchange.arrive()
    with jax.named_scope("wait_gather2"):
        gather2.arrive()
    mixed = mix[...].reshape(64, DV)
    stacked = jnp.concatenate([mixed[:, 0:128], mixed[:, 128:256]], axis=0)
    total = jnp.dot(stacked, w_mix[...], preferred_element_type=F32)
    lane64 = lax.broadcasted_iota(jnp.int32, (64, 128), 1)
    pairs = []
    for p in range(4):
        low, high = [
            (total[0:64, first : first + 128], total[64:128, first : first + 128])
            for first in (256 * p, 256 * p + 128)
        ]
        pairs.append(
            jnp.where(
                lane64 < 64,
                low[0] + pltpu.roll(low[1], 64, 1),
                pltpu.roll(high[0], 64, 1) + high[1],
            )
        )
    for j in range(NT):
        rows = slice(8 * j, 8 * j + 8)
        part2[j] = jnp.concatenate([pair[rows] for pair in pairs], axis=0).astype(BF16)
    got2[t] = part2[t]
    scatter2 = Exchange(got2.at[0:7])
    for other in ring_t:
        scatter2.send(part2.at[other], got2.at[t], (kv, other))
    up_along_y(1)
    with jax.named_scope("wait_scatter2"):
        scatter2.arrive()
    total = got2[0].astype(F32)
    for j in range(1, NT):
        total += got2[j].astype(F32)
    attn_own[...] = total.astype(BF16)

    attn_all[z] = attn_own[...]
    spread = Exchange(attn_all.at[0:7])
    for d, peer in ring_z:
        spread.send(attn_own, attn_all.at[z], peer)

    with jax.named_scope("wait_down_blocks"):
        down_blocks.arrive()
    down_y, down_core = Exchange(down_all.at[0:3], DOWN), Exchange(down_all.at[0:4], DOWN)
    for d in FAR_Y:
        down_y.send(down_all.at[t], down_all.at[t], (kv, along_y(d)))
    for half in range(2):
        with jax.named_scope(f"wait_up_y_{half}"):
            up_y[half].arrive()
        for d in range(1, NY):
            other = along_y(d)
            up_core[half].send(up_all.at[half, other], up_all.at[half, other], partner)
    down_core.send(down_all.at[t], down_all.at[t], partner)

    with jax.named_scope("wait_tok_blocks"):
        tok_blocks.arrive()
    with jax.named_scope("wait_spread"):
        spread.arrive()

    squares = jnp.zeros((64, 128), F32)
    pieces = []
    sums = [attn_all[j].astype(F32) for j in range(NZ)]
    middles = []
    for p in range(4):
        low, high = tok_all[2 * p].astype(F32), tok_all[2 * p + 1].astype(F32)
        residual = jnp.concatenate(
            [
                jnp.where(lane32 < 64, low, pltpu.roll(high, 64, 1)),
                jnp.where(lane32 < 64, pltpu.roll(low, 64, 1), high),
            ],
            axis=0,
        )
        added = jnp.concatenate([total[8 * p : 8 * p + 8] for total in sums], axis=0)
        wide = (residual + added).astype(BF16).astype(F32)
        middles.append(wide)
        squares += wide * wide
        turned = pltpu.roll(wide, 64, 1)
        for here, there in ((wide, turned), (turned, wide)):
            pieces.append(
                jnp.concatenate(
                    [jnp.where(lane64 < 64, here, 0.0), jnp.where(lane64 < 64, 0.0, there)], axis=0
                ).astype(BF16)
            )
    left = jnp.concatenate(pieces, axis=1)
    squares = as_pair(jnp.sum(squares, axis=1, keepdims=True))
    parts3, gots3 = (part3a, part3b), (got3a, got3b)
    scatter3 = [Exchange(got3.at[0:3]) for got3 in gots3]
    for half, (part3, got3) in enumerate(zip(parts3, gots3)):
        with jax.named_scope(f"wait_up_core_{half}"):
            up_core[half].arrive()
        terms = lax.dot_general(
            left,
            up_all[half].reshape(384, 1024),
            (((1,), (1,)), ((), ())),
            preferred_element_type=F32,
        )
        for j in range(NX):
            rows = slice(16 * j, 16 * j + 16)
            part3[j, :, 0:384] = terms[rows].astype(BF16)
            part3[j, :, 384:768] = terms[64 + 16 * j : 80 + 16 * j].astype(BF16)
            if half == 0:
                part3[j, :, 768:896] = squares[rows]
        got3[x] = part3[x]
        for d, peer in ring_x:
            scatter3[half].send(part3.at[at_x(d)], got3.at[x], peer)
    for p, wide in enumerate(middles):
        turned = pltpu.roll(wide, 64, 1)
        middle[2 * p] = jnp.where(lane32 < 64, wide[0:32], turned[32:64]).astype(BF16)
        middle[2 * p + 1] = jnp.where(lane32 < 64, turned[0:32], wide[32:64]).astype(BF16)
    with jax.named_scope("wait_down_y"):
        down_y.arrive()
    for d in range(1, NY):
        other = along_y(d)
        down_core.send(down_all.at[other], down_all.at[other], partner)
    gather3 = [Exchange(hid.at[half, 0:3]) for half in range(2)]
    inv = None
    for half, got3 in enumerate(gots3):
        with jax.named_scope(f"wait_scatter3_{half}"):
            scatter3[half].arrive()
        total = got3[0].astype(F32)
        for j in range(1, NX):
            total += got3[j].astype(F32)
        if half == 0:
            inv = lax.rsqrt(of_pair(total[:, 768:896]) / D + EPS)
        gate = total[:, 0:384] * inv
        hid[half, x] = (gate * sigmoid(gate) * (total[:, 384:768] * inv)).astype(BF16)
        for d, peer in ring_x:
            gather3[half].send(hid.at[half, x], hid.at[half, x], peer)
    with jax.named_scope("wait_down_core"):
        down_core.arrive()

    weights = down_all[...].reshape(NT * 48, 1024)
    products = []
    for half in range(2):
        with jax.named_scope(f"wait_gather3_{half}"):
            gather3[half].arrive()
        products.append(
            jnp.dot(hid[half].reshape(64, 384), weights, preferred_element_type=F32)
        )
    for j, block in enumerate(packed_products(*products, lane32)):
        part4[j] = block.astype(BF16)
    got4[z] = part4[z]
    scatter4 = Exchange(got4.at[0:7])
    for d, peer in ring_z:
        scatter4.send(part4.at[at_z(d)], got4.at[z], peer)
    with jax.named_scope("wait_scatter4"):
        scatter4.arrive()
    total = got4[0].astype(F32)
    for j in range(1, NZ):
        total += got4[j].astype(F32)
    res_own[...] = (middle[z].astype(F32) + total).astype(BF16)
    res_all[t] = res_own[...]
    gather4 = Exchange(res_all.at[0:7], LAST)
    for other in ring_t:
        gather4.send(res_own, res_all.at[t], (kv, other))
    with jax.named_scope("wait_gather4"):
        gather4.arrive()
    blocks = [res_all[j].astype(F32) for j in range(NT)]
    blocks = [blocks, [pltpu.roll(block, 64, 1) for block in blocks]]
    rows = jnp.concatenate(
        [
            blocks[j // 4][k][8 * (j % 4) : 8 * (j % 4) + 8]
            for j in range(NZ)
            for k in range(NT)
        ],
        axis=0,
    )
    result[...] = jnp.transpose(rows, (1, 0))[0:64].astype(BF16)
    with jax.named_scope("wait_sends"):
        everything = (state.at[0:15, 0:80], up_all, up_all.at[0], res_all.at[0:7])
        for group, size in enumerate(everything):
            pltpu.make_async_copy(size, size, send_sems.at[group]).wait()


def finish(result_in, state_in, result_out, state_out, sems):
    result = pltpu.make_async_copy(result_in, result_out, sems.at[0])
    states = pltpu.make_async_copy(state_in, state_out, sems.at[1])
    parts = [pl.ds(2 * i, 2) for i in range(8)]
    result.start()
    for part in parts:
        pltpu.make_async_copy(state_in.at[part], state_out.at[part], sems.at[1]).start()
    result.wait()
    states.wait()


def body(
    tokens,
    norm_gain,
    w_query,
    w_key,
    w_value,
    w_gate,
    w_decay,
    log_decay,
    state,
    out_gain,
    w_out,
    mixer_gain,
    w_ffgate,
    w_ffup,
    w_down,
):
    vmem = pl.BlockSpec(memory_space=pltpu.VMEM)
    hbm = pl.BlockSpec(memory_space=pltpu.HBM)
    shape = state.shape
    arguments = (
        tokens.T,
        norm_gain.reshape(1, 64),
        w_query,
        w_key,
        w_value,
        w_gate,
        w_decay,
        log_decay,
        state.reshape(shape[0], DK, DV),
        out_gain.reshape(1, DV),
        w_out.T,
        mixer_gain.reshape(1, 64),
        w_ffgate,
        w_ffup,
        w_down.T,
    )
    arguments = [pltpu.with_memory_space_constraint(value, pltpu.HBM) for value in arguments]
    result, new_state = pl.pallas_call(
        kernel,
        out_shape=(
            pltpu.VMEM((64, 512), BF16),
            pltpu.VMEM((shape[0], DK, DV), F32),
        ),
        in_specs=[hbm] * 15,
        out_specs=(vmem, vmem),
        scratch_shapes=[pltpu.VMEM(value.shape, value.dtype) for value in arguments]
        + [
            pltpu.VMEM((16, DV), F32),
            pltpu.VMEM((NX, 64, 256), BF16),
            pltpu.VMEM((4, 64, 128), F32),
            pltpu.VMEM((NX, 4, 64, 128), BF16),
            pltpu.VMEM((NX, 64, 256), BF16),
            pltpu.VMEM((NX, 128, 512), BF16),
            pltpu.VMEM((NZ * NX, 16, 256), BF16),
            pltpu.VMEM((NX * NZ, 16, 256), BF16),
            pltpu.VMEM((NX, 16, 256), BF16),
            pltpu.VMEM((128, 1024), BF16),
            pltpu.VMEM((NT, 32, 128), BF16),
            pltpu.VMEM((NT, 32, 128), BF16),
            pltpu.VMEM((32, 128), BF16),
            pltpu.VMEM((NT, 32, 128), BF16),
            pltpu.VMEM((32, 128), BF16),
            pltpu.VMEM((NZ, 32, 128), BF16),
            pltpu.VMEM((NZ, 32, 128), BF16),
            pltpu.VMEM((2, NZ, 48, 128), BF16),
            pltpu.VMEM((2, NT, 48, 1024), BF16),
            pltpu.VMEM((NZ, 48, 128), BF16),
            pltpu.VMEM((NT, 48, 1024), BF16),
            pltpu.VMEM((NX, 16, 896), BF16),
            pltpu.VMEM((NX, 16, 896), BF16),
            pltpu.VMEM((NX, 16, 768), BF16),
            pltpu.VMEM((NX, 16, 768), BF16),
            pltpu.VMEM((2, NX, 16, 384), BF16),
            pltpu.VMEM((NZ, 32, 128), BF16),
            pltpu.VMEM((NZ, 32, 128), BF16),
            pltpu.VMEM((32, 128), BF16),
            pltpu.VMEM((NT, 32, 128), BF16),
            pltpu.SemaphoreType.DMA((4,)),
            pltpu.SemaphoreType.DMA((COPIES,)),
            pltpu.SemaphoreType.DMA((8,)),
        ],
        compiler_params=pltpu.CompilerParams(
            collective_id=0, has_side_effects=True, vmem_limit_bytes=40 * 1024 * 1024
        ),
    )(*arguments)
    result, new_state = pl.pallas_call(
        finish,
        out_shape=(
            jax.ShapeDtypeStruct((64, 512), BF16),
            jax.ShapeDtypeStruct((shape[0], DK, DV), F32),
        ),
        in_specs=[vmem, vmem],
        out_specs=(hbm, hbm),
        scratch_shapes=[pltpu.SemaphoreType.DMA((2,))],
        compiler_params=pltpu.CompilerParams(vmem_limit_bytes=8 * 1024 * 1024),
    )(result, new_state)
    return (result.T, new_state.reshape(shape))


def solution(mesh):
    return jax.shard_map(
        body,
        mesh=mesh,
        in_specs=(
            P(None, "kv"),
            P("kv"),
            P("kv", "tp"),
            P("kv", "tp"),
            P("kv", "tp"),
            P("kv", "tp"),
            P("kv", "tp"),
            P("kv", "tp"),
            P("kv", "tp", None, None),
            P(),
            P("tp", "kv"),
            P("kv"),
            P("kv", "tp"),
            P("kv", "tp"),
            P("tp", "kv"),
        ),
        out_specs=(P(None, "kv"), P("kv", "tp", None, None)),
        check_vma=False,
    )
```

```python
import functools

import jax
import jax.numpy as jnp
from jax import lax
from jax.experimental import pallas as pl
from jax.experimental.pallas import tpu as pltpu
from jax.sharding import PartitionSpec as P

MESH = pl.DeviceIdType.MESH
F32 = jnp.float32
BF16 = jnp.bfloat16

D = 2048
DK = 128
DV = 256
EPS = 1e-06
GATE_NORM = 16.0

NX, NY, NZ = 4, 4, 8
NT = 2 * NY
COPIES = 32
SMALL, UP, DOWN, LAST = range(4)
FAR_X = [2, 1, 3]
FAR_Y = [2, 1, 3]
FAR_Z = [4, 3, 5, 2, 6, 1, 7]
FAR_T = [4, 5, 2, 3, 6, 7, 1]
X_ORDER = [(0, 4), (2, 6), (3, 7), (1, 5)]
PLANE = [(dz, dx) for dz in FAR_Z + [0] for dx in FAR_X + [0] if (dz, dx) != (0, 0)]
LOADS = [(0, 0), (1, 1), (2, 0), (3, 0), (4, 0), (5, 0), (6, 0)]
LOADS += [(10, 3), (12, 2), (13, 2), (14, 2), (11, 4), (7, 5), (9, 6), (8, 7)]


def sigmoid(value):
    return 1.0 / (1.0 + jnp.exp(-value))


def as_pair(total):
    high = jnp.broadcast_to(total, (total.shape[0], 128)).astype(BF16).astype(F32)
    low = jnp.broadcast_to(total, (total.shape[0], 128)) - high
    lane = lax.broadcasted_iota(jnp.int32, high.shape, 1)
    return jnp.where(lane < 64, high, low).astype(BF16)


def of_pair(pair):
    return pair[:, 0:1] + pair[:, 64:65]


def packed_products(first, second, lane):
    blocks = []
    for j in range(8):
        low = first[:, 128 * j : 128 * j + 128]
        high = second[:, 128 * j : 128 * j + 128]
        top = low[0:32] + pltpu.roll(high[0:32], 64, 1)
        bottom = pltpu.roll(low[32:64], 64, 1) + high[32:64]
        blocks.append(jnp.where(lane < 64, top, bottom))
    return blocks


def kernel(*refs):
    inputs, (result, new_state), refs = refs[:15], refs[15:17], refs[17:]
    held, refs = refs[:15], refs[15:]
    (
        tokens,
        norm_gain,
        w_query,
        w_key,
        w_value,
        w_gate,
        w_decay,
        log_decay,
        state,
        out_gain,
        w_out,
        mixer_gain,
        w_ffgate,
        w_ffup,
        w_down,
    ) = held
    (
        att,
        w_own,
        x_own,
        x_all,
        w_all,
        w_diag,
        part1,
        got1,
        mix,
        w_mix,
        part2,
        got2,
        attn_own,
        attn_all,
        tok_own,
        tok_all,
        middle,
        up_own,
        up_all,
        down_own,
        down_all,
        part3a,
        got3a,
        part3b,
        got3b,
        hid,
        part4,
        got4,
        res_own,
        res_all,
        send_sems,
        recv_sems,
        local_sems,
    ) = refs
    kv = lax.axis_index("kv")
    t = lax.axis_index("tp")
    z, x = lax.div(kv, NX), lax.rem(kv, NX)
    y, core = lax.div(t, 2), lax.rem(t, 2)

    def at_x(d):
        return lax.rem(x + d, NX)

    def at_z(d):
        return lax.rem(z + d, NZ)

    def at_t(d):
        return lax.rem(t + d, NT)

    counter = [0]

    class Exchange:
        def __init__(self, size, group=SMALL):
            self.number, self.group, self.size = counter[0], group, size
            counter[0] += 1

        def send(self, src, dst, peer):
            pltpu.make_async_remote_copy(
                src_ref=src,
                dst_ref=dst,
                send_sem=send_sems.at[self.group],
                recv_sem=recv_sems.at[self.number],
                device_id=peer,
                device_id_type=MESH,
            ).start()

        def arrive(self):
            pltpu.make_async_copy(self.size, self.size, recv_sems.at[self.number]).wait()

    barrier = pltpu.get_barrier_semaphore()

    def greet(peer):
        pl.semaphore_signal(barrier, inc=1, device_id=peer, device_id_type=MESH)

    for dz, dx in PLANE:
        greet((at_z(dz) * NX + at_x(dx), t))
    for d in FAR_T:
        greet((kv, at_t(d)))
    for i, sem in LOADS:
        pltpu.make_async_copy(inputs[i], held[i], local_sems.at[sem]).start()

    def loaded(sem, size):
        pltpu.make_async_copy(size, size, local_sems.at[sem]).wait()

    with jax.named_scope("wait_first"):
        loaded(0, part1.at[0:22])
        loaded(1, norm_gain)
    square = (64, 64)
    row = lax.broadcasted_iota(jnp.int32, square, 0)
    column = lax.broadcasted_iota(jnp.int32, square, 1)
    gain = jnp.sum(
        jnp.where(row == column, jnp.broadcast_to(norm_gain[...].astype(F32), square), 0.0),
        axis=1,
        keepdims=True,
    )

    def gained(weight):
        return (weight[...].astype(F32) * gain).astype(BF16)

    w_own[0, :, 0:128] = gained(w_query)
    w_own[0, :, 128:256] = gained(w_key)
    w_own[1] = gained(w_value)
    w_own[2] = gained(w_gate)
    w_own[3, :, 0:128] = gained(w_decay)
    w_own[3, :, 128:256] = jnp.zeros((64, 128), BF16)
    own = jnp.concatenate([tokens[:, 0:256], tokens[:, 256:512]], axis=0).astype(F32)
    own = jnp.transpose(own, (1, 0))
    x_own[...] = own.reshape(4, 64, 128)
    x_all[x] = own.astype(BF16).reshape(4, 64, 128)
    w_all[x] = w_own[x]

    with jax.named_scope("wait_barrier"):
        pl.semaphore_wait(barrier, len(PLANE) + len(FAR_T))

    tile_z = w_mix.at[:, 0:128]

    def lanes_of(block):
        return pl.ds(pl.multiple_of(block * 128, 128), 128)

    ring_x = [(d, (z * NX + at_x(d), t)) for d in FAR_X]
    ring_z = [(d, (at_z(d) * NX + x, t)) for d in FAR_Z]
    ring_t = [(d, (kv, at_t(d))) for d in FAR_T]
    gather_w = Exchange(w_all.at[0:3], DOWN)
    gather_x = [Exchange(x_all.at[0:3, 0], UP) for _ in X_ORDER]
    x_blocks = [lax.rem(z + steps[0], 4) for steps in X_ORDER]
    for d, peer in ring_x:
        gather_w.send(w_own.at[at_x(d)], w_all.at[x], peer)
    for exchange, r in zip(gather_x, x_blocks):
        for d, peer in ring_x:
            exchange.send(x_all.at[x, r], x_all.at[x, r], peer)

    with jax.named_scope("wait_later"):
        loaded(3, w_out)
    out_rows = jnp.concatenate([w_out[:, 0:128], w_out[:, 128:256]], axis=0).astype(F32)
    w_mix[:, lanes_of(z)] = jnp.transpose(out_rows, (1, 0)).astype(BF16)
    mix_steps = []

    def mix_step(step):
        if step > 1:
            for exchange in mix_steps[-1]:
                exchange.arrive()
        exchanges = []
        for way in (1, -1):
            if step <= (4 if way > 0 else 3):
                lanes = lanes_of(at_z(NZ - way * (step - 1)))
                exchange = Exchange(tile_z)
                exchange.send(
                    w_mix.at[:, lanes], w_mix.at[:, lanes], (at_z(NZ + way) * NX + x, t)
                )
                exchanges.append(exchange)
        mix_steps.append(exchanges)

    mix_step(1)

    with jax.named_scope("wait_later"):
        loaded(2, up_all.at[0, 0:3])
        loaded(4, mixer_gain)
        loaded(5, log_decay)
        loaded(6, out_gain)
    gains = mixer_gain[...].astype(F32)
    units = jnp.transpose(
        jnp.concatenate([w_ffgate[...], w_ffup[...]], axis=0).astype(F32), (1, 0)
    )
    units = (units * jnp.concatenate([gains, gains], axis=1)).astype(BF16)
    down = w_down[...].astype(F32)
    down = jnp.concatenate([down, pltpu.roll(down, 768 - 48, 1)], axis=0)
    down = jnp.transpose(down, (1, 0)).astype(BF16)
    for j in range(NZ):
        up_own[0, j] = units[96 * j : 96 * j + 48]
        up_own[1, j] = units[96 * j + 48 : 96 * j + 96]
        down_own[j] = down[96 * j : 96 * j + 48]
    lanes_z = lanes_of(z)
    for half in range(2):
        up_all[half, t, :, lanes_z] = up_own[half, z]
    down_all[t, :, lanes_z] = down_own[z]
    up_blocks = [Exchange(up_own.at[half, 0:7]) for half in range(2)]
    up_y = [Exchange(up_all.at[half, 0:3], UP) for half in range(2)]
    up_core = [Exchange(up_all.at[half, 0:4], UP) for half in range(2)]
    partner = (kv, t + 1 - 2 * core)

    def along_y(d):
        return lax.rem(y + d, NY) * 2 + core

    def up_along_z(half):
        for d, peer in ring_z:
            up_blocks[half].send(
                up_own.at[half, at_z(d)], up_all.at[half, t, :, lanes_z], peer
            )

    def up_along_y(half):
        with jax.named_scope(f"wait_up_blocks_{half}"):
            up_blocks[half].arrive()
        for d in FAR_Y:
            up_y[half].send(up_all.at[half, t], up_all.at[half, t], (kv, along_y(d)))
        up_core[half].send(up_all.at[half, t], up_all.at[half, t], partner)

    up_along_z(0)
    lane32 = lax.broadcasted_iota(jnp.int32, (32, 128), 1)
    ours = x_own[:, pl.ds(pl.multiple_of(8 * t, 8), 8), :]
    tok_own[...] = ours.reshape(32, 128).astype(BF16)
    tok_all[z] = tok_own[...]
    w_diag[...] = jnp.zeros(w_diag.shape, BF16)

    with jax.named_scope("wait_mix_step"):
        mix_step(2)

    with jax.named_scope("wait_gather1_w"):
        gather_w.arrive()
    for j in range(NX):
        w_diag[j, 0:64, 0:256] = w_all[j]
        w_diag[j, 64:128, 256:512] = w_all[j]
    lane64 = lax.broadcasted_iota(jnp.int32, (64, 128), 1)
    has_sums = x == NX - 1
    scatter1 = Exchange(got1.at[0:31])
    for number, (r, steps) in enumerate(zip(x_blocks, X_ORDER)):
        with jax.named_scope(f"wait_gather1_{number}"):
            gather_x[number].arrive()
        total = jnp.zeros((64, 512), F32)
        squares = jnp.zeros((64, 128), F32)
        for j in range(NX):
            block = x_all[j, r]
            total += jnp.dot(block, w_diag[j], preferred_element_type=F32)
            wide = block.astype(F32)
            squares += wide * wide
        for side in range(2):
            ours = (lane64 < 64) if side == 0 else (lane64 >= 64)
            sums = as_pair(jnp.sum(jnp.where(ours, squares, 0.0), axis=1, keepdims=True))
            first = 256 * side
            for k in range(NX):
                rows = slice(16 * k, 16 * k + 16)
                owner = NX * (r + 4 * side) + k
                part1[owner, :, 0:128] = total[rows, first : first + 128].astype(BF16)
                part1[owner, :, 128:256] = jnp.where(
                    has_sums, sums[rows].astype(F32), total[rows, first + 128 : first + 256]
                ).astype(BF16)
        for dz in sorted(steps, key=lambda step: -min(step, NZ - step)):
            for dx in FAR_X + [0]:
                if (dz, dx) != (0, 0):
                    peer = at_z(dz) * NX + at_x(dx)
                    scatter1.send(part1.at[peer], got1.at[x * NZ + z], (peer, t))
    got1[x * NZ + z] = part1[kv]

    with jax.named_scope("wait_mix_step3"):
        mix_step(3)
    up_along_y(0)
    with jax.named_scope("wait_mix_step4"):
        mix_step(4)
    up_along_z(1)

    with jax.named_scope("wait_scatter1"):
        scatter1.arrive()
    proj = []
    for j in range(NX):
        total = got1[NZ * j].astype(F32)
        for k in range(1, NZ):
            total += got1[NZ * j + k].astype(F32)
        proj.append(total)
    loaded(7, state)

    inv = lax.rsqrt(of_pair(proj[3][:, 128:256]) / D + EPS)
    query = proj[0][:, 0:128] * (inv * DK ** (-0.5))
    keys = proj[0][:, 128:256] * inv
    values = proj[1] * inv
    gate = proj[2] * inv
    decay_pre = proj[3][:, 0:128] * inv
    log_sigmoid = jnp.minimum(decay_pre, 0.0) - jnp.log1p(jnp.exp(-jnp.abs(decay_pre)))
    decay = jnp.exp(log_sigmoid / GATE_NORM + log_decay[...])
    columns = jnp.transpose(
        jnp.concatenate([query * decay, keys, decay, jnp.zeros((80, 128), F32)], axis=0), (1, 0)
    )
    for b in range(16):
        att[b : b + 1, :] = jnp.sum(state[b] * columns[:, b : b + 1], axis=0, keepdims=True)
    attended = att[...] + jnp.sum(query * keys, axis=1, keepdims=True) * values
    normed = (
        attended
        * lax.rsqrt(jnp.mean(attended * attended, axis=1, keepdims=True) + EPS)
        * out_gain[...]
    )
    mix[x] = (normed * (gate * sigmoid(gate))).astype(BF16)
    gather2 = Exchange(mix.at[0:3])
    for d, peer in ring_x:
        gather2.send(mix.at[x], mix.at[x], peer)
    down_blocks = Exchange(down_own.at[0:7])
    for d, peer in ring_z:
        down_blocks.send(down_own.at[at_z(d)], down_all.at[t, :, lanes_z], peer)
    tok_blocks = Exchange(tok_all.at[0:7])
    for d, peer in ring_z:
        tok_blocks.send(tok_own, tok_all.at[z], peer)
    for b in range(16):
        k_col = columns[:, 16 + b : 17 + b]
        a_col = columns[:, 32 + b : 33 + b]
        new_state[b] = state[b] * a_col + k_col * values[b : b + 1, :]

    with jax.named_scope("wait_mix_blocks"):
        for exchange in mix_steps[-1]:
            exchange.arrive()
    with jax.named_scope("wait_gather2"):
        gather2.arrive()
    mixed = mix[...].reshape(64, DV)
    stacked = jnp.concatenate([mixed[:, 0:128], mixed[:, 128:256]], axis=0)
    total = jnp.dot(stacked, w_mix[...], preferred_element_type=F32)
    lane64 = lax.broadcasted_iota(jnp.int32, (64, 128), 1)
    pairs = []
    for p in range(4):
        low, high = [
            (total[0:64, first : first + 128], total[64:128, first : first + 128])
            for first in (256 * p, 256 * p + 128)
        ]
        pairs.append(
            jnp.where(
                lane64 < 64,
                low[0] + pltpu.roll(low[1], 64, 1),
                pltpu.roll(high[0], 64, 1) + high[1],
            )
        )
    for j in range(NT):
        rows = slice(8 * j, 8 * j + 8)
        part2[j] = jnp.concatenate([pair[rows] for pair in pairs], axis=0).astype(BF16)
    got2[t] = part2[t]
    scatter2 = Exchange(got2.at[0:7])
    for d, peer in ring_t:
        scatter2.send(part2.at[at_t(d)], got2.at[t], peer)
    up_along_y(1)
    with jax.named_scope("wait_scatter2"):
        scatter2.arrive()
    total = got2[0].astype(F32)
    for j in range(1, NT):
        total += got2[j].astype(F32)
    attn_own[...] = total.astype(BF16)

    attn_all[z] = attn_own[...]
    spread = Exchange(attn_all.at[0:7])
    for d, peer in ring_z:
        spread.send(attn_own, attn_all.at[z], peer)

    with jax.named_scope("wait_down_blocks"):
        down_blocks.arrive()
    down_y, down_core = Exchange(down_all.at[0:3], DOWN), Exchange(down_all.at[0:4], DOWN)
    for d in FAR_Y:
        down_y.send(down_all.at[t], down_all.at[t], (kv, along_y(d)))
    for half in range(2):
        with jax.named_scope(f"wait_up_y_{half}"):
            up_y[half].arrive()
        for d in range(1, NY):
            other = along_y(d)
            up_core[half].send(up_all.at[half, other], up_all.at[half, other], partner)
    down_core.send(down_all.at[t], down_all.at[t], partner)

    with jax.named_scope("wait_tok_blocks"):
        tok_blocks.arrive()
    with jax.named_scope("wait_spread"):
        spread.arrive()

    squares = jnp.zeros((64, 128), F32)
    pieces = []
    sums = [attn_all[j].astype(F32) for j in range(NZ)]
    middles = []
    for p in range(4):
        low, high = tok_all[2 * p].astype(F32), tok_all[2 * p + 1].astype(F32)
        residual = jnp.concatenate(
            [
                jnp.where(lane32 < 64, low, pltpu.roll(high, 64, 1)),
                jnp.where(lane32 < 64, pltpu.roll(low, 64, 1), high),
            ],
            axis=0,
        )
        added = jnp.concatenate([total[8 * p : 8 * p + 8] for total in sums], axis=0)
        wide = (residual + added).astype(BF16).astype(F32)
        middles.append(wide)
        squares += wide * wide
        turned = pltpu.roll(wide, 64, 1)
        for here, there in ((wide, turned), (turned, wide)):
            pieces.append(
                jnp.concatenate(
                    [jnp.where(lane64 < 64, here, 0.0), jnp.where(lane64 < 64, 0.0, there)], axis=0
                ).astype(BF16)
            )
    left = jnp.concatenate(pieces, axis=1)
    squares = as_pair(jnp.sum(squares, axis=1, keepdims=True))
    parts3, gots3 = (part3a, part3b), (got3a, got3b)
    scatter3 = [Exchange(got3.at[0:3]) for got3 in gots3]
    for half, (part3, got3) in enumerate(zip(parts3, gots3)):
        with jax.named_scope(f"wait_up_core_{half}"):
            up_core[half].arrive()
        terms = lax.dot_general(
            left,
            up_all[half].reshape(384, 1024),
            (((1,), (1,)), ((), ())),
            preferred_element_type=F32,
        )
        for j in range(NX):
            rows = slice(16 * j, 16 * j + 16)
            part3[j, :, 0:384] = terms[rows].astype(BF16)
            part3[j, :, 384:768] = terms[64 + 16 * j : 80 + 16 * j].astype(BF16)
            if half == 0:
                part3[j, :, 768:896] = squares[rows]
        got3[x] = part3[x]
        for d, peer in ring_x:
            scatter3[half].send(part3.at[at_x(d)], got3.at[x], peer)
    for p, wide in enumerate(middles):
        turned = pltpu.roll(wide, 64, 1)
        middle[2 * p] = jnp.where(lane32 < 64, wide[0:32], turned[32:64]).astype(BF16)
        middle[2 * p + 1] = jnp.where(lane32 < 64, turned[0:32], wide[32:64]).astype(BF16)
    with jax.named_scope("wait_down_y"):
        down_y.arrive()
    for d in range(1, NY):
        other = along_y(d)
        down_core.send(down_all.at[other], down_all.at[other], partner)
    gather3 = [Exchange(hid.at[half, 0:3]) for half in range(2)]
    inv = None
    for half, got3 in enumerate(gots3):
        with jax.named_scope(f"wait_scatter3_{half}"):
            scatter3[half].arrive()
        total = got3[0].astype(F32)
        for j in range(1, NX):
            total += got3[j].astype(F32)
        if half == 0:
            inv = lax.rsqrt(of_pair(total[:, 768:896]) / D + EPS)
        gate = total[:, 0:384] * inv
        hid[half, x] = (gate * sigmoid(gate) * (total[:, 384:768] * inv)).astype(BF16)
        for d, peer in ring_x:
            gather3[half].send(hid.at[half, x], hid.at[half, x], peer)
    with jax.named_scope("wait_down_core"):
        down_core.arrive()

    weights = down_all[...].reshape(NT * 48, 1024)
    products = []
    for half in range(2):
        with jax.named_scope(f"wait_gather3_{half}"):
            gather3[half].arrive()
        products.append(
            jnp.dot(hid[half].reshape(64, 384), weights, preferred_element_type=F32)
        )
    for j, block in enumerate(packed_products(*products, lane32)):
        part4[j] = block.astype(BF16)
    got4[z] = part4[z]
    scatter4 = Exchange(got4.at[0:7])
    for d, peer in ring_z:
        scatter4.send(part4.at[at_z(d)], got4.at[z], peer)
    with jax.named_scope("wait_scatter4"):
        scatter4.arrive()
    total = got4[0].astype(F32)
    for j in range(1, NZ):
        total += got4[j].astype(F32)
    res_own[...] = (middle[z].astype(F32) + total).astype(BF16)
    res_all[t] = res_own[...]
    gather4 = Exchange(res_all.at[0:7], LAST)
    for d, peer in ring_t:
        gather4.send(res_own, res_all.at[t], peer)
    with jax.named_scope("wait_gather4"):
        gather4.arrive()
    blocks = [res_all[j].astype(F32) for j in range(NT)]
    blocks = [blocks, [pltpu.roll(block, 64, 1) for block in blocks]]
    rows = jnp.concatenate(
        [
            blocks[j // 4][k][8 * (j % 4) : 8 * (j % 4) + 8]
            for j in range(NZ)
            for k in range(NT)
        ],
        axis=0,
    )
    result[...] = jnp.transpose(rows, (1, 0))[0:64].astype(BF16)
    with jax.named_scope("wait_sends"):
        everything = (state.at[0:15, 0:80], up_all, up_all.at[0], res_all.at[0:7])
        for group, size in enumerate(everything):
            pltpu.make_async_copy(size, size, send_sems.at[group]).wait()


def finish(result_in, state_in, result_out, state_out, sems):
    result = pltpu.make_async_copy(result_in, result_out, sems.at[0])
    states = pltpu.make_async_copy(state_in, state_out, sems.at[1])
    parts = [pl.ds(2 * i, 2) for i in range(8)]
    result.start()
    for part in parts:
        pltpu.make_async_copy(state_in.at[part], state_out.at[part], sems.at[1]).start()
    result.wait()
    states.wait()


def body(
    tokens,
    norm_gain,
    w_query,
    w_key,
    w_value,
    w_gate,
    w_decay,
    log_decay,
    state,
    out_gain,
    w_out,
    mixer_gain,
    w_ffgate,
    w_ffup,
    w_down,
):
    vmem = pl.BlockSpec(memory_space=pltpu.VMEM)
    hbm = pl.BlockSpec(memory_space=pltpu.HBM)
    shape = state.shape
    arguments = (
        tokens.T,
        norm_gain.reshape(1, 64),
        w_query,
        w_key,
        w_value,
        w_gate,
        w_decay,
        log_decay,
        state.reshape(shape[0], DK, DV),
        out_gain.reshape(1, DV),
        w_out.T,
        mixer_gain.reshape(1, 64),
        w_ffgate,
        w_ffup,
        w_down.T,
    )
    arguments = [pltpu.with_memory_space_constraint(value, pltpu.HBM) for value in arguments]
    result, new_state = pl.pallas_call(
        kernel,
        out_shape=(
            pltpu.VMEM((64, 512), BF16),
            pltpu.VMEM((shape[0], DK, DV), F32),
        ),
        in_specs=[hbm] * 15,
        out_specs=(vmem, vmem),
        scratch_shapes=[pltpu.VMEM(value.shape, value.dtype) for value in arguments]
        + [
            pltpu.VMEM((16, DV), F32),
            pltpu.VMEM((NX, 64, 256), BF16),
            pltpu.VMEM((4, 64, 128), F32),
            pltpu.VMEM((NX, 4, 64, 128), BF16),
            pltpu.VMEM((NX, 64, 256), BF16),
            pltpu.VMEM((NX, 128, 512), BF16),
            pltpu.VMEM((NZ * NX, 16, 256), BF16),
            pltpu.VMEM((NX * NZ, 16, 256), BF16),
            pltpu.VMEM((NX, 16, 256), BF16),
            pltpu.VMEM((128, 1024), BF16),
            pltpu.VMEM((NT, 32, 128), BF16),
            pltpu.VMEM((NT, 32, 128), BF16),
            pltpu.VMEM((32, 128), BF16),
            pltpu.VMEM((NT, 32, 128), BF16),
            pltpu.VMEM((32, 128), BF16),
            pltpu.VMEM((NZ, 32, 128), BF16),
            pltpu.VMEM((NZ, 32, 128), BF16),
            pltpu.VMEM((2, NZ, 48, 128), BF16),
            pltpu.VMEM((2, NT, 48, 1024), BF16),
            pltpu.VMEM((NZ, 48, 128), BF16),
            pltpu.VMEM((NT, 48, 1024), BF16),
            pltpu.VMEM((NX, 16, 896), BF16),
            pltpu.VMEM((NX, 16, 896), BF16),
            pltpu.VMEM((NX, 16, 768), BF16),
            pltpu.VMEM((NX, 16, 768), BF16),
            pltpu.VMEM((2, NX, 16, 384), BF16),
            pltpu.VMEM((NZ, 32, 128), BF16),
            pltpu.VMEM((NZ, 32, 128), BF16),
            pltpu.VMEM((32, 128), BF16),
            pltpu.VMEM((NT, 32, 128), BF16),
            pltpu.SemaphoreType.DMA((4,)),
            pltpu.SemaphoreType.DMA((COPIES,)),
            pltpu.SemaphoreType.DMA((8,)),
        ],
        compiler_params=pltpu.CompilerParams(
            collective_id=0, has_side_effects=True, vmem_limit_bytes=40 * 1024 * 1024
        ),
    )(*arguments)
    result, new_state = pl.pallas_call(
        finish,
        out_shape=(
            jax.ShapeDtypeStruct((64, 512), BF16),
            jax.ShapeDtypeStruct((shape[0], DK, DV), F32),
        ),
        in_specs=[vmem, vmem],
        out_specs=(hbm, hbm),
        scratch_shapes=[pltpu.SemaphoreType.DMA((2,))],
        compiler_params=pltpu.CompilerParams(vmem_limit_bytes=8 * 1024 * 1024),
    )(result, new_state)
    return (result.T, new_state.reshape(shape))


def solution(mesh):
    return jax.shard_map(
        body,
        mesh=mesh,
        in_specs=(
            P(None, "kv"),
            P("kv"),
            P("kv", "tp"),
            P("kv", "tp"),
            P("kv", "tp"),
            P("kv", "tp"),
            P("kv", "tp"),
            P("kv", "tp"),
            P("kv", "tp", None, None),
            P(),
            P("tp", "kv"),
            P("kv"),
            P("kv", "tp"),
            P("kv", "tp"),
            P("tp", "kv"),
        ),
        out_specs=(P(None, "kv"), P("kv", "tp", None, None)),
        check_vma=False,
    )
```
